256 devices in a mesh: sp: 64 (over z, x, core), tp: 4 (over y).
Axes of the slice: x: 4, y: 4, z: 8, core: 2. Of those that a mesh axis runs over, the one named last changes fastest.
Arguments:
- tokens: bfloat16 [24576, 2048], P('sp', 'tp'), may hold values from -6 to 6
- norm_gain: float32 [2048], replicated, may hold values from 0.1 to 1.9
- w_pool_in: bfloat16 [2048, 2048], P('sp', 'tp'), may hold values from -0.125 to 0.125
- w_lru_in: bfloat16 [2048, 2048], P('sp', 'tp'), may hold values from -0.125 to 0.125
- pool_mix: bfloat16 [4, 512, 512], P('tp'), may hold values from -0.25 to 0.25
- conv_taps: bfloat16 [4, 2048], P(None, 'tp'), may hold values from -3 to 3
- rec_gate: bfloat16 [2, 16, 128, 128], P(None, 'tp'), may hold values from -0.5 to 0.5
- in_gate: bfloat16 [2, 16, 128, 128], P(None, 'tp'), may hold values from -0.5 to 0.5
- decay_rate: float32 [2, 2048], P(None, 'tp'), may hold values from 0 to 1, as said below
- log_decay: float32 [2, 24576], P(None, 'sp'), may hold values from -2 to 0, as said below
- start_state: float32 [2, 2048], P(None, 'tp'), may hold values from -8 to 8
- w_out_pool: bfloat16 [2048, 2048], P('tp', 'sp'), may hold values from -0.09375 to 0.09375
- w_out_lru: bfloat16 [2048, 2048], P('tp', 'sp'), may hold values from -0.09375 to 0.09375
Outputs:
- mixed: bfloat16 [24576, 2048], P(('sp', 'tp'))
The draws below stay inside these ranges and needn't reach their ends.
Inputs may be any that keep to these rules, and one draw needn't show every extreme that they name: `decay_rate`: positive. `log_decay`: at most zero.
All inputs are finite; a program needn't handle non-finite values.
Results may differ from the reference program's by a relative error of at most 0.0068.
Values may be sent and summed in bfloat16 or wider, within the bound.
A program may use at most 64 MiB of HBM per device.

```python
import math
import jax
import jax.numpy as jnp
from jax import lax

D = 2048
D_POOL = 2048
POOL_GROUPS = 4
GROUP_W = 512
D_LRU = 2048
HEAD = 128
BLOCKS = 16
CONV = 4
GRID_W = 32
TOKENS = 24576
ROWS = 768


def draw_decay_rate(key, part):
    pick_key, slow_key, fast_key = jax.random.split(jax.random.fold_in(key, 11), 3)
    slow_rate = jnp.exp(jax.random.uniform(slow_key, (2, D_LRU), jnp.float32, math.log(0.02), math.log(0.1))) / TOKENS
    fast_rate = jnp.exp(jax.random.uniform(fast_key, (2, D_LRU), jnp.float32, math.log(1.0 / 400.0), math.log(1.0 / 120.0)))
    share = 0.5
    chosen = jax.random.uniform(pick_key, (2, D_LRU), jnp.float32) < share
    return jnp.where(chosen, fast_rate, slow_rate).astype(jnp.float32)


def draw_log_decay(key, part):
    rate_key, place_key, depth_key = jax.random.split(jax.random.fold_in(key, 23), 3)
    lower_rate = 0.2
    upper_rate = 0.8
    grid_rows = TOKENS // GRID_W
    row_rates = jnp.exp(jax.random.uniform(rate_key, (2, grid_rows), jnp.float32, math.log(lower_rate), math.log(upper_rate))) / TOKENS
    equilibrium_hidden = -jnp.repeat(row_rates, GRID_W, axis=1)
    element_slots = jax.random.randint(place_key, (2, 3), 0, TOKENS)
    layer_counts_drawn = jax.random.uniform(depth_key, (2, 3), jnp.float32, math.log(0.5), math.log(0.8))
    element_offsets = jnp.arange(TOKENS, dtype=jnp.int32)
    segment_extents = jnp.sum((element_offsets[None, None, :] == element_slots[:, :, None]).astype(jnp.float32) * layer_counts_drawn[:, :, None], axis=1)
    return (equilibrium_hidden + segment_extents).astype(jnp.float32)


def block_levels(stream_key, shape, pieces, least, top_value):
    gain, own = 1.0, jax.random.fold_in(stream_key, 6)
    for position, shards_of in pieces:
        draws = jnp.exp(jax.random.uniform(jax.random.fold_in(own, position), (shards_of,), jnp.float32, least / len(pieces), top_value / len(pieces)))
        gain = gain * jnp.repeat(draws, shape[position] // shards_of).reshape([-1 if axis == position else 1 for axis in range(len(shape))])
    return gain


def noise(own_key, shape, width, reach, pieces=(), kind=jnp.bfloat16):
    values = jax.random.normal(own_key, shape, jnp.float32) * width
    if len(pieces) > 0:
        values = block_levels(own_key, shape, pieces, -0.22, 0.18) * values
    return jnp.clip(values, min=-reach, max=reach).astype(kind)


def setup_inputs(seed: int = 0) -> dict:
    streams_of = jax.random.split(jax.random.key(seed), 14)
    tokens = noise(streams_of[0], (TOKENS, D), 1.0, 6.0, ((0, 64), (1, 4)))
    norm_gain = jnp.clip(1.0 + 0.18 * jax.random.normal(streams_of[1], (D,), jnp.float32), 0.1, 1.9)
    w_pool_in = noise(streams_of[2], (D, D_POOL), D ** -0.5, 0.125, ((0, 64), (1, 4)))
    w_lru_in = noise(streams_of[3], (D, D_LRU), D ** -0.5, 0.125, ((0, 64), (1, 4)))
    pool_mix = noise(streams_of[4], (POOL_GROUPS, GROUP_W, GROUP_W), GROUP_W ** -0.5, 0.25, ((0, 4),))
    conv_taps = noise(streams_of[5], (CONV, D_LRU), 0.5, 3.0, ((1, 4),))
    rec_gate = noise(streams_of[6], (2, BLOCKS, HEAD, HEAD), HEAD ** -0.5, 0.5, ((1, 4),))
    in_gate = noise(streams_of[7], (2, BLOCKS, HEAD, HEAD), HEAD ** -0.5, 0.5, ((1, 4),))
    decay_rate = draw_decay_rate(jax.random.fold_in(streams_of[13], 71), 0)
    log_decay = draw_log_decay(jax.random.fold_in(streams_of[13], 71), 0)
    start_state = noise(streams_of[10], (2, D_LRU), 2.0, 8.0, ((1, 4),), jnp.float32)
    w_out_pool = noise(streams_of[11], (D_POOL, D), (D_POOL + D_LRU) ** -0.5, 0.09375, ((0, 4), (1, 64)))
    w_out_lru = noise(streams_of[12], (D_LRU, D), (D_POOL + D_LRU) ** -0.5, 0.09375, ((0, 4), (1, 64)))
    return {"tokens": tokens, "norm_gain": norm_gain, "w_pool_in": w_pool_in, "w_lru_in": w_lru_in, "pool_mix": pool_mix, "conv_taps": conv_taps, "rec_gate": rec_gate, "in_gate": in_gate, "decay_rate": decay_rate, "log_decay": log_decay, "start_state": start_state, "w_out_pool": w_out_pool, "w_out_lru": w_out_lru}


epsilon = 1e-06

def box_bounds(length, span_len):
    element_offsets = jnp.arange(length, dtype=jnp.int32)
    lower_end = jnp.clip(element_offsets - span_len // 2, 0, length)
    upper_end = jnp.clip(element_offsets + span_len - span_len // 2, 0, length)
    return (lower_end, upper_end)

def box_sum(values, span_len, axis_dim):
    length = values.shape[axis_dim]
    pad_widths = [(0, 0)] * values.ndim
    pad_widths[axis_dim] = (span_len // 2, span_len // 2)
    padded = jnp.pad(values, pad_widths)
    total_sum = jnp.zeros_like(values)
    for offset in range(span_len):
        total_sum = total_sum + lax.slice_in_dim(padded, offset, offset + length, axis=axis_dim)
    return total_sum

def reference(tokens, norm_gain, w_pool_in, w_lru_in, pool_mix, conv_taps, rec_gate, in_gate, decay_rate, log_decay, start_state, w_out_pool, w_out_lru):
    values = tokens.astype(jnp.float32)
    root_mean_square_scale = lax.rsqrt(lax.optimization_barrier(jnp.mean(values * values, axis=1, keepdims=True)) + epsilon)
    normed = (values * root_mean_square_scale * norm_gain).astype(jnp.bfloat16)
    u_pool = jnp.dot(normed, w_pool_in, preferred_element_type=jnp.float32).astype(jnp.bfloat16)
    u_lru = jnp.dot(normed, w_lru_in, preferred_element_type=jnp.float32).astype(jnp.bfloat16)
    grid_pooled_image = u_pool.reshape(ROWS, GRID_W, D_POOL)
    outputs_pool = []
    for group_index in range(POOL_GROUPS):
        span_len = 2 ** (group_index + 1)
        channels = grid_pooled_image[:, :, group_index * GROUP_W:(group_index + 1) * GROUP_W].astype(jnp.float32)
        total_sum = box_sum(box_sum(channels, span_len, 0), span_len, 1)
        row_lower, row_upper = box_bounds(ROWS, span_len)
        col_lower, col_upper = box_bounds(GRID_W, span_len)
        counts = ((row_upper - row_lower)[:, None] * (col_upper - col_lower)[None, :]).astype(jnp.float32)
        pool_diff = (total_sum / counts[:, :, None] - channels).astype(jnp.bfloat16).reshape(TOKENS, GROUP_W)
        outputs_pool.append(jnp.dot(pool_diff, pool_mix[group_index], preferred_element_type=jnp.float32).astype(jnp.bfloat16))
    y_pool = jnp.concatenate(outputs_pool, axis=1)
    left_taps = CONV // 2
    padded = jnp.pad(u_lru.astype(jnp.float32), ((left_taps, CONV - 1 - left_taps), (0, 0)))
    tap_weights = conv_taps.astype(jnp.float32)
    conv_sum = padded[0:TOKENS] * tap_weights[0]
    for tap_index in range(1, CONV):
        conv_sum = conv_sum + padded[tap_index:tap_index + TOKENS] * tap_weights[tap_index]
    conv_in = conv_sum.astype(jnp.bfloat16)
    blocks = conv_in.astype(jnp.float32).reshape(TOKENS, BLOCKS, HEAD)
    drive_in = conv_in.astype(jnp.float32)
    histories = []
    for direction in range(2):
        recur_gate = jax.nn.sigmoid(jnp.einsum('tnc,ncd->tnd', blocks, rec_gate[direction].astype(jnp.float32)).reshape(TOKENS, D_LRU))
        input_gate = jax.nn.sigmoid(jnp.einsum('tnc,ncd->tnd', blocks, in_gate[direction].astype(jnp.float32)).reshape(TOKENS, D_LRU))
        log_keep = -8.0 * recur_gate * decay_rate[direction] + log_decay[direction][:, None]
        keep_rate = jnp.exp(log_keep)
        drive_term = jnp.sqrt(-jnp.expm1(2.0 * log_keep)) * input_gate * drive_in

        def recurrence_step(carried, pair_now):
            updated = pair_now[0] * carried + pair_now[1]
            return (updated, updated)
        _, history = lax.scan(recurrence_step, start_state[direction], (keep_rate, drive_term), reverse=direction == 1)
        histories.append(history)
    y_lru = (histories[0] + histories[1]).astype(jnp.bfloat16)
    mixed = jnp.dot(y_pool, w_out_pool, preferred_element_type=jnp.float32) + jnp.dot(y_lru, w_out_lru, preferred_element_type=jnp.float32)
    return mixed.astype(jnp.bfloat16)
```

```python
import functools

import jax
import jax.numpy as jnp
from jax import lax
from jax.experimental import pallas as pl
from jax.experimental.pallas import tpu as pltpu
from jax.sharding import Mesh
from jax.sharding import PartitionSpec as P

GRID_W = 32
REACH = 8
EPS = 1e-06
SP = ("sp_0", "sp_1", "sp_2")
SP_TP = ("sp_0", "sp_1", "sp_2", "tp")
NZ, NX, NC, NY = 8, 4, 2, 4
TOK = 384
D = 2048
CH = 512
SEGS = 8
SEG = TOK // SEGS
OWN = REACH * GRID_W
EXT = TOK + 2 * OWN
PAD = 16
OUT_ROWS = TOK // NY
N_DMA = 176
N_LOCAL = 8
F32 = jnp.float32
BF16 = jnp.bfloat16
NT = (((1,), (1,)), ((), ()))


class Links:
    def __init__(self, send, recv):
        self.send, self.recv, self.used, self.sent = send, recv, 0, []

    def slot(self):
        self.used += 1
        return self.used - 1

    def put(self, src, dst, slot, **dev):
        copy = pltpu.make_async_remote_copy(
            src_ref=src,
            dst_ref=dst,
            send_sem=self.send.at[slot],
            recv_sem=self.recv.at[slot],
            device_id=dev,
            device_id_type=pl.DeviceIdType.MESH,
        )
        copy.start()
        self.sent.append(copy)

    def got(self, region, slot, **dev):
        pltpu.make_async_remote_copy(
            src_ref=region,
            dst_ref=region,
            send_sem=self.send.at[slot],
            recv_sem=self.recv.at[slot],
            device_id=dev,
            device_id_type=pl.DeviceIdType.MESH,
        ).wait_recv()

    def drain(self):
        for copy in self.sent:
            copy.wait_send()


def weight_gather(links, buf, z, x, c):
    lo, hi = pl.ds(0, 16), pl.ds(16, 16)

    def zz(d):
        return lax.rem(z + (d + NZ), NZ)

    def xx(d):
        return lax.rem(x + (d + NX), NX)

    other = {"sp_2": 1 - c}
    a1 = {dx: links.slot() for dx in (1, 3, 2)}
    a2 = {
        (s, k, g): links.slot()
        for s in (1, -1)
        for g in (0, 1)
        for k in range(1, (5 if (s == 1) == (g == 0) else 4))
    }
    b1 = {(s, k): links.slot() for s in (1, -1) for k in range(1, 5 if s == 1 else 4)}
    rel = [0, -1, 1, -2, 2, -3, 3, 4]
    b2 = {(d, s): links.slot() for d in rel for s in (1, -1)}
    b3 = {d: links.slot() for d in rel}
    dd = {d: links.slot() for d in rel}

    def pair(d, g):
        return buf.at[zz(d), pl.ds(2 * g, 2), c, lo]

    def b_spread(d):
        piece = buf.at[zz(d), x, c, hi]
        for s in (1, -1):
            links.put(piece, piece, b2[d, s], sp_1=xx(s))

    def b_relay(d):
        for s in (1, -1):
            piece = buf.at[zz(d), xx(-s), c, hi]
            links.got(piece, b2[d, s], sp_1=xx(s))
            if (d % 2 == 0) == (s == 1):
                links.put(piece, piece, b3[d], sp_1=xx(s))

    def row_done(d):
        s = 1 if d % 2 == 0 else -1
        links.got(buf.at[zz(d), xx(2), c, hi], b3[d], sp_1=xx(s))
        row = buf.at[zz(d), pl.ds(0, NX), c]
        links.put(row, row, dd[d], **other)

    def first():
        own = buf.at[z, x, c, lo]
        for dx in (1, 3, 2):
            links.put(own, own, a1[dx], sp_1=xx(dx))
        own = buf.at[z, x, c, hi]
        for s in (1, -1):
            links.put(own, own, b1[s, 1], sp_0=zz(s))
        b_spread(0)

    def second():
        for dx in (1, 3, 2):
            links.got(buf.at[z, xx(-dx), c, lo], a1[dx], sp_1=xx(dx))
        for g in (0, 1):
            for s in (1, -1):
                links.put(pair(0, g), pair(0, g), a2[s, 1, g], sp_0=zz(s))

    def hop(k):
        for s in (1, -1):
            if (s, k) in b1:
                piece = buf.at[zz(-s * k), x, c, hi]
                links.got(piece, b1[s, k], sp_0=zz(s))
                if (s, k + 1) in b1:
                    links.put(piece, piece, b1[s, k + 1], sp_0=zz(s))
                b_spread(-s * k if k < 4 else 4)
        for g in (0, 1):
            for s in (1, -1):
                if (s, k, g) in a2:
                    piece = pair(-s * k, g)
                    links.got(piece, a2[s, k, g], sp_0=zz(s))
                    if (s, k + 1, g) in a2:
                        links.put(piece, piece, a2[s, k + 1, g], sp_0=zz(s))
        if k == 1:
            b_relay(0)
        else:
            b_relay(-(k - 1))
            b_relay(k - 1)
        if k == 2:
            row_done(0)
        if k > 2:
            row_done(-(k - 2))
            row_done(k - 2)

    def last():
        b_relay(4)
        for d in (-3, 3, 4):
            row_done(d)

    def arrived():
        for d in rel:
            links.got(buf.at[zz(d), pl.ds(0, NX), 1 - c], dd[d], **other)

    return [first, second] + [functools.partial(hop, k) for k in (1, 2, 3, 4)] + [last, arrived]


def logistic(v):
    return 1.0 / (1.0 + jnp.exp(-v))


def one_minus_exp(y, e):
    series = 1.0 + y * (1.0 / 8.0)
    for n in (7, 6, 5, 4, 3, 2):
        series = 1.0 + y * (1.0 / n) * series
    return jnp.where(y > -0.3, -y * series, 1.0 - e)


def layer(
    tokens, gain, wpi, wli, pmix, taps, rgate, igate, decay, logd, start, wop, wol, out,
    tok, nrm, win, wout, pmv, rgv, igv, box, rcp, ulb, ulf, hb, cvb, pext, pdf, gs, aa, bb,
    sg, ex, c1, c2, ycat, part, rs1, rs2, rs3, mg, send, recv, local,
):
    z, x, c = (lax.axis_index(n) for n in SP)
    y = lax.axis_index("tp")
    s = (z * NX + x) * NC + c
    links = Links(send, recv)

    def zz(d):
        return lax.rem(z + (d + NZ), NZ)

    def xx(d):
        return lax.rem(x + (d + NX), NX)

    def yy(d):
        return lax.rem(y + (d + NY), NY)

    def run_dev(d):
        t = lax.rem(s + (d + NZ * NX * NC), NZ * NX * NC)
        return {"sp_0": t // (NX * NC), "sp_1": lax.rem(t // NC, NX), "sp_2": lax.rem(t, NC)}

    after, before = run_dev(1), run_dev(-1)

    loads = [
        pltpu.make_async_copy(tokens, tok.at[y], local.at[0]),
        pltpu.make_async_copy(wpi, win.at[z, x, c, :, pl.ds(0, CH)], local.at[1]),
        pltpu.make_async_copy(wli, win.at[z, x, c, :, pl.ds(CH, CH)], local.at[2]),
        pltpu.make_async_copy(pmix, pmv, local.at[3]),
        pltpu.make_async_copy(rgate, rgv, local.at[4]),
        pltpu.make_async_copy(igate, igv, local.at[5]),
    ]
    for load in loads:
        load.start()

    barrier = pltpu.get_barrier_semaphore()
    peers = [{"tp": yy(1)}, {"tp": yy(-1)}, after, before]
    peers += [{"sp_0": zz(d)} for d in range(1, NZ)]
    around = [(dx, dc) for dx in range(NX) for dc in range(NC) if dx or dc]
    for dx, dc in around:
        peers.append({"sp_1": xx(dx), "sp_2": lax.rem(c + dc, NC)})
    for peer in peers:
        pl.semaphore_signal(barrier, inc=1, device_id=peer, device_id_type=pl.DeviceIdType.MESH)

    eye = (
        lax.broadcasted_iota(jnp.int32, (32, 32), 0) == lax.broadcasted_iota(jnp.int32, (32, 32), 1)
    ).astype(BF16)
    for k, w in enumerate((wop, wol)):
        turned = lax.dot_general(eye, w[...], NT, preferred_element_type=F32)
        wout[z, x, c, :, k * CH : (k + 1) * CH] = turned.astype(BF16)

    pl.semaphore_wait(barrier, len(peers))
    for load in loads[:3]:
        load.wait()

    halves = (pl.ds(0, TOK // 2), pl.ds(TOK // 2, TOK // 2))
    t1 = {(d, h): links.slot() for d in (1, -1) for h in (0, 1)}
    t2 = {d: links.slot() for d in (1, -1)}
    for i in (0, 1):
        for d in (1, -1):
            h = i if d == 1 else 1 - i
            piece = tok.at[y, halves[h]]
            links.put(piece, piece, t1[d, h], tp=yy(d))
    w_in = weight_gather(links, win, z, x, c)
    w_out = weight_gather(links, wout, z, x, c)
    w_in[0]()

    def token_relay():
        for d, h in ((1, 0), (-1, 1)):
            piece = tok.at[yy(-d), halves[h]]
            links.got(piece, t1[d, h], tp=yy(d))
            links.put(piece, piece, t2[d], tp=yy(d))

    half = lax.shift_left(jnp.int32(1), y)
    grid_rows = TOK // GRID_W
    row_count = grid_rows * NZ * NX * NC
    first_row = s * grid_rows

    def boxes(i, _):
        at = pl.multiple_of(i * 32, 32)
        er = lax.shift_right_logical(lax.broadcasted_iota(jnp.int32, (32, EXT), 1), 5)
        ec = lax.broadcasted_iota(jnp.int32, (32, EXT), 1) & (GRID_W - 1)
        col = lax.broadcasted_iota(jnp.int32, (32, EXT), 0)
        low = jnp.maximum(i - half, -first_row) + REACH
        high = jnp.minimum(i + half, row_count - first_row) + REACH
        inside = (er >= low) & (er < high) & (ec >= col - half) & (ec < col + half)
        box[pl.ds(at, 32), :] = jnp.where(inside, 1.0, 0.0).astype(BF16)
        cc = lax.broadcasted_iota(jnp.int32, (32, 128), 0)
        cols = jnp.minimum(cc + half, GRID_W) - jnp.maximum(cc - half, 0)
        rcp[pl.ds(at, 32), :] = 1.0 / (cols * (high - low)).astype(F32)
        return 0

    lax.fori_loop(0, grid_rows, boxes, 0)

    w_in[1]()
    w_in[2]()
    token_relay()
    for step in w_in[3:7]:
        step()
    w_out[0]()
    for d, h in ((1, 1), (-1, 0)):
        links.got(tok.at[yy(-d), halves[h]], t1[d, h], tp=yy(d))
    for d, h in ((1, 0), (-1, 1)):
        links.got(tok.at[yy(2), halves[h]], t2[d], tp=yy(d))

    def norm(i, _):
        rows = pl.ds(pl.multiple_of(i * 32, 32), 32)
        total = jnp.zeros((32, 1), F32)
        for k in range(NY):
            v = tok[k, rows, :].astype(F32)
            total = total + jnp.sum(v * v, axis=1, keepdims=True)
        scale = lax.rsqrt(total * (1.0 / D) + EPS)
        for k in range(NY):
            cols = slice(k * CH, (k + 1) * CH)
            v = tok[k, rows, :].astype(F32)
            nrm[rows, cols] = (v * scale * gain[:, cols]).astype(BF16)
        return 0

    lax.fori_loop(0, TOK // 32, norm, 0)
    w_in[7]()
    w_out[1]()

    def project(col):
        w = win[:, :, :, :, col : col + 256].reshape(D, 256)
        return jnp.dot(nrm[...], w, preferred_element_type=F32).astype(BF16)

    for n in range(2):
        u = project(CH + n * 256)
        ulb[:, n * 256 : (n + 1) * 256] = u
        for k in range(2):
            ulf[2 * n + k, PAD : PAD + TOK, :] = u[:, k * 128 : (k + 1) * 128].astype(F32)
    ch = {d: links.slot() for d in (1, -1)}
    links.put(ulb.at[pl.ds(TOK - PAD, PAD)], hb.at[0], ch[1], **after)
    links.put(ulb.at[pl.ds(0, PAD)], hb.at[1], ch[-1], **before)
    for n in range(2):
        pext[OWN : OWN + TOK, n * 256 : (n + 1) * 256] = project(n * 256)
    ph = {d: links.slot() for d in (1, -1)}
    links.put(pext.at[pl.ds(TOK, OWN)], pext.at[pl.ds(0, OWN)], ph[1], **after)
    links.put(pext.at[pl.ds(OWN, OWN)], pext.at[pl.ds(OWN + TOK, OWN)], ph[-1], **before)
    w_out[2]()

    links.got(hb.at[0], ch[1], **after)
    links.got(hb.at[1], ch[-1], **before)
    has_before = jnp.where(s > 0, 1.0, 0.0).astype(F32)
    has_after = jnp.where(s < NZ * NX * NC - 1, 1.0, 0.0).astype(F32)
    for b in range(4):
        lanes = slice(b * 128, (b + 1) * 128)
        ulf[b, 0:PAD, :] = hb[0, :, lanes].astype(F32) * has_before
        ulf[b, PAD + TOK :, :] = hb[1, :, lanes].astype(F32) * has_after
    for load in loads[4:6]:
        load.wait()

    def block(b):
        lanes = slice(b * 128, (b + 1) * 128)
        tap = taps[:, lanes].astype(F32)
        acc = ulf[b, PAD - 2 : PAD - 2 + TOK, :] * tap[0:1]
        for k in range(1, 4):
            acc = acc + ulf[b, PAD - 2 + k : PAD - 2 + k + TOK, :] * tap[k : k + 1]
        conv = acc.astype(BF16)
        cvb[...] = conv.astype(F32)
        for d in range(2):
            gs[2 * d] = jnp.dot(conv, rgv[d, b], preferred_element_type=F32)
            gs[2 * d + 1] = jnp.dot(conv, igv[d, b], preferred_element_type=F32)

        def rows_of(i, _):
            rows = pl.ds(pl.multiple_of(i * 32, 32), 32)
            value = cvb[rows, :]
            for d in range(2):
                rate = logistic(gs[2 * d, rows, :])
                gate = logistic(gs[2 * d + 1, rows, :])
                keep_log = -8.0 * rate * decay[d : d + 1, lanes] + logd[d, rows, :]
                keep = jnp.exp(keep_log)
                rest = one_minus_exp(2.0 * keep_log, keep * keep)
                aa[d, b, rows, :] = keep
                bb[d, b, rows, :] = jnp.sqrt(rest) * gate * value
            return 0

        lax.fori_loop(0, TOK // 32, rows_of, 0)

    block(0)
    w_out[3]()
    block(1)
    block(2)
    w_out[4]()
    block(3)

    def scan_step(t, carry):
        new = []
        for d in range(2):
            at = pl.ds(t if d == 0 else SEG - 1 - t, SEGS, stride=SEG)
            for b in range(4):
                prod, state = carry[2 * (4 * d + b)], carry[2 * (4 * d + b) + 1]
                keep = aa[d, b, at, :]
                state = keep * state + bb[d, b, at, :]
                prod = prod * keep
                aa[d, b, at, :] = prod
                bb[d, b, at, :] = state
                new += [prod, state]
        return tuple(new)

    ones, zeros = jnp.ones((SEGS, 128), F32), jnp.zeros((SEGS, 128), F32)
    ends = lax.fori_loop(0, SEG, scan_step, (ones, zeros) * 8, unroll=2)
    for d in range(2):
        for b in range(4):
            for k in range(2):
                sg[k, d, :, b * 128 : (b + 1) * 128] = ends[2 * (4 * d + b) + k]
    me = x * NC + c
    for d in range(2):
        prod, state = jnp.ones((1, CH), F32), jnp.zeros((1, CH), F32)
        for j in range(SEGS) if d == 0 else reversed(range(SEGS)):
            ex[0, d, j : j + 1, :] = prod
            ex[1, d, j : j + 1, :] = state
            keep = sg[0, d, j : j + 1, :]
            state = keep * state + sg[1, d, j : j + 1, :]
            prod = prod * keep
        c1[me, 2 * d : 2 * d + 1, :] = prod
        c1[me, 2 * d + 1 : 2 * d + 2, :] = state
    k1 = {p: links.slot() for p in around}
    for dx, dc in around:
        links.put(
            c1.at[me], c1.at[me], k1[dx, dc], sp_1=xx(dx), sp_2=lax.rem(c + dc, NC)
        )
    w_out[5]()

    loads[3].wait()
    links.got(pext.at[pl.ds(0, OWN)], ph[1], **after)
    links.got(pext.at[pl.ds(OWN + TOK, OWN)], ph[-1], **before)

    def combine(table, mine):
        full, inside = [], []
        for d in range(2):
            count = NZ
            prod, state = jnp.ones((1, CH), F32), jnp.zeros((1, CH), F32)
            in_p, in_s = prod, state
            for k in range(count) if d == 0 else reversed(range(count)):
                keep = table[k, 2 * d : 2 * d + 1, :]
                state = keep * state + table[k, 2 * d + 1 : 2 * d + 2, :]
                prod = prod * keep
                passed = (k < mine) if d == 0 else (k > mine)
                in_p = jnp.where(passed, prod, in_p)
                in_s = jnp.where(passed, state, in_s)
            full.append((prod, state))
            inside.append((in_p, in_s))
        return full, inside

    def pooled(n):
        cols = slice(n * 256, (n + 1) * 256)
        total = jnp.dot(box[...], pext[:, cols], preferred_element_type=F32)
        own = pext[OWN : OWN + TOK, cols].astype(F32)
        scale = jnp.concatenate([rcp[...], rcp[...]], axis=1)
        pdf[:, cols] = (total * scale - own).astype(BF16)

    for n in range(2):
        pooled(n)

    for dx, dc in around:
        links.got(
            c1.at[xx(-dx) * NC + lax.rem(c + dc, NC)],
            k1[dx, dc],
            sp_1=xx(dx),
            sp_2=lax.rem(c + dc, NC),
        )
    full, near = combine(c1, me)
    for d in range(2):
        c2[z, 2 * d : 2 * d + 1, :] = full[d][0]
        c2[z, 2 * d + 1 : 2 * d + 2, :] = full[d][1]
    k2 = {d: links.slot() for d in range(1, NZ)}
    for d in range(1, NZ):
        links.put(c2.at[z], c2.at[z], k2[d], sp_0=zz(d))
    w_out[6]()

    for n in range(2):
        cols = slice(n * 256, (n + 1) * 256)
        ycat[:, cols] = jnp.dot(pdf[...], pmv[0, :, cols], preferred_element_type=F32).astype(BF16)

    for d in range(1, NZ):
        links.got(c2.at[zz(-d)], k2[d], sp_0=zz(d))
    _, far = combine(c2, z)
    for d in range(2):
        (np_, ns_), (fp_, fs_) = near[d], far[d]
        enter = np_ * fs_ + ns_ + (np_ * fp_) * start[d : d + 1, :]
        ex[0, d] = ex[1, d] + ex[0, d] * enter
    for j in range(SEGS):
        rows = slice(j * SEG, (j + 1) * SEG)
        for b in range(4):
            lanes = slice(b * 128, (b + 1) * 128)
            h0 = bb[0, b, rows, :] + aa[0, b, rows, :] * ex[0, 0, j : j + 1, lanes]
            h1 = bb[1, b, rows, :] + aa[1, b, rows, :] * ex[0, 1, j : j + 1, lanes]
            ycat[rows, CH + b * 128 : CH + (b + 1) * 128] = (h0 + h1).astype(BF16)
    w_out[7]()

    q1 = [links.slot() for _ in range(NZ)]
    q2 = [links.slot() for _ in range(NZ)]
    q3 = [links.slot() for _ in range(NZ)]

    def relay(n):
        cols = slice(n * 256, (n + 1) * 256)
        d = 1 if n % 2 == 0 else -1
        at = rs2.at[:, pl.ds(n * 256, 256)]
        links.got(at, q2[n], tp=yy(d))
        mg[:, cols] = (rs2[:, cols].astype(F32) + part[yy(d), :, cols].astype(F32)).astype(BF16)
        there = pl.ds(n * 256, 256)
        links.put(mg.at[:, there], rs3.at[:, there], q3[n], tp=yy(d))

    for n in range(NZ):
        cols = slice(n * 256, (n + 1) * 256)
        there = pl.ds(n * 256, 256)
        w = wout[n].reshape(256, 2 * CH)
        acc = lax.dot_general(ycat[...], w, NT, preferred_element_type=F32)
        for k in range(NY):
            part[k, :, cols] = acc[k * OUT_ROWS : (k + 1) * OUT_ROWS].astype(BF16)
        d = 1 if n % 2 == 0 else -1
        links.put(part.at[yy(2), :, there], rs2.at[:, there], q2[n], tp=yy(d))
        links.put(part.at[yy(-d), :, there], rs1.at[:, there], q1[n], tp=yy(-d))
        if n >= 2:
            relay(n - 2)
    relay(NZ - 2)
    relay(NZ - 1)
    for n in range(NZ):
        cols = slice(n * 256, (n + 1) * 256)
        there = pl.ds(n * 256, 256)
        d = 1 if n % 2 == 0 else -1
        links.got(rs1.at[:, there], q1[n], tp=yy(-d))
        links.got(rs3.at[:, there], q3[n], tp=yy(d))
        total = part[y, :, cols].astype(F32) + rs1[:, cols].astype(F32) + rs3[:, cols].astype(F32)
        out[:, cols] = total.astype(BF16)
    links.drain()


def per_device(
    tokens, norm_gain, w_pool_in, w_lru_in, pool_mix, conv_taps, rec_gate, in_gate, decay_rate,
    log_decay, start_state, w_out_pool, w_out_lru,
):
    spread = jnp.broadcast_to(log_decay[:, :, None], (2, TOK, 128))
    anywhere = pl.BlockSpec(memory_space=pl.ANY)
    near = pl.BlockSpec(memory_space=pltpu.VMEM)
    buf = pltpu.VMEM
    return pl.pallas_call(
        layer,
        out_shape=jax.ShapeDtypeStruct((OUT_ROWS, D), BF16),
        in_specs=[
            anywhere, near, anywhere, anywhere, anywhere, near, anywhere, anywhere, near, near,
            near, near, near,
        ],
        out_specs=near,
        scratch_shapes=[
            buf((NY, TOK, CH), BF16),
            buf((TOK, D), BF16),
            buf((NZ, NX, NC, 32, 2 * CH), BF16),
            buf((NZ, NX, NC, 32, 2 * CH), BF16),
            buf((1, CH, CH), BF16),
            buf((2, 4, 128, 128), BF16),
            buf((2, 4, 128, 128), BF16),
            buf((TOK, EXT), BF16),
            buf((TOK, 128), F32),
            buf((TOK, CH), BF16),
            buf((4, TOK + 2 * PAD, 128), F32),
            buf((2, PAD, CH), BF16),
            buf((TOK, 128), F32),
            buf((EXT, CH), BF16),
            buf((TOK, CH), BF16),
            buf((4, TOK, 128), F32),
            buf((2, 4, TOK, 128), F32),
            buf((2, 4, TOK, 128), F32),
            buf((2, 2, SEGS, CH), F32),
            buf((2, 2, SEGS, CH), F32),
            buf((NX * NC, 4, CH), F32),
            buf((NZ, 4, CH), F32),
            buf((TOK, 2 * CH), BF16),
            buf((NY, OUT_ROWS, D), BF16),
            buf((OUT_ROWS, D), BF16),
            buf((OUT_ROWS, D), BF16),
            buf((OUT_ROWS, D), BF16),
            buf((OUT_ROWS, D), BF16),
            pltpu.SemaphoreType.DMA((N_DMA,)),
            pltpu.SemaphoreType.DMA((N_DMA,)),
            pltpu.SemaphoreType.DMA((N_LOCAL,)),
        ],
        compiler_params=pltpu.CompilerParams(
            collective_id=0, has_side_effects=True, vmem_limit_bytes=60 * 1024 * 1024
        ),
        name="layer",
    )(
        tokens, norm_gain.reshape(1, D), w_pool_in, w_lru_in, pool_mix, conv_taps, rec_gate,
        in_gate, decay_rate, spread, start_state, w_out_pool, w_out_lru,
    )


def solution(mesh):
    torus = Mesh(mesh.devices.reshape(NZ, NX, NC, mesh.shape["tp"]), SP_TP)
    in_specs = (
        P(SP, "tp"),
        P(),
        P(SP, "tp"),
        P(SP, "tp"),
        P("tp", None, None),
        P(None, "tp"),
        P(None, "tp", None, None),
        P(None, "tp", None, None),
        P(None, "tp"),
        P(None, SP),
        P(None, "tp"),
        P("tp", SP),
        P("tp", SP),
    )
    return jax.shard_map(
        per_device, mesh=torus, in_specs=in_specs, out_specs=P(SP_TP, None), check_vma=False
    )
```

```python
import functools

import jax
import jax.numpy as jnp
from jax import lax
from jax.experimental import pallas as pl
from jax.experimental.pallas import tpu as pltpu
from jax.sharding import Mesh
from jax.sharding import PartitionSpec as P

GRID_W = 32
REACH = 8
EPS = 1e-06
SP = ("sp_0", "sp_1", "sp_2")
SP_TP = ("sp_0", "sp_1", "sp_2", "tp")
NZ, NX, NC, NY = 8, 4, 2, 4
TOK = 384
D = 2048
CH = 512
SEGS = 8
SEG = TOK // SEGS
OWN = REACH * GRID_W
EXT = TOK + 2 * OWN
PAD = 16
OUT_ROWS = TOK // NY
N_DMA = 192
N_LOCAL = 8
F32 = jnp.float32
BF16 = jnp.bfloat16
NT = (((1,), (1,)), ((), ()))


class Links:
    def __init__(self, send, recv):
        self.send, self.recv, self.used, self.sent = send, recv, 0, []

    def slot(self):
        self.used += 1
        return self.used - 1

    def put(self, src, dst, slot, **dev):
        copy = pltpu.make_async_remote_copy(
            src_ref=src,
            dst_ref=dst,
            send_sem=self.send.at[slot],
            recv_sem=self.recv.at[slot],
            device_id=dev,
            device_id_type=pl.DeviceIdType.MESH,
        )
        copy.start()
        self.sent.append(copy)

    def got(self, region, slot, **dev):
        pltpu.make_async_remote_copy(
            src_ref=region,
            dst_ref=region,
            send_sem=self.send.at[slot],
            recv_sem=self.recv.at[slot],
            device_id=dev,
            device_id_type=pl.DeviceIdType.MESH,
        ).wait_recv()

    def drain(self):
        for copy in self.sent:
            copy.wait_send()


def weight_gather(links, buf, z, x, c):
    lo, hi = pl.ds(0, 16), pl.ds(16, 16)

    def zz(d):
        return lax.rem(z + (d + NZ), NZ)

    def xx(d):
        return lax.rem(x + (d + NX), NX)

    other = {"sp_2": 1 - c}
    both = (1, -1)
    rel = [0, -1, 1, -2, 2, -3, 3, 4]
    a1 = {dx: links.slot() for dx in (1, 3, 2)}
    a2 = {
        (s, k, e): links.slot()
        for s in both
        for e in range(NX)
        for k in range(1, 5 if (s == 1) == (e < 2) else 4)
    }
    b1 = {(s, k): links.slot() for s in both for k in range(1, 5 if s == 1 else 4)}
    b2 = {(d, s): links.slot() for d in rel for s in both}
    b3 = {d: links.slot() for d in rel}
    dd = {d: links.slot() for d in rel}

    def a_send(s, k, e):
        if (s, k, e) in a2:
            piece = buf.at[zz(-s * (k - 1)), xx(e), c, lo]
            links.put(piece, piece, a2[s, k, e], sp_0=zz(s))

    def a_hop(s, k, e):
        if (s, k, e) in a2:
            links.got(buf.at[zz(-s * k), xx(e), c, lo], a2[s, k, e], sp_0=zz(s))
            a_send(s, k + 1, e)

    def a_side(dx):
        links.got(buf.at[z, xx(-dx), c, lo], a1[dx], sp_1=xx(dx))
        for s in both:
            a_send(s, 1, NX - dx)

    def b_send(s, k):
        if (s, k) in b1:
            piece = buf.at[zz(-s * (k - 1)), x, c, hi]
            links.put(piece, piece, b1[s, k], sp_0=zz(s))

    def b_spread(d):
        piece = buf.at[zz(d), x, c, hi]
        for s in both:
            links.put(piece, piece, b2[d, s], sp_1=xx(s))

    def b_hop(s, k):
        if (s, k) in b1:
            links.got(buf.at[zz(-s * k), x, c, hi], b1[s, k], sp_0=zz(s))
            b_send(s, k + 1)
            b_spread(-s * k if k < 4 else 4)

    def b_relay(d):
        for s in both:
            piece = buf.at[zz(d), xx(-s), c, hi]
            links.got(piece, b2[d, s], sp_1=xx(s))
            if (d % 2 == 0) == (s == 1):
                links.put(piece, piece, b3[d], sp_1=xx(s))

    def row_done(d):
        s = 1 if d % 2 == 0 else -1
        links.got(buf.at[zz(d), xx(2), c, hi], b3[d], sp_1=xx(s))
        row = buf.at[zz(d), pl.ds(0, NX), c]
        links.put(row, row, dd[d], **other)

    def first():
        own = buf.at[z, x, c, lo]
        for dx in (1, 3, 2):
            links.put(own, own, a1[dx], sp_1=xx(dx))
        for s in both:
            b_send(s, 1)
            a_send(s, 1, 0)
        b_spread(0)

    def arrived():
        for d in rel:
            links.got(buf.at[zz(d), pl.ds(0, NX), 1 - c], dd[d], **other)

    def at(f, *args):
        return functools.partial(f, *args)

    rounds = [[first]]
    rounds.append(
        [at(a_side, 1), at(a_side, 3)]
        + [at(b_hop, s, 1) for s in both]
        + [at(a_hop, s, 1, 0) for s in both]
        + [at(a_side, 2), at(b_relay, 0)]
    )
    for k in (2, 3, 4, 5):
        turn = [at(b_hop, s, k) for s in both] + [at(a_hop, s, k, 0) for s in both]
        turn += [at(a_hop, s, k - 1, e) for e in (3, 1, 2) for s in both]
        turn += [at(b_relay, d) for d in ((1 - k, k - 1) if k < 5 else (4,))]
        turn += [at(row_done, d) for d in ((0,) if k == 2 else (2 - k, k - 2))]
        rounds.append(turn)
    rounds.append([at(row_done, 4)])
    return rounds, arrived


def logistic(v):
    return 1.0 / (1.0 + jnp.exp(-v))


def one_minus_exp(y, e):
    series = y * (-1.0 / 720.0) - 1.0 / 120.0
    for n in (24.0, 6.0, 2.0, 1.0):
        series = y * series - 1.0 / n
    return jnp.where(y > -0.125, y * series, 1.0 - e)


def root(v):
    return v * lax.rsqrt(jnp.maximum(v, 1e-37))


def layer(
    tokens, gain, wpi, wli, pmix, taps, rgate, igate, decay, logd, start, wop, wol, out,
    tok, nrm, win, wout, pmv, rgv, igv, ldb, box, rcp, ulb, ulf, hb, cvb, pext, pdf, gs, aa, bb,
    sg, ex, c1, c2, ycat, part, rs1, rs2, rs3, mg, send, recv, local,
):
    z, x, c = (lax.axis_index(n) for n in SP)
    y = lax.axis_index("tp")
    s = (z * NX + x) * NC + c
    links = Links(send, recv)

    def zz(d):
        return lax.rem(z + (d + NZ), NZ)

    def xx(d):
        return lax.rem(x + (d + NX), NX)

    def yy(d):
        return lax.rem(y + (d + NY), NY)

    def run_dev(d):
        t = lax.rem(s + (d + NZ * NX * NC), NZ * NX * NC)
        return {"sp_0": t // (NX * NC), "sp_1": lax.rem(t // NC, NX), "sp_2": lax.rem(t, NC)}

    after, before = run_dev(1), run_dev(-1)

    loads = [
        pltpu.make_async_copy(tokens, tok.at[y], local.at[0]),
        pltpu.make_async_copy(wpi, win.at[z, x, c, :, pl.ds(0, CH)], local.at[1]),
        pltpu.make_async_copy(wli, win.at[z, x, c, :, pl.ds(CH, CH)], local.at[2]),
        pltpu.make_async_copy(pmix, pmv, local.at[3]),
        pltpu.make_async_copy(rgate, rgv, local.at[4]),
        pltpu.make_async_copy(igate, igv, local.at[5]),
        pltpu.make_async_copy(wop, wout.at[z, x, c, :, pl.ds(0, CH)], local.at[6]),
        pltpu.make_async_copy(wol, wout.at[z, x, c, :, pl.ds(CH, CH)], local.at[7]),
    ]
    for load in loads:
        load.start()

    barrier = pltpu.get_barrier_semaphore()
    peers = [{"tp": yy(1)}, {"tp": yy(-1)}, after, before]
    peers += [{"sp_0": zz(d)} for d in range(1, NZ)]
    around = [(dx, dc) for dx in range(NX) for dc in range(NC) if dx or dc]
    for dx, dc in around:
        peers.append({"sp_1": xx(dx), "sp_2": lax.rem(c + dc, NC)})
    for peer in peers:
        pl.semaphore_signal(barrier, inc=1, device_id=peer, device_id_type=pl.DeviceIdType.MESH)

    for d in range(2):
        for i in range(TOK // 128):
            rows = slice(i * 128, (i + 1) * 128)
            ldb[d, rows, :] = jnp.broadcast_to(logd[d : d + 1, rows], (128, 128)).T
    half = lax.shift_left(jnp.int32(1), y)
    grid_rows = TOK // GRID_W
    row_count = grid_rows * NZ * NX * NC
    first_row = s * grid_rows

    def boxes(i, _):
        at = pl.multiple_of(i * 32, 32)
        er = lax.shift_right_logical(lax.broadcasted_iota(jnp.int32, (32, EXT), 1), 5)
        ec = lax.broadcasted_iota(jnp.int32, (32, EXT), 1) & (GRID_W - 1)
        col = lax.broadcasted_iota(jnp.int32, (32, EXT), 0)
        low = jnp.maximum(i - half, -first_row) + REACH
        high = jnp.minimum(i + half, row_count - first_row) + REACH
        inside = (er >= low) & (er < high) & (ec >= col - half) & (ec < col + half)
        box[pl.ds(at, 32), :] = jnp.where(inside, 1.0, 0.0).astype(BF16)
        cc = lax.broadcasted_iota(jnp.int32, (32, 128), 0)
        cols = jnp.minimum(cc + half, GRID_W) - jnp.maximum(cc - half, 0)
        rcp[pl.ds(at, 32), :] = 1.0 / (cols * (high - low)).astype(F32)
        return 0

    lax.fori_loop(0, grid_rows, boxes, 0)

    pl.semaphore_wait(barrier, len(peers))
    for load in loads[:3]:
        load.wait()

    halves = (pl.ds(0, TOK // 2), pl.ds(TOK // 2, TOK // 2))
    t1 = {(d, h): links.slot() for d in (1, -1) for h in (0, 1)}
    t2 = {d: links.slot() for d in (1, -1)}
    for i in (0, 1):
        for d in (1, -1):
            h = i if d == 1 else 1 - i
            piece = tok.at[y, halves[h]]
            links.put(piece, piece, t1[d, h], tp=yy(d))
    r_in, in_arrived = weight_gather(links, win, z, x, c)
    r_out, out_arrived = weight_gather(links, wout, z, x, c)

    def serve(*rounds):
        for turn in rounds:
            for step in turn:
                step()

    serve(r_in[0])

    def token_relay():
        for d, h in ((1, 0), (-1, 1)):
            piece = tok.at[yy(-d), halves[h]]
            links.got(piece, t1[d, h], tp=yy(d))
            links.put(piece, piece, t2[d], tp=yy(d))

    serve(r_in[1])
    serve(r_in[2])
    token_relay()
    serve(r_in[3], r_in[4])
    for load in loads[6:8]:
        load.wait()
    serve(r_out[0])
    serve(r_in[5], r_in[6])
    for d, h in ((1, 1), (-1, 0)):
        links.got(tok.at[yy(-d), halves[h]], t1[d, h], tp=yy(d))
    for d, h in ((1, 0), (-1, 1)):
        links.got(tok.at[yy(2), halves[h]], t2[d], tp=yy(d))

    def norm(i, _):
        rows = pl.ds(pl.multiple_of(i * 32, 32), 32)
        total = jnp.zeros((32, 1), F32)
        for k in range(NY):
            v = tok[k, rows, :].astype(F32)
            total = total + jnp.sum(v * v, axis=1, keepdims=True)
        scale = lax.rsqrt(total * (1.0 / D) + EPS)
        for k in range(NY):
            cols = slice(k * CH, (k + 1) * CH)
            v = tok[k, rows, :].astype(F32)
            nrm[rows, cols] = (v * scale * gain[:, cols]).astype(BF16)
        return 0

    lax.fori_loop(0, TOK // 32, norm, 0)
    in_arrived()
    serve(r_out[1])

    def project(col):
        w = win[:, :, :, :, col : col + 256].reshape(D, 256)
        return jnp.dot(nrm[...], w, preferred_element_type=F32).astype(BF16)

    for n in range(2):
        u = project(CH + n * 256)
        ulb[:, n * 256 : (n + 1) * 256] = u
        for k in range(2):
            ulf[2 * n + k, PAD : PAD + TOK, :] = u[:, k * 128 : (k + 1) * 128].astype(F32)
    ch = {d: links.slot() for d in (1, -1)}
    links.put(ulb.at[pl.ds(TOK - PAD, PAD)], hb.at[0], ch[1], **after)
    links.put(ulb.at[pl.ds(0, PAD)], hb.at[1], ch[-1], **before)
    for n in range(2):
        pext[OWN : OWN + TOK, n * 256 : (n + 1) * 256] = project(n * 256)
    ph = {d: links.slot() for d in (1, -1)}
    links.put(pext.at[pl.ds(TOK, OWN)], pext.at[pl.ds(0, OWN)], ph[1], **after)
    links.put(pext.at[pl.ds(OWN, OWN)], pext.at[pl.ds(OWN + TOK, OWN)], ph[-1], **before)

    links.got(hb.at[0], ch[1], **after)
    links.got(hb.at[1], ch[-1], **before)
    has_before = jnp.where(s > 0, 1.0, 0.0).astype(F32)
    has_after = jnp.where(s < NZ * NX * NC - 1, 1.0, 0.0).astype(F32)
    for b in range(4):
        lanes = slice(b * 128, (b + 1) * 128)
        ulf[b, 0:PAD, :] = hb[0, :, lanes].astype(F32) * has_before
        ulf[b, PAD + TOK :, :] = hb[1, :, lanes].astype(F32) * has_after
    for load in loads[4:6]:
        load.wait()

    def block(b):
        lanes = slice(b * 128, (b + 1) * 128)
        tap = taps[:, lanes].astype(F32)
        acc = ulf[b, PAD - 2 : PAD - 2 + TOK, :] * tap[0:1]
        for k in range(1, 4):
            acc = acc + ulf[b, PAD - 2 + k : PAD - 2 + k + TOK, :] * tap[k : k + 1]
        conv = acc.astype(BF16)
        cvb[...] = conv.astype(F32)
        for d in range(2):
            gs[2 * d] = jnp.dot(conv, rgv[d, b], preferred_element_type=F32)
            gs[2 * d + 1] = jnp.dot(conv, igv[d, b], preferred_element_type=F32)

        def rows_of(i, _):
            rows = pl.ds(pl.multiple_of(i * 32, 32), 32)
            value = cvb[rows, :]
            for d in range(2):
                rate = logistic(gs[2 * d, rows, :])
                gate = logistic(gs[2 * d + 1, rows, :])
                keep_log = -8.0 * rate * decay[d : d + 1, lanes] + ldb[d, rows, :]
                keep = jnp.exp(keep_log)
                rest = one_minus_exp(2.0 * keep_log, keep * keep)
                aa[d, b, rows, :] = keep
                bb[d, b, rows, :] = root(rest) * gate * value
            return 0

        lax.fori_loop(0, TOK // 32, rows_of, 0)

    block(0)
    serve(r_out[2][:6])
    block(1)
    serve(r_out[2][6:])
    block(2)
    serve(r_out[3][:6])
    block(3)

    def scan_step(t, carry):
        new = []
        for d in range(2):
            at = pl.ds(t if d == 0 else SEG - 1 - t, SEGS, stride=SEG)
            for b in range(4):
                prod, state = carry[2 * (4 * d + b)], carry[2 * (4 * d + b) + 1]
                keep = aa[d, b, at, :]
                state = keep * state + bb[d, b, at, :]
                prod = prod * keep
                aa[d, b, at, :] = prod
                bb[d, b, at, :] = state
                new += [prod, state]
        return tuple(new)

    serve(r_out[3][6:])
    ones, zeros = jnp.ones((SEGS, 128), F32), jnp.zeros((SEGS, 128), F32)
    ends = lax.fori_loop(0, SEG, scan_step, (ones, zeros) * 8, unroll=2)
    for d in range(2):
        for b in range(4):
            for k in range(2):
                sg[k, d, :, b * 128 : (b + 1) * 128] = ends[2 * (4 * d + b) + k]
    me = x * NC + c
    for d in range(2):
        prod, state = jnp.ones((1, CH), F32), jnp.zeros((1, CH), F32)
        for j in range(SEGS) if d == 0 else reversed(range(SEGS)):
            ex[0, d, j : j + 1, :] = prod
            ex[1, d, j : j + 1, :] = state
            keep = sg[0, d, j : j + 1, :]
            state = keep * state + sg[1, d, j : j + 1, :]
            prod = prod * keep
        c1[me, 2 * d : 2 * d + 1, :] = prod
        c1[me, 2 * d + 1 : 2 * d + 2, :] = state
    k1 = {p: links.slot() for p in around}
    for dx, dc in around:
        links.put(
            c1.at[me], c1.at[me], k1[dx, dc], sp_1=xx(dx), sp_2=lax.rem(c + dc, NC)
        )
    serve(r_out[4])

    loads[3].wait()
    links.got(pext.at[pl.ds(0, OWN)], ph[1], **after)
    links.got(pext.at[pl.ds(OWN + TOK, OWN)], ph[-1], **before)

    def combine(table, mine):
        full, inside = [], []
        for d in range(2):
            count = NZ
            prod, state = jnp.ones((1, CH), F32), jnp.zeros((1, CH), F32)
            in_p, in_s = prod, state
            for k in range(count) if d == 0 else reversed(range(count)):
                keep = table[k, 2 * d : 2 * d + 1, :]
                state = keep * state + table[k, 2 * d + 1 : 2 * d + 2, :]
                prod = prod * keep
                passed = (k < mine) if d == 0 else (k > mine)
                in_p = jnp.where(passed, prod, in_p)
                in_s = jnp.where(passed, state, in_s)
            full.append((prod, state))
            inside.append((in_p, in_s))
        return full, inside

    def pooled(n):
        cols = slice(n * 256, (n + 1) * 256)
        total = jnp.dot(box[...], pext[:, cols], preferred_element_type=F32)
        own = pext[OWN : OWN + TOK, cols].astype(F32)
        scale = jnp.concatenate([rcp[...], rcp[...]], axis=1)
        pdf[:, cols] = (total * scale - own).astype(BF16)

    for n in range(2):
        pooled(n)

    for dx, dc in around:
        links.got(
            c1.at[xx(-dx) * NC + lax.rem(c + dc, NC)],
            k1[dx, dc],
            sp_1=xx(dx),
            sp_2=lax.rem(c + dc, NC),
        )
    full, near = combine(c1, me)
    for d in range(2):
        c2[z, 2 * d : 2 * d + 1, :] = full[d][0]
        c2[z, 2 * d + 1 : 2 * d + 2, :] = full[d][1]
    k2 = {d: links.slot() for d in range(1, NZ)}
    for d in range(1, NZ):
        links.put(c2.at[z], c2.at[z], k2[d], sp_0=zz(d))
    serve(r_out[5])

    for n in range(2):
        cols = slice(n * 256, (n + 1) * 256)
        ycat[:, cols] = jnp.dot(pdf[...], pmv[0, :, cols], preferred_element_type=F32).astype(BF16)

    serve(r_out[6])
    for d in range(1, NZ):
        links.got(c2.at[zz(-d)], k2[d], sp_0=zz(d))
    _, far = combine(c2, z)
    for d in range(2):
        (np_, ns_), (fp_, fs_) = near[d], far[d]
        enter = np_ * fs_ + ns_ + (np_ * fp_) * start[d : d + 1, :]
        ex[0, d] = ex[1, d] + ex[0, d] * enter
    for j in range(SEGS):
        rows = slice(j * SEG, (j + 1) * SEG)
        for b in range(4):
            lanes = slice(b * 128, (b + 1) * 128)
            h0 = bb[0, b, rows, :] + aa[0, b, rows, :] * ex[0, 0, j : j + 1, lanes]
            h1 = bb[1, b, rows, :] + aa[1, b, rows, :] * ex[0, 1, j : j + 1, lanes]
            ycat[rows, CH + b * 128 : CH + (b + 1) * 128] = (h0 + h1).astype(BF16)
    out_arrived()

    q1 = [links.slot() for _ in range(NZ)]
    q2 = [links.slot() for _ in range(NZ)]
    q3 = [links.slot() for _ in range(NZ)]

    def relay(n):
        cols = slice(n * 256, (n + 1) * 256)
        d = 1 if n % 2 == 0 else -1
        at = rs2.at[:, pl.ds(n * 256, 256)]
        links.got(at, q2[n], tp=yy(d))
        mg[:, cols] = (rs2[:, cols].astype(F32) + part[yy(d), :, cols].astype(F32)).astype(BF16)
        there = pl.ds(n * 256, 256)
        links.put(mg.at[:, there], rs3.at[:, there], q3[n], tp=yy(d))

    for n in range(NZ):
        cols = slice(n * 256, (n + 1) * 256)
        there = pl.ds(n * 256, 256)
        w = wout[n].reshape(256, 2 * CH)
        acc = lax.dot_general(ycat[...], w, NT, preferred_element_type=F32)
        for k in range(NY):
            part[k, :, cols] = acc[k * OUT_ROWS : (k + 1) * OUT_ROWS].astype(BF16)
        d = 1 if n % 2 == 0 else -1
        links.put(part.at[yy(2), :, there], rs2.at[:, there], q2[n], tp=yy(d))
        links.put(part.at[yy(-d), :, there], rs1.at[:, there], q1[n], tp=yy(-d))
        if n >= 2:
            relay(n - 2)
    relay(NZ - 2)
    relay(NZ - 1)
    for n in range(NZ):
        cols = slice(n * 256, (n + 1) * 256)
        there = pl.ds(n * 256, 256)
        d = 1 if n % 2 == 0 else -1
        links.got(rs1.at[:, there], q1[n], tp=yy(-d))
        links.got(rs3.at[:, there], q3[n], tp=yy(d))
        total = part[y, :, cols].astype(F32) + rs1[:, cols].astype(F32) + rs3[:, cols].astype(F32)
        out[:, cols] = total.astype(BF16)
    links.drain()


def per_device(
    tokens, norm_gain, w_pool_in, w_lru_in, pool_mix, conv_taps, rec_gate, in_gate, decay_rate,
    log_decay, start_state, w_out_pool, w_out_lru,
):
    anywhere = pl.BlockSpec(memory_space=pl.ANY)
    near = pl.BlockSpec(memory_space=pltpu.VMEM)
    buf = pltpu.VMEM
    return pl.pallas_call(
        layer,
        out_shape=jax.ShapeDtypeStruct((OUT_ROWS, D), BF16),
        in_specs=[
            anywhere, near, anywhere, anywhere, anywhere, near, anywhere, anywhere, near, near,
            near, anywhere, anywhere,
        ],
        out_specs=near,
        scratch_shapes=[
            buf((NY, TOK, CH), BF16),
            buf((TOK, D), BF16),
            buf((NZ, NX, NC, 32, 2 * CH), BF16),
            buf((NZ, NX, NC, 32, 2 * CH), BF16),
            buf((1, CH, CH), BF16),
            buf((2, 4, 128, 128), BF16),
            buf((2, 4, 128, 128), BF16),
            buf((2, TOK, 128), F32),
            buf((TOK, EXT), BF16),
            buf((TOK, 128), F32),
            buf((TOK, CH), BF16),
            buf((4, TOK + 2 * PAD, 128), F32),
            buf((2, PAD, CH), BF16),
            buf((TOK, 128), F32),
            buf((EXT, CH), BF16),
            buf((TOK, CH), BF16),
            buf((4, TOK, 128), F32),
            buf((2, 4, TOK, 128), F32),
            buf((2, 4, TOK, 128), F32),
            buf((2, 2, SEGS, CH), F32),
            buf((2, 2, SEGS, CH), F32),
            buf((NX * NC, 4, CH), F32),
            buf((NZ, 4, CH), F32),
            buf((TOK, 2 * CH), BF16),
            buf((NY, OUT_ROWS, D), BF16),
            buf((OUT_ROWS, D), BF16),
            buf((OUT_ROWS, D), BF16),
            buf((OUT_ROWS, D), BF16),
            buf((OUT_ROWS, D), BF16),
            pltpu.SemaphoreType.DMA((N_DMA,)),
            pltpu.SemaphoreType.DMA((N_DMA,)),
            pltpu.SemaphoreType.DMA((N_LOCAL,)),
        ],
        compiler_params=pltpu.CompilerParams(
            collective_id=0, has_side_effects=True, vmem_limit_bytes=60 * 1024 * 1024
        ),
        name="layer",
    )(
        tokens, norm_gain.reshape(1, D), w_pool_in, w_lru_in, pool_mix, conv_taps, rec_gate,
        in_gate, decay_rate, log_decay, start_state, w_out_pool.T, w_out_lru.T,
    )


def solution(mesh):
    torus = Mesh(mesh.devices.reshape(NZ, NX, NC, mesh.shape["tp"]), SP_TP)
    in_specs = (
        P(SP, "tp"),
        P(),
        P(SP, "tp"),
        P(SP, "tp"),
        P("tp", None, None),
        P(None, "tp"),
        P(None, "tp", None, None),
        P(None, "tp", None, None),
        P(None, "tp"),
        P(None, SP),
        P(None, "tp"),
        P("tp", SP),
        P("tp", SP),
    )
    return jax.shard_map(
        per_device, mesh=torus, in_specs=in_specs, out_specs=P(SP_TP, None), check_vma=False
    )
```

```python
import functools

import jax
import jax.numpy as jnp
from jax import lax
from jax.experimental import pallas as pl
from jax.experimental.pallas import tpu as pltpu
from jax.sharding import Mesh
from jax.sharding import PartitionSpec as P

GRID_W = 32
REACH = 8
EPS = 1e-06
SP = ("sp_0", "sp_1", "sp_2")
SP_TP = ("sp_0", "sp_1", "sp_2", "tp")
NZ, NX, NC, NY = 8, 4, 2, 4
TOK = 384
D = 2048
CH = 512
SEGS = 8
SEG = TOK // SEGS
OWN = REACH * GRID_W
EXT = TOK + 2 * OWN
PAD = 16
OUT_ROWS = TOK // NY
N_SEND = 19
N_RECV = 130
N_LOCAL = 8
F32 = jnp.float32
BF16 = jnp.bfloat16
NT = (((1,), (1,)), ((), ()))


class Links:
    def __init__(self, send, recv):
        self.send, self.recv, self.groups, self.used = send, recv, [], 0

    def slot(self):
        self.used += 1
        return self.used - 1

    def group(self, region):
        self.groups.append(region)
        return len(self.groups) - 1

    def copy(self, src, dst, group, slot, dev):
        return pltpu.make_async_remote_copy(
            src_ref=src,
            dst_ref=dst,
            send_sem=self.send.at[group],
            recv_sem=self.recv.at[slot],
            device_id=dev,
            device_id_type=pl.DeviceIdType.MESH,
        )

    def put(self, src, dst, group, slot, **dev):
        self.copy(src, dst, group, slot, dev).start()

    def got(self, region, slot, **dev):
        self.copy(region, region, 0, slot, dev).wait_recv()

    def drain(self, **dev):
        for group, region in enumerate(self.groups):
            self.copy(region, region, group, 0, dev).wait_send()


def weight_gather(links, buf, z, x, c):
    lo, hi = pl.ds(0, 16), pl.ds(16, 16)

    def zz(d):
        return lax.rem(z + (d + NZ), NZ)

    def xx(d):
        return lax.rem(x + (d + NX), NX)

    other = {"sp_2": 1 - c}
    both = (1, -1)
    rel = [0, -1, 1, -2, 2, -3, 3, 4]
    a1 = {dx: links.slot() for dx in (1, 3, 2)}
    a2 = {
        (s, k, e): links.slot()
        for s in both
        for e in range(NX)
        for k in range(1, 5 if (s == 1) == (e < 2) else 4)
    }
    b1 = {(s, k): links.slot() for s in both for k in range(1, 5 if s == 1 else 4)}
    b2 = {d: links.slot() for d in rel}
    dd = links.slot()
    g_a1 = links.group(buf.at[0, pl.ds(0, 3), c, lo])
    g_a2 = links.group(buf.at[pl.ds(0, 7), pl.ds(0, NX), c, lo])
    g_b1 = links.group(buf.at[pl.ds(0, 7), 0, c, lo])
    g_b2 = links.group(buf.at[pl.ds(0, NZ), pl.ds(0, 3), c, lo])
    g_dd = links.group(buf.at[pl.ds(0, NZ), pl.ds(0, NX), c])

    def a_send(s, k, e):
        if (s, k, e) in a2:
            piece = buf.at[zz(-s * (k - 1)), xx(e), c, lo]
            links.put(piece, piece, g_a2, a2[s, k, e], sp_0=zz(s))

    def a_hop(s, k, e):
        if (s, k, e) in a2:
            links.got(buf.at[zz(-s * k), xx(e), c, lo], a2[s, k, e], sp_0=zz(s))
            a_send(s, k + 1, e)

    def a_side(dx):
        links.got(buf.at[z, xx(-dx), c, lo], a1[dx], sp_1=xx(dx))
        for s in both:
            a_send(s, 1, NX - dx)

    def b_send(s, k):
        if (s, k) in b1:
            piece = buf.at[zz(-s * (k - 1)), x, c, hi]
            links.put(piece, piece, g_b1, b1[s, k], sp_0=zz(s))

    def b_spread(d):
        piece = buf.at[zz(d), x, c, hi]
        for dx in (1, 3, 2):
            links.put(piece, piece, g_b2, b2[d], sp_1=xx(dx))

    def b_hop(s, k):
        if (s, k) in b1:
            links.got(buf.at[zz(-s * k), x, c, hi], b1[s, k], sp_0=zz(s))
            b_send(s, k + 1)
            b_spread(-s * k if k < 4 else 4)

    def row_done(d):
        links.got(buf.at[zz(d), pl.ds(0, 3), c, hi], b2[d], sp_1=xx(1))
        row = buf.at[zz(d), pl.ds(0, NX), c]
        links.put(row, row, g_dd, dd, **other)

    def first():
        own = buf.at[z, x, c, lo]
        for dx in (1, 3, 2):
            links.put(own, own, g_a1, a1[dx], sp_1=xx(dx))
        for s in both:
            b_send(s, 1)
            a_send(s, 1, 0)

    def arrived():
        links.got(buf.at[pl.ds(0, NZ), pl.ds(0, NX), 1 - c], dd, **other)

    def at(f, *args):
        return functools.partial(f, *args)

    rounds = [[first, at(b_spread, 0)]]
    rounds.append(
        [at(a_side, 1), at(a_side, 3)]
        + [at(b_hop, s, 1) for s in both]
        + [at(a_hop, s, 1, 0) for s in both]
        + [at(a_side, 2)]
    )
    for k in (2, 3, 4, 5):
        turn = [at(b_hop, s, k) for s in both] + [at(a_hop, s, k, 0) for s in both]
        turn += [at(a_hop, s, k - 1, e) for e in (3, 1, 2) for s in both]
        turn += [at(row_done, d) for d in ((0,) if k == 2 else (2 - k, k - 2))]
        rounds.append(turn)
    rounds.append([at(row_done, 4)])
    return rounds, arrived


def logistic(v):
    return 1.0 / (1.0 + jnp.exp(-v))


def one_minus_exp(y, e):
    series = y * (-1.0 / 720.0) - 1.0 / 120.0
    for n in (24.0, 6.0, 2.0, 1.0):
        series = y * series - 1.0 / n
    return jnp.where(y > -0.125, y * series, 1.0 - e)


def root(v):
    return v * lax.rsqrt(jnp.maximum(v, 1e-37))


def layer(
    tokens, gain, wpi, wli, pmix, taps, rgate, igate, decay, logd, start, wop, wol, out,
    tok, nrm, win, wout, pmv, rgv, igv, ldb, box, rcp, ulb, ulf, hb, cvb, pext, pdf, gs, aa, bb,
    sg, ex, c1, c2, ycat, part, rs1, rs2, rs3, mg, send, recv, local,
):
    z, x, c = (lax.axis_index(n) for n in SP)
    y = lax.axis_index("tp")
    s = (z * NX + x) * NC + c
    links = Links(send, recv)

    def zz(d):
        return lax.rem(z + (d + NZ), NZ)

    def xx(d):
        return lax.rem(x + (d + NX), NX)

    def yy(d):
        return lax.rem(y + (d + NY), NY)

    def run_dev(d):
        t = lax.rem(s + (d + NZ * NX * NC), NZ * NX * NC)
        return {"sp_0": t // (NX * NC), "sp_1": lax.rem(t // NC, NX), "sp_2": lax.rem(t, NC)}

    after, before = run_dev(1), run_dev(-1)

    loads = [
        pltpu.make_async_copy(tokens, tok.at[y], local.at[0]),
        pltpu.make_async_copy(wpi, win.at[z, x, c, :, pl.ds(0, CH)], local.at[1]),
        pltpu.make_async_copy(wli, win.at[z, x, c, :, pl.ds(CH, CH)], local.at[2]),
        pltpu.make_async_copy(pmix, pmv, local.at[3]),
        pltpu.make_async_copy(rgate, rgv, local.at[4]),
        pltpu.make_async_copy(igate, igv, local.at[5]),
        pltpu.make_async_copy(wop, wout.at[z, x, c, :, pl.ds(0, CH)], local.at[6]),
        pltpu.make_async_copy(wol, wout.at[z, x, c, :, pl.ds(CH, CH)], local.at[7]),
    ]
    for load in loads:
        load.start()

    barrier = pltpu.get_barrier_semaphore()
    peers = [{"tp": yy(1)}, {"tp": yy(-1)}, after, before]
    peers += [{"sp_0": zz(d)} for d in range(1, NZ)]
    around = [(dx, dc) for dx in range(NX) for dc in range(NC) if dx or dc]
    for dx, dc in around:
        peers.append({"sp_1": xx(dx), "sp_2": lax.rem(c + dc, NC)})
    for peer in peers:
        pl.semaphore_signal(barrier, inc=1, device_id=peer, device_id_type=pl.DeviceIdType.MESH)

    for d in range(2):
        for i in range(TOK // 128):
            rows = slice(i * 128, (i + 1) * 128)
            ldb[d, rows, :] = jnp.broadcast_to(logd[d : d + 1, rows], (128, 128)).T
    half = lax.shift_left(jnp.int32(1), y)
    grid_rows = TOK // GRID_W
    row_count = grid_rows * NZ * NX * NC
    first_row = s * grid_rows

    def boxes(i, _):
        at = pl.multiple_of(i * 32, 32)
        er = lax.shift_right_logical(lax.broadcasted_iota(jnp.int32, (32, EXT), 1), 5)
        ec = lax.broadcasted_iota(jnp.int32, (32, EXT), 1) & (GRID_W - 1)
        col = lax.broadcasted_iota(jnp.int32, (32, EXT), 0)
        low = jnp.maximum(i - half, -first_row) + REACH
        high = jnp.minimum(i + half, row_count - first_row) + REACH
        inside = (er >= low) & (er < high) & (ec >= col - half) & (ec < col + half)
        box[pl.ds(at, 32), :] = jnp.where(inside, 1.0, 0.0).astype(BF16)
        cc = lax.broadcasted_iota(jnp.int32, (32, 128), 0)
        cols = jnp.minimum(cc + half, GRID_W) - jnp.maximum(cc - half, 0)
        rcp[pl.ds(at, 32), :] = 1.0 / (cols * (high - low)).astype(F32)
        return 0

    lax.fori_loop(0, grid_rows, boxes, 0)

    pl.semaphore_wait(barrier, len(peers))
    for load in loads[:3] + loads[6:]:
        load.wait()

    halves = (pl.ds(0, TOK // 2), pl.ds(TOK // 2, TOK // 2))
    g_t1 = links.group(tok.at[pl.ds(0, 2)])
    g_t2 = links.group(tok.at[0])
    t1 = {(d, h): links.slot() for d in (1, -1) for h in (0, 1)}
    t2 = {d: links.slot() for d in (1, -1)}
    for i in (0, 1):
        for d in (1, -1):
            h = i if d == 1 else 1 - i
            piece = tok.at[y, halves[h]]
            links.put(piece, piece, g_t1, t1[d, h], tp=yy(d))
    r_in, in_arrived = weight_gather(links, win, z, x, c)
    r_out, out_arrived = weight_gather(links, wout, z, x, c)

    def serve(*rounds):
        for turn in rounds:
            for step in turn:
                step()

    serve(r_in[0])
    serve(r_out[0][:1])

    def token_relay():
        for d, h in ((1, 0), (-1, 1)):
            piece = tok.at[yy(-d), halves[h]]
            links.got(piece, t1[d, h], tp=yy(d))
            links.put(piece, piece, g_t2, t2[d], tp=yy(d))

    serve(r_in[1])
    serve(r_in[2])
    token_relay()
    serve(r_out[0][1:])
    serve(r_in[3])
    serve(r_in[4])
    serve(r_out[1])
    serve(r_in[5], r_in[6])
    for d, h in ((1, 1), (-1, 0)):
        links.got(tok.at[yy(-d), halves[h]], t1[d, h], tp=yy(d))
    for d, h in ((1, 0), (-1, 1)):
        links.got(tok.at[yy(2), halves[h]], t2[d], tp=yy(d))

    def norm(i, _):
        rows = pl.ds(pl.multiple_of(i * 32, 32), 32)
        total = jnp.zeros((32, 1), F32)
        for k in range(NY):
            v = tok[k, rows, :].astype(F32)
            total = total + jnp.sum(v * v, axis=1, keepdims=True)
        scale = lax.rsqrt(total * (1.0 / D) + EPS)
        for k in range(NY):
            cols = slice(k * CH, (k + 1) * CH)
            v = tok[k, rows, :].astype(F32)
            nrm[rows, cols] = (v * scale * gain[:, cols]).astype(BF16)
        return 0

    lax.fori_loop(0, TOK // 32, norm, 0)
    serve(r_out[2])
    in_arrived()

    def project(col):
        w = win[:, :, :, :, col : col + 256].reshape(D, 256)
        return jnp.dot(nrm[...], w, preferred_element_type=F32).astype(BF16)

    for n in range(2):
        u = project(CH + n * 256)
        ulb[:, n * 256 : (n + 1) * 256] = u
        for k in range(2):
            ulf[2 * n + k, PAD : PAD + TOK, :] = u[:, k * 128 : (k + 1) * 128].astype(F32)
    g_ch = links.group(hb)
    ch = {d: links.slot() for d in (1, -1)}
    links.put(ulb.at[pl.ds(TOK - PAD, PAD)], hb.at[0], g_ch, ch[1], **after)
    links.put(ulb.at[pl.ds(0, PAD)], hb.at[1], g_ch, ch[-1], **before)
    for n in range(2):
        pext[OWN : OWN + TOK, n * 256 : (n + 1) * 256] = project(n * 256)
    g_ph = links.group(pext.at[pl.ds(0, 2 * OWN)])
    ph = {d: links.slot() for d in (1, -1)}
    links.put(pext.at[pl.ds(TOK, OWN)], pext.at[pl.ds(0, OWN)], g_ph, ph[1], **after)
    links.put(pext.at[pl.ds(OWN, OWN)], pext.at[pl.ds(OWN + TOK, OWN)], g_ph, ph[-1], **before)

    serve(r_out[3])
    links.got(hb.at[0], ch[1], **after)
    links.got(hb.at[1], ch[-1], **before)
    has_before = jnp.where(s > 0, 1.0, 0.0).astype(F32)
    has_after = jnp.where(s < NZ * NX * NC - 1, 1.0, 0.0).astype(F32)
    for b in range(4):
        lanes = slice(b * 128, (b + 1) * 128)
        ulf[b, 0:PAD, :] = hb[0, :, lanes].astype(F32) * has_before
        ulf[b, PAD + TOK :, :] = hb[1, :, lanes].astype(F32) * has_after
    for load in loads[4:6]:
        load.wait()

    def block(b):
        lanes = slice(b * 128, (b + 1) * 128)
        tap = taps[:, lanes].astype(F32)
        acc = ulf[b, PAD - 2 : PAD - 2 + TOK, :] * tap[0:1]
        for k in range(1, 4):
            acc = acc + ulf[b, PAD - 2 + k : PAD - 2 + k + TOK, :] * tap[k : k + 1]
        conv = acc.astype(BF16)
        cvb[...] = conv.astype(F32)
        for d in range(2):
            gs[2 * d] = jnp.dot(conv, rgv[d, b], preferred_element_type=F32)
            gs[2 * d + 1] = jnp.dot(conv, igv[d, b], preferred_element_type=F32)

        def rows_of(i, _):
            rows = pl.ds(pl.multiple_of(i * 32, 32), 32)
            value = cvb[rows, :]
            for d in range(2):
                rate = logistic(gs[2 * d, rows, :])
                gate = logistic(gs[2 * d + 1, rows, :])
                keep_log = -8.0 * rate * decay[d : d + 1, lanes] + ldb[d, rows, :]
                keep = jnp.exp(keep_log)
                rest = one_minus_exp(2.0 * keep_log, keep * keep)
                aa[d, b, rows, :] = keep
                bb[d, b, rows, :] = root(rest) * gate * value
            return 0

        lax.fori_loop(0, TOK // 32, rows_of, 0)

    block(0)
    block(1)
    serve(r_out[4][:5])
    block(2)
    serve(r_out[4][5:])
    block(3)

    def scan_step(t, carry):
        new = []
        for d in range(2):
            at = pl.ds(t if d == 0 else SEG - 1 - t, SEGS, stride=SEG)
            for b in range(4):
                prod, state = carry[2 * (4 * d + b)], carry[2 * (4 * d + b) + 1]
                keep = aa[d, b, at, :]
                state = keep * state + bb[d, b, at, :]
                prod = prod * keep
                aa[d, b, at, :] = prod
                bb[d, b, at, :] = state
                new += [prod, state]
        return tuple(new)

    ones, zeros = jnp.ones((SEGS, 128), F32), jnp.zeros((SEGS, 128), F32)
    ends = lax.fori_loop(0, SEG, scan_step, (ones, zeros) * 8, unroll=2)
    for d in range(2):
        for b in range(4):
            for k in range(2):
                sg[k, d, :, b * 128 : (b + 1) * 128] = ends[2 * (4 * d + b) + k]
    me = x * NC + c
    for d in range(2):
        prod, state = jnp.ones((1, CH), F32), jnp.zeros((1, CH), F32)
        for j in range(SEGS) if d == 0 else reversed(range(SEGS)):
            ex[0, d, j : j + 1, :] = prod
            ex[1, d, j : j + 1, :] = state
            keep = sg[0, d, j : j + 1, :]
            state = keep * state + sg[1, d, j : j + 1, :]
            prod = prod * keep
        c1[me, 2 * d : 2 * d + 1, :] = prod
        c1[me, 2 * d + 1 : 2 * d + 2, :] = state
    g_k1, k1 = links.group(c1.at[pl.ds(0, 7)]), links.slot()
    for dx, dc in around:
        links.put(c1.at[me], c1.at[me], g_k1, k1, sp_1=xx(dx), sp_2=lax.rem(c + dc, NC))

    serve(r_out[5], r_out[6])
    loads[3].wait()
    links.got(pext.at[pl.ds(0, OWN)], ph[1], **after)
    links.got(pext.at[pl.ds(OWN + TOK, OWN)], ph[-1], **before)

    def combine(table, mine):
        full, inside = [], []
        for d in range(2):
            count = NZ
            prod, state = jnp.ones((1, CH), F32), jnp.zeros((1, CH), F32)
            in_p, in_s = prod, state
            for k in range(count) if d == 0 else reversed(range(count)):
                keep = table[k, 2 * d : 2 * d + 1, :]
                state = keep * state + table[k, 2 * d + 1 : 2 * d + 2, :]
                prod = prod * keep
                passed = (k < mine) if d == 0 else (k > mine)
                in_p = jnp.where(passed, prod, in_p)
                in_s = jnp.where(passed, state, in_s)
            full.append((prod, state))
            inside.append((in_p, in_s))
        return full, inside

    def pooled(n):
        cols = slice(n * 256, (n + 1) * 256)
        total = jnp.dot(box[...], pext[:, cols], preferred_element_type=F32)
        own = pext[OWN : OWN + TOK, cols].astype(F32)
        scale = jnp.concatenate([rcp[...], rcp[...]], axis=1)
        pdf[:, cols] = (total * scale - own).astype(BF16)

    for n in range(2):
        pooled(n)

    links.got(c1.at[pl.ds(0, 7)], k1, **after)
    full, near = combine(c1, me)
    for d in range(2):
        c2[z, 2 * d : 2 * d + 1, :] = full[d][0]
        c2[z, 2 * d + 1 : 2 * d + 2, :] = full[d][1]
    g_k2, k2 = links.group(c2.at[pl.ds(0, 7)]), links.slot()
    for d in range(1, NZ):
        links.put(c2.at[z], c2.at[z], g_k2, k2, sp_0=zz(d))

    for n in range(2):
        cols = slice(n * 256, (n + 1) * 256)
        ycat[:, cols] = jnp.dot(pdf[...], pmv[0, :, cols], preferred_element_type=F32).astype(BF16)

    links.got(c2.at[pl.ds(0, 7)], k2, **after)
    _, far = combine(c2, z)
    for d in range(2):
        (np_, ns_), (fp_, fs_) = near[d], far[d]
        enter = np_ * fs_ + ns_ + (np_ * fp_) * start[d : d + 1, :]
        ex[0, d] = ex[1, d] + ex[0, d] * enter
    for j in range(SEGS):
        rows = slice(j * SEG, (j + 1) * SEG)
        for b in range(4):
            lanes = slice(b * 128, (b + 1) * 128)
            h0 = bb[0, b, rows, :] + aa[0, b, rows, :] * ex[0, 0, j : j + 1, lanes]
            h1 = bb[1, b, rows, :] + aa[1, b, rows, :] * ex[0, 1, j : j + 1, lanes]
            ycat[rows, CH + b * 128 : CH + (b + 1) * 128] = (h0 + h1).astype(BF16)
    out_arrived()

    g_q1, g_q2, g_q3 = links.group(rs1), links.group(rs2), links.group(rs3)
    q1 = [links.slot() for _ in range(NZ)]
    q2 = [links.slot() for _ in range(NZ)]
    q3 = [links.slot() for _ in range(NZ)]

    def relay(n):
        cols = slice(n * 256, (n + 1) * 256)
        d = 1 if n % 2 == 0 else -1
        at = rs2.at[:, pl.ds(n * 256, 256)]
        links.got(at, q2[n], tp=yy(d))
        mg[:, cols] = (rs2[:, cols].astype(F32) + part[yy(d), :, cols].astype(F32)).astype(BF16)
        there = pl.ds(n * 256, 256)
        links.put(mg.at[:, there], rs3.at[:, there], g_q3, q3[n], tp=yy(d))

    for n in range(NZ):
        cols = slice(n * 256, (n + 1) * 256)
        there = pl.ds(n * 256, 256)
        w = wout[n].reshape(256, 2 * CH)
        acc = lax.dot_general(ycat[...], w, NT, preferred_element_type=F32)
        for k in range(NY):
            part[k, :, cols] = acc[k * OUT_ROWS : (k + 1) * OUT_ROWS].astype(BF16)
        d = 1 if n % 2 == 0 else -1
        links.put(part.at[yy(2), :, there], rs2.at[:, there], g_q2, q2[n], tp=yy(d))
        links.put(part.at[yy(-d), :, there], rs1.at[:, there], g_q1, q1[n], tp=yy(-d))
        if n >= 2:
            relay(n - 2)
    relay(NZ - 2)
    relay(NZ - 1)
    for n in range(NZ):
        cols = slice(n * 256, (n + 1) * 256)
        there = pl.ds(n * 256, 256)
        d = 1 if n % 2 == 0 else -1
        links.got(rs1.at[:, there], q1[n], tp=yy(-d))
        links.got(rs3.at[:, there], q3[n], tp=yy(d))
        total = part[y, :, cols].astype(F32) + rs1[:, cols].astype(F32) + rs3[:, cols].astype(F32)
        out[:, cols] = total.astype(BF16)
    links.drain(**after)


def per_device(
    tokens, norm_gain, w_pool_in, w_lru_in, pool_mix, conv_taps, rec_gate, in_gate, decay_rate,
    log_decay, start_state, w_out_pool, w_out_lru,
):
    anywhere = pl.BlockSpec(memory_space=pl.ANY)
    near = pl.BlockSpec(memory_space=pltpu.VMEM)
    buf = pltpu.VMEM
    return pl.pallas_call(
        layer,
        out_shape=jax.ShapeDtypeStruct((OUT_ROWS, D), BF16),
        in_specs=[
            anywhere, near, anywhere, anywhere, anywhere, near, anywhere, anywhere, near, near,
            near, anywhere, anywhere,
        ],
        out_specs=near,
        scratch_shapes=[
            buf((NY, TOK, CH), BF16),
            buf((TOK, D), BF16),
            buf((NZ, NX, NC, 32, 2 * CH), BF16),
            buf((NZ, NX, NC, 32, 2 * CH), BF16),
            buf((1, CH, CH), BF16),
            buf((2, 4, 128, 128), BF16),
            buf((2, 4, 128, 128), BF16),
            buf((2, TOK, 128), F32),
            buf((TOK, EXT), BF16),
            buf((TOK, 128), F32),
            buf((TOK, CH), BF16),
            buf((4, TOK + 2 * PAD, 128), F32),
            buf((2, PAD, CH), BF16),
            buf((TOK, 128), F32),
            buf((EXT, CH), BF16),
            buf((TOK, CH), BF16),
            buf((4, TOK, 128), F32),
            buf((2, 4, TOK, 128), F32),
            buf((2, 4, TOK, 128), F32),
            buf((2, 2, SEGS, CH), F32),
            buf((2, 2, SEGS, CH), F32),
            buf((NX * NC, 4, CH), F32),
            buf((NZ, 4, CH), F32),
            buf((TOK, 2 * CH), BF16),
            buf((NY, OUT_ROWS, D), BF16),
            buf((OUT_ROWS, D), BF16),
            buf((OUT_ROWS, D), BF16),
            buf((OUT_ROWS, D), BF16),
            buf((OUT_ROWS, D), BF16),
            pltpu.SemaphoreType.DMA((N_SEND,)),
            pltpu.SemaphoreType.DMA((N_RECV,)),
            pltpu.SemaphoreType.DMA((N_LOCAL,)),
        ],
        compiler_params=pltpu.CompilerParams(
            collective_id=0, has_side_effects=True, vmem_limit_bytes=60 * 1024 * 1024
        ),
        name="layer",
    )(
        tokens, norm_gain.reshape(1, D), w_pool_in, w_lru_in, pool_mix, conv_taps, rec_gate,
        in_gate, decay_rate, log_decay, start_state, w_out_pool.T, w_out_lru.T,
    )


def solution(mesh):
    torus = Mesh(mesh.devices.reshape(NZ, NX, NC, mesh.shape["tp"]), SP_TP)
    in_specs = (
        P(SP, "tp"),
        P(),
        P(SP, "tp"),
        P(SP, "tp"),
        P("tp", None, None),
        P(None, "tp"),
        P(None, "tp", None, None),
        P(None, "tp", None, None),
        P(None, "tp"),
        P(None, SP),
        P(None, "tp"),
        P("tp", SP),
        P("tp", SP),
    )
    return jax.shard_map(
        per_device, mesh=torus, in_specs=in_specs, out_specs=P(SP_TP, None), check_vma=False
    )
```

```python
import functools

import jax
import jax.numpy as jnp
from jax import lax
from jax.experimental import pallas as pl
from jax.experimental.pallas import tpu as pltpu
from jax.sharding import Mesh
from jax.sharding import PartitionSpec as P

GRID_W = 32
REACH = 8
EPS = 1e-06
SP = ("sp_0", "sp_1", "sp_2")
SP_TP = ("sp_0", "sp_1", "sp_2", "tp")
NZ, NX, NC, NY = 8, 4, 2, 4
TOK = 384
D = 2048
CH = 512
SEGS = 8
SEG = TOK // SEGS
STEP = SEG + 1
OWN = REACH * GRID_W
EXT = TOK + 2 * OWN
PAD = 16
OUT_ROWS = TOK // NY
N_SEND = 19
N_RECV = 130
N_LOCAL = 8
F32 = jnp.float32
BF16 = jnp.bfloat16
NT = (((1,), (1,)), ((), ()))


class Links:
    def __init__(self, send, recv):
        self.send, self.recv, self.groups, self.used = send, recv, [], 0

    def slot(self):
        self.used += 1
        return self.used - 1

    def group(self, region):
        self.groups.append(region)
        return len(self.groups) - 1

    def copy(self, src, dst, group, slot, dev):
        return pltpu.make_async_remote_copy(
            src_ref=src,
            dst_ref=dst,
            send_sem=self.send.at[group],
            recv_sem=self.recv.at[slot],
            device_id=dev,
            device_id_type=pl.DeviceIdType.MESH,
        )

    def put(self, src, dst, group, slot, **dev):
        self.copy(src, dst, group, slot, dev).start()

    def got(self, region, slot, **dev):
        self.copy(region, region, 0, slot, dev).wait_recv()

    def drain(self, **dev):
        for group, region in enumerate(self.groups):
            self.copy(region, region, group, 0, dev).wait_send()


def weight_gather(links, buf, z, x, c):
    lo, hi = pl.ds(0, 16), pl.ds(16, 16)

    def zz(d):
        return lax.rem(z + (d + NZ), NZ)

    def xx(d):
        return lax.rem(x + (d + NX), NX)

    other = {"sp_2": 1 - c}
    both = (1, -1)
    rel = [0, -1, 1, -2, 2, -3, 3, 4]
    a1 = {dx: links.slot() for dx in (1, 3, 2)}
    a2 = {
        (s, k, e): links.slot()
        for s in both
        for e in range(NX)
        for k in range(1, 5 if (s == 1) == (e < 2) else 4)
    }
    b1 = {(s, k): links.slot() for s in both for k in range(1, 5 if s == 1 else 4)}
    b2 = {d: links.slot() for d in rel}
    dd = links.slot()
    g_a1 = links.group(buf.at[0, pl.ds(0, 3), c, lo])
    g_a2 = links.group(buf.at[pl.ds(0, 7), pl.ds(0, NX), c, lo])
    g_b1 = links.group(buf.at[pl.ds(0, 7), 0, c, lo])
    g_b2 = links.group(buf.at[pl.ds(0, NZ), pl.ds(0, 3), c, lo])
    g_dd = links.group(buf.at[pl.ds(0, NZ), pl.ds(0, NX), c])

    def a_send(s, k, e):
        if (s, k, e) in a2:
            piece = buf.at[zz(-s * (k - 1)), xx(e), c, lo]
            links.put(piece, piece, g_a2, a2[s, k, e], sp_0=zz(s))

    def a_hop(s, k, e):
        if (s, k, e) in a2:
            links.got(buf.at[zz(-s * k), xx(e), c, lo], a2[s, k, e], sp_0=zz(s))
            a_send(s, k + 1, e)

    def a_side(dx):
        links.got(buf.at[z, xx(-dx), c, lo], a1[dx], sp_1=xx(dx))
        for s in both:
            a_send(s, 1, NX - dx)

    def b_send(s, k):
        if (s, k) in b1:
            piece = buf.at[zz(-s * (k - 1)), x, c, hi]
            links.put(piece, piece, g_b1, b1[s, k], sp_0=zz(s))

    def b_spread(d):
        piece = buf.at[zz(d), x, c, hi]
        for dx in (1, 3, 2):
            links.put(piece, piece, g_b2, b2[d], sp_1=xx(dx))

    def b_hop(s, k):
        if (s, k) in b1:
            links.got(buf.at[zz(-s * k), x, c, hi], b1[s, k], sp_0=zz(s))
            b_send(s, k + 1)
            b_spread(-s * k if k < 4 else 4)

    def row_done(d):
        links.got(buf.at[zz(d), pl.ds(0, 3), c, hi], b2[d], sp_1=xx(1))
        row = buf.at[zz(d), pl.ds(0, NX), c]
        links.put(row, row, g_dd, dd, **other)

    def first():
        own = buf.at[z, x, c, lo]
        for dx in (1, 3, 2):
            links.put(own, own, g_a1, a1[dx], sp_1=xx(dx))
        for s in both:
            b_send(s, 1)
            a_send(s, 1, 0)

    def arrived():
        links.got(buf.at[pl.ds(0, NZ), pl.ds(0, NX), 1 - c], dd, **other)

    def at(f, *args):
        return functools.partial(f, *args)

    along_b = [[at(b_spread, 0)]] + [[at(b_hop, s, k) for s in both] for k in range(1, 5)]
    along_a = [[first], [at(a_side, 1), at(a_side, 3)]]
    along_a[1] += [at(a_hop, s, 1, 0) for s in both] + [at(a_side, 2)]
    for k in range(2, 6):
        along_a.append(
            [at(a_hop, s, k, 0) for s in both]
            + [at(a_hop, s, k - 1, e) for e in (3, 1, 2) for s in both]
        )
    rows = [[at(row_done, d) for d in ds] for ds in ((0,), (-1, 1), (-2, 2), (-3, 3), (4,))]
    return along_a, along_b, rows, arrived


def logistic(v):
    return 1.0 / (1.0 + jnp.exp(-v))


def one_minus_exp(y, e):
    series = y * (-1.0 / 720.0) - 1.0 / 120.0
    for n in (24.0, 6.0, 2.0, 1.0):
        series = y * series - 1.0 / n
    return jnp.where(y > -0.125, y * series, 1.0 - e)


def root(v):
    return v * lax.rsqrt(jnp.maximum(v, 1e-37))


def layer(
    tokens, gain, wpi, wli, pmix, taps, rgate, igate, decay, logd, start, wop, wol, out,
    tok, nrm, win, wout, pmv, rgv, igv, ldb, box, rcp, ulb, ulf, hb, cvb, pext, pdf, gs, aa, bb,
    sg, ex, c1, c2, ycat, part, rs1, rs2, rs3, mg, send, recv, local,
):
    z, x, c = (lax.axis_index(n) for n in SP)
    y = lax.axis_index("tp")
    s = (z * NX + x) * NC + c
    links = Links(send, recv)

    def zz(d):
        return lax.rem(z + (d + NZ), NZ)

    def xx(d):
        return lax.rem(x + (d + NX), NX)

    def yy(d):
        return lax.rem(y + (d + NY), NY)

    def run_dev(d):
        t = lax.rem(s + (d + NZ * NX * NC), NZ * NX * NC)
        return {"sp_0": t // (NX * NC), "sp_1": lax.rem(t // NC, NX), "sp_2": lax.rem(t, NC)}

    after, before = run_dev(1), run_dev(-1)

    loads = [
        pltpu.make_async_copy(tokens, tok.at[y], local.at[0]),
        pltpu.make_async_copy(wpi, win.at[z, x, c, :, pl.ds(0, CH)], local.at[1]),
        pltpu.make_async_copy(wli, win.at[z, x, c, :, pl.ds(CH, CH)], local.at[2]),
        pltpu.make_async_copy(pmix, pmv, local.at[3]),
        pltpu.make_async_copy(rgate, rgv, local.at[4]),
        pltpu.make_async_copy(igate, igv, local.at[5]),
        pltpu.make_async_copy(wop, wout.at[z, x, c, :, pl.ds(0, CH)], local.at[6]),
        pltpu.make_async_copy(wol, wout.at[z, x, c, :, pl.ds(CH, CH)], local.at[7]),
    ]
    for load in loads:
        load.start()

    barrier = pltpu.get_barrier_semaphore()
    peers = [{"tp": yy(1)}, {"tp": yy(-1)}, after, before]
    peers += [{"sp_0": zz(d)} for d in range(1, NZ)]
    around = [(dx, dc) for dx in range(NX) for dc in range(NC) if dx or dc]
    for dx, dc in around:
        peers.append({"sp_1": xx(dx), "sp_2": lax.rem(c + dc, NC)})
    for peer in peers:
        pl.semaphore_signal(barrier, inc=1, device_id=peer, device_id_type=pl.DeviceIdType.MESH)

    for d in range(2):
        for i in range(TOK // 128):
            rows = slice(i * 128, (i + 1) * 128)
            ldb[d, rows, :] = jnp.broadcast_to(logd[d : d + 1, rows], (128, 128)).T
    half = lax.shift_left(jnp.int32(1), y)
    grid_rows = TOK // GRID_W
    row_count = grid_rows * NZ * NX * NC
    first_row = s * grid_rows

    def boxes(i, _):
        at = pl.multiple_of(i * 32, 32)
        er = lax.shift_right_logical(lax.broadcasted_iota(jnp.int32, (32, EXT), 1), 5)
        ec = lax.broadcasted_iota(jnp.int32, (32, EXT), 1) & (GRID_W - 1)
        col = lax.broadcasted_iota(jnp.int32, (32, EXT), 0)
        low = jnp.maximum(i - half, -first_row) + REACH
        high = jnp.minimum(i + half, row_count - first_row) + REACH
        inside = (er >= low) & (er < high) & (ec >= col - half) & (ec < col + half)
        box[pl.ds(at, 32), :] = jnp.where(inside, 1.0, 0.0).astype(BF16)
        cc = lax.broadcasted_iota(jnp.int32, (32, 128), 0)
        cols = jnp.minimum(cc + half, GRID_W) - jnp.maximum(cc - half, 0)
        rcp[pl.ds(at, 32), :] = 1.0 / (cols * (high - low)).astype(F32)
        return 0

    lax.fori_loop(0, grid_rows, boxes, 0)

    pl.semaphore_wait(barrier, len(peers))
    for load in loads[:3] + loads[6:]:
        load.wait()

    halves = (pl.ds(0, TOK // 2), pl.ds(TOK // 2, TOK // 2))
    g_t1 = links.group(tok.at[pl.ds(0, 2)])
    g_t2 = links.group(tok.at[0])
    t1 = {(d, h): links.slot() for d in (1, -1) for h in (0, 1)}
    t2 = {d: links.slot() for d in (1, -1)}
    for i in (0, 1):
        for d in (1, -1):
            h = i if d == 1 else 1 - i
            piece = tok.at[y, halves[h]]
            links.put(piece, piece, g_t1, t1[d, h], tp=yy(d))
    in_a, in_b, in_rows, in_arrived = weight_gather(links, win, z, x, c)
    out_a, out_b, out_rows, out_arrived = weight_gather(links, wout, z, x, c)

    def serve(*rounds):
        for turn in rounds:
            for step in turn:
                step()

    serve(in_a[0], in_b[0], out_a[0])

    def token_relay():
        for d, h in ((1, 0), (-1, 1)):
            piece = tok.at[yy(-d), halves[h]]
            links.got(piece, t1[d, h], tp=yy(d))
            links.put(piece, piece, g_t2, t2[d], tp=yy(d))

    serve(in_a[1][:2], in_b[1], in_a[1][2:])
    serve(in_b[2], in_a[2], in_rows[0])
    token_relay()
    serve(out_b[0])
    serve(in_b[3], in_a[3], in_rows[1])
    serve(in_b[4], in_a[4], in_rows[2])
    serve(out_b[1], out_a[1])
    serve(in_a[5], in_rows[3], in_rows[4])
    for d, h in ((1, 1), (-1, 0)):
        links.got(tok.at[yy(-d), halves[h]], t1[d, h], tp=yy(d))
    for d, h in ((1, 0), (-1, 1)):
        links.got(tok.at[yy(2), halves[h]], t2[d], tp=yy(d))

    def norm(i, _):
        rows = pl.ds(pl.multiple_of(i * 32, 32), 32)
        total = jnp.zeros((32, 1), F32)
        for k in range(NY):
            v = tok[k, rows, :].astype(F32)
            total = total + jnp.sum(v * v, axis=1, keepdims=True)
        scale = lax.rsqrt(total * (1.0 / D) + EPS)
        for k in range(NY):
            cols = slice(k * CH, (k + 1) * CH)
            v = tok[k, rows, :].astype(F32)
            nrm[rows, cols] = (v * scale * gain[:, cols]).astype(BF16)
        return 0

    serve(out_b[2])
    lax.fori_loop(0, TOK // 32, norm, 0)
    serve(out_b[3], out_a[2])
    in_arrived()

    def project(col):
        w = win[:, :, :, :, col : col + 256].reshape(D, 256)
        return jnp.dot(nrm[...], w, preferred_element_type=F32).astype(BF16)

    for n in range(2):
        u = project(CH + n * 256)
        ulb[:, n * 256 : (n + 1) * 256] = u
        for k in range(2):
            ulf[2 * n + k, PAD : PAD + TOK, :] = u[:, k * 128 : (k + 1) * 128].astype(F32)
    g_ch = links.group(hb)
    ch = {d: links.slot() for d in (1, -1)}
    links.put(ulb.at[pl.ds(TOK - PAD, PAD)], hb.at[0], g_ch, ch[1], **after)
    links.put(ulb.at[pl.ds(0, PAD)], hb.at[1], g_ch, ch[-1], **before)
    for n in range(2):
        pext[OWN : OWN + TOK, n * 256 : (n + 1) * 256] = project(n * 256)
    g_ph = links.group(pext.at[pl.ds(0, 2 * OWN)])
    ph = {d: links.slot() for d in (1, -1)}
    links.put(pext.at[pl.ds(TOK, OWN)], pext.at[pl.ds(0, OWN)], g_ph, ph[1], **after)
    links.put(pext.at[pl.ds(OWN, OWN)], pext.at[pl.ds(OWN + TOK, OWN)], g_ph, ph[-1], **before)

    serve(out_rows[0])
    links.got(hb.at[0], ch[1], **after)
    links.got(hb.at[1], ch[-1], **before)
    has_before = jnp.where(s > 0, 1.0, 0.0).astype(F32)
    has_after = jnp.where(s < NZ * NX * NC - 1, 1.0, 0.0).astype(F32)
    for b in range(4):
        lanes = slice(b * 128, (b + 1) * 128)
        ulf[b, 0:PAD, :] = hb[0, :, lanes].astype(F32) * has_before
        ulf[b, PAD + TOK :, :] = hb[1, :, lanes].astype(F32) * has_after
    for load in loads[4:6]:
        load.wait()

    def block(b):
        lanes = slice(b * 128, (b + 1) * 128)
        tap = taps[:, lanes].astype(F32)
        acc = ulf[b, PAD - 2 : PAD - 2 + TOK, :] * tap[0:1]
        for k in range(1, 4):
            acc = acc + ulf[b, PAD - 2 + k : PAD - 2 + k + TOK, :] * tap[k : k + 1]
        conv = acc.astype(BF16)
        cvb[...] = conv.astype(F32)
        for d in range(2):
            gs[2 * d] = jnp.dot(conv, rgv[d, b], preferred_element_type=F32)
            gs[2 * d + 1] = jnp.dot(conv, igv[d, b], preferred_element_type=F32)

        for j in range(SEGS):
            rows, padded = slice(j * SEG, (j + 1) * SEG), slice(j * STEP, j * STEP + SEG)
            value = cvb[rows, :]
            for d in range(2):
                rate = logistic(gs[2 * d, rows, :])
                gate = logistic(gs[2 * d + 1, rows, :])
                keep_log = -8.0 * rate * decay[d : d + 1, lanes] + ldb[d, rows, :]
                keep = jnp.exp(keep_log)
                rest = one_minus_exp(2.0 * keep_log, keep * keep)
                aa[d, b, padded, :] = keep
                bb[d, b, padded, :] = root(rest) * gate * value

    block(0)
    block(1)
    serve(out_b[4], out_a[3])
    block(2)
    block(3)

    def scan_step(t, carry):
        new = []
        for d in range(2):
            at = pl.ds(t if d == 0 else SEG - 1 - t, SEGS, stride=STEP)
            for b in range(4):
                prod, state = carry[2 * (4 * d + b)], carry[2 * (4 * d + b) + 1]
                keep = aa[d, b, at, :]
                state = keep * state + bb[d, b, at, :]
                prod = prod * keep
                aa[d, b, at, :] = prod
                bb[d, b, at, :] = state
                new += [prod, state]
        return tuple(new)

    ones, zeros = jnp.ones((SEGS, 128), F32), jnp.zeros((SEGS, 128), F32)
    ends = lax.fori_loop(0, SEG, scan_step, (ones, zeros) * 8, unroll=2)
    for d in range(2):
        for b in range(4):
            for k in range(2):
                sg[k, d, :, b * 128 : (b + 1) * 128] = ends[2 * (4 * d + b) + k]
    me = x * NC + c
    for d in range(2):
        prod, state = jnp.ones((1, CH), F32), jnp.zeros((1, CH), F32)
        for j in range(SEGS) if d == 0 else reversed(range(SEGS)):
            ex[0, d, j : j + 1, :] = prod
            ex[1, d, j : j + 1, :] = state
            keep = sg[0, d, j : j + 1, :]
            state = keep * state + sg[1, d, j : j + 1, :]
            prod = prod * keep
        c1[me, 2 * d : 2 * d + 1, :] = prod
        c1[me, 2 * d + 1 : 2 * d + 2, :] = state
    g_k1, k1 = links.group(c1.at[pl.ds(0, 7)]), links.slot()
    for dx, dc in around:
        links.put(c1.at[me], c1.at[me], g_k1, k1, sp_1=xx(dx), sp_2=lax.rem(c + dc, NC))

    loads[3].wait()
    links.got(pext.at[pl.ds(0, OWN)], ph[1], **after)
    links.got(pext.at[pl.ds(OWN + TOK, OWN)], ph[-1], **before)

    def combine(table, mine):
        full, inside = [], []
        for d in range(2):
            count = NZ
            prod, state = jnp.ones((1, CH), F32), jnp.zeros((1, CH), F32)
            in_p, in_s = prod, state
            for k in range(count) if d == 0 else reversed(range(count)):
                keep = table[k, 2 * d : 2 * d + 1, :]
                state = keep * state + table[k, 2 * d + 1 : 2 * d + 2, :]
                prod = prod * keep
                passed = (k < mine) if d == 0 else (k > mine)
                in_p = jnp.where(passed, prod, in_p)
                in_s = jnp.where(passed, state, in_s)
            full.append((prod, state))
            inside.append((in_p, in_s))
        return full, inside

    def pooled(n):
        cols = slice(n * 256, (n + 1) * 256)
        total = jnp.dot(box[...], pext[:, cols], preferred_element_type=F32)
        own = pext[OWN : OWN + TOK, cols].astype(F32)
        scale = jnp.concatenate([rcp[...], rcp[...]], axis=1)
        pdf[:, cols] = (total * scale - own).astype(BF16)

    for n in range(2):
        pooled(n)

    serve(out_rows[1], out_a[4])
    links.got(c1.at[pl.ds(0, 7)], k1, **after)
    full, near = combine(c1, me)
    for d in range(2):
        c2[z, 2 * d : 2 * d + 1, :] = full[d][0]
        c2[z, 2 * d + 1 : 2 * d + 2, :] = full[d][1]
    g_k2, k2 = links.group(c2.at[pl.ds(0, 7)]), links.slot()
    for d in range(1, NZ):
        links.put(c2.at[z], c2.at[z], g_k2, k2, sp_0=zz(d))

    for n in range(2):
        cols = slice(n * 256, (n + 1) * 256)
        ycat[:, cols] = jnp.dot(pdf[...], pmv[0, :, cols], preferred_element_type=F32).astype(BF16)

    serve(out_rows[2], out_a[5], out_rows[3], out_rows[4])
    links.got(c2.at[pl.ds(0, 7)], k2, **after)
    _, far = combine(c2, z)
    for d in range(2):
        (np_, ns_), (fp_, fs_) = near[d], far[d]
        enter = np_ * fs_ + ns_ + (np_ * fp_) * start[d : d + 1, :]
        ex[0, d] = ex[1, d] + ex[0, d] * enter
    for j in range(SEGS):
        rows, padded = slice(j * SEG, (j + 1) * SEG), slice(j * STEP, j * STEP + SEG)
        for b in range(4):
            lanes = slice(b * 128, (b + 1) * 128)
            h0 = bb[0, b, padded, :] + aa[0, b, padded, :] * ex[0, 0, j : j + 1, lanes]
            h1 = bb[1, b, padded, :] + aa[1, b, padded, :] * ex[0, 1, j : j + 1, lanes]
            ycat[rows, CH + b * 128 : CH + (b + 1) * 128] = (h0 + h1).astype(BF16)
    out_arrived()

    g_q1, g_q2, g_q3 = links.group(rs1), links.group(rs2), links.group(rs3)
    q1 = [links.slot() for _ in range(NZ)]
    q2 = [links.slot() for _ in range(NZ)]
    q3 = [links.slot() for _ in range(NZ)]

    def relay(n):
        cols = slice(n * 256, (n + 1) * 256)
        d = 1 if n % 2 == 0 else -1
        at = rs2.at[:, pl.ds(n * 256, 256)]
        links.got(at, q2[n], tp=yy(d))
        mg[:, cols] = (rs2[:, cols].astype(F32) + part[yy(d), :, cols].astype(F32)).astype(BF16)
        there = pl.ds(n * 256, 256)
        links.put(mg.at[:, there], rs3.at[:, there], g_q3, q3[n], tp=yy(d))

    for n in range(NZ):
        cols = slice(n * 256, (n + 1) * 256)
        there = pl.ds(n * 256, 256)
        w = wout[n].reshape(256, 2 * CH)
        acc = lax.dot_general(ycat[...], w, NT, preferred_element_type=F32)
        for k in range(NY):
            part[k, :, cols] = acc[k * OUT_ROWS : (k + 1) * OUT_ROWS].astype(BF16)
        d = 1 if n % 2 == 0 else -1
        links.put(part.at[yy(2), :, there], rs2.at[:, there], g_q2, q2[n], tp=yy(d))
        links.put(part.at[yy(-d), :, there], rs1.at[:, there], g_q1, q1[n], tp=yy(-d))
        if n >= 2:
            relay(n - 2)
    relay(NZ - 2)
    relay(NZ - 1)
    for n in range(NZ):
        cols = slice(n * 256, (n + 1) * 256)
        there = pl.ds(n * 256, 256)
        d = 1 if n % 2 == 0 else -1
        links.got(rs1.at[:, there], q1[n], tp=yy(-d))
        links.got(rs3.at[:, there], q3[n], tp=yy(d))
        total = part[y, :, cols].astype(F32) + rs1[:, cols].astype(F32) + rs3[:, cols].astype(F32)
        out[:, cols] = total.astype(BF16)
    links.drain(**after)


def per_device(
    tokens, norm_gain, w_pool_in, w_lru_in, pool_mix, conv_taps, rec_gate, in_gate, decay_rate,
    log_decay, start_state, w_out_pool, w_out_lru,
):
    anywhere = pl.BlockSpec(memory_space=pl.ANY)
    near = pl.BlockSpec(memory_space=pltpu.VMEM)
    buf = pltpu.VMEM
    return pl.pallas_call(
        layer,
        out_shape=jax.ShapeDtypeStruct((OUT_ROWS, D), BF16),
        in_specs=[
            anywhere, near, anywhere, anywhere, anywhere, near, anywhere, anywhere, near, near,
            near, anywhere, anywhere,
        ],
        out_specs=near,
        scratch_shapes=[
            buf((NY, TOK, CH), BF16),
            buf((TOK, D), BF16),
            buf((NZ, NX, NC, 32, 2 * CH), BF16),
            buf((NZ, NX, NC, 32, 2 * CH), BF16),
            buf((1, CH, CH), BF16),
            buf((2, 4, 128, 128), BF16),
            buf((2, 4, 128, 128), BF16),
            buf((2, TOK, 128), F32),
            buf((TOK, EXT), BF16),
            buf((TOK, 128), F32),
            buf((TOK, CH), BF16),
            buf((4, TOK + 2 * PAD, 128), F32),
            buf((2, PAD, CH), BF16),
            buf((TOK, 128), F32),
            buf((EXT, CH), BF16),
            buf((TOK, CH), BF16),
            buf((4, TOK, 128), F32),
            buf((2, 4, SEGS * STEP, 128), F32),
            buf((2, 4, SEGS * STEP, 128), F32),
            buf((2, 2, SEGS, CH), F32),
            buf((2, 2, SEGS, CH), F32),
            buf((NX * NC, 4, CH), F32),
            buf((NZ, 4, CH), F32),
            buf((TOK, 2 * CH), BF16),
            buf((NY, OUT_ROWS, D), BF16),
            buf((OUT_ROWS, D), BF16),
            buf((OUT_ROWS, D), BF16),
            buf((OUT_ROWS, D), BF16),
            buf((OUT_ROWS, D), BF16),
            pltpu.SemaphoreType.DMA((N_SEND,)),
            pltpu.SemaphoreType.DMA((N_RECV,)),
            pltpu.SemaphoreType.DMA((N_LOCAL,)),
        ],
        compiler_params=pltpu.CompilerParams(
            collective_id=0, has_side_effects=True, vmem_limit_bytes=60 * 1024 * 1024
        ),
        name="layer",
    )(
        tokens, norm_gain.reshape(1, D), w_pool_in, w_lru_in, pool_mix, conv_taps, rec_gate,
        in_gate, decay_rate, log_decay, start_state, w_out_pool.T, w_out_lru.T,
    )


def solution(mesh):
    torus = Mesh(mesh.devices.reshape(NZ, NX, NC, mesh.shape["tp"]), SP_TP)
    in_specs = (
        P(SP, "tp"),
        P(),
        P(SP, "tp"),
        P(SP, "tp"),
        P("tp", None, None),
        P(None, "tp"),
        P(None, "tp", None, None),
        P(None, "tp", None, None),
        P(None, "tp"),
        P(None, SP),
        P(None, "tp"),
        P("tp", SP),
        P("tp", SP),
    )
    return jax.shard_map(
        per_device, mesh=torus, in_specs=in_specs, out_specs=P(SP_TP, None), check_vma=False
    )
```

```python
import functools

import jax
import jax.numpy as jnp
from jax import lax
from jax.experimental import pallas as pl
from jax.experimental.pallas import tpu as pltpu
from jax.sharding import Mesh
from jax.sharding import PartitionSpec as P

GRID_W = 32
REACH = 8
EPS = 1e-06
SP = ("sp_0", "sp_1", "sp_2")
SP_TP = ("sp_0", "sp_1", "sp_2", "tp")
NZ, NX, NC, NY = 8, 4, 2, 4
TOK = 384
D = 2048
CH = 512
SEGS = 8
SEG = TOK // SEGS
STEP = SEG + 1
OWN = REACH * GRID_W
EXT = TOK + 2 * OWN
PAD = 16
OUT_ROWS = TOK // NY
N_SEND = 19
N_RECV = 116
N_LOCAL = 8
F32 = jnp.float32
BF16 = jnp.bfloat16
NT = (((1,), (1,)), ((), ()))


class Links:
    def __init__(self, send, recv):
        self.send, self.recv, self.groups, self.used = send, recv, [], 0

    def slot(self):
        self.used += 1
        return self.used - 1

    def group(self, region):
        self.groups.append(region)
        return len(self.groups) - 1

    def copy(self, src, dst, group, slot, dev):
        return pltpu.make_async_remote_copy(
            src_ref=src,
            dst_ref=dst,
            send_sem=self.send.at[group],
            recv_sem=self.recv.at[slot],
            device_id=dev,
            device_id_type=pl.DeviceIdType.MESH,
        )

    def put(self, src, dst, group, slot, **dev):
        self.copy(src, dst, group, slot, dev).start()

    def got(self, region, slot, **dev):
        self.copy(region, region, 0, slot, dev).wait_recv()

    def drain(self, **dev):
        for group, region in enumerate(self.groups):
            self.copy(region, region, group, 0, dev).wait_send()


def weight_gather(links, buf, z, x, c):
    lo, hi = pl.ds(0, 16), pl.ds(16, 16)

    def zz(d):
        return lax.rem(z + (d + NZ), NZ)

    def xx(d):
        return lax.rem(x + (d + NX), NX)

    other = {"sp_2": 1 - c}
    both = (1, -1)
    rel = [0, -1, 1, -2, 2, -3, 3, 4]
    a1 = {dx: links.slot() for dx in (1, 3, 2)}
    a2 = {
        (s, k, e): links.slot()
        for s in both
        for e in range(NX)
        for k in range(1, 5 if (s == 1) == (e < 2) else 4)
    }
    b1 = {(s, k): links.slot() for s in both for k in range(1, 5 if s == 1 else 4)}
    b2 = {d: links.slot() for d in rel}
    dd = links.slot()
    g_a1 = links.group(buf.at[0, pl.ds(0, 3), c, lo])
    g_a2 = links.group(buf.at[pl.ds(0, 7), pl.ds(0, NX), c, lo])
    g_b1 = links.group(buf.at[pl.ds(0, 7), 0, c, lo])
    g_b2 = links.group(buf.at[pl.ds(0, NZ), pl.ds(0, 3), c, lo])
    g_dd = links.group(buf.at[pl.ds(0, NZ), pl.ds(0, NX), c])

    def a_send(s, k, e):
        if (s, k, e) in a2:
            piece = buf.at[zz(-s * (k - 1)), xx(e), c, lo]
            links.put(piece, piece, g_a2, a2[s, k, e], sp_0=zz(s))

    def a_hop(s, k, e):
        if (s, k, e) in a2:
            links.got(buf.at[zz(-s * k), xx(e), c, lo], a2[s, k, e], sp_0=zz(s))
            a_send(s, k + 1, e)

    def a_side(dx):
        links.got(buf.at[z, xx(-dx), c, lo], a1[dx], sp_1=xx(dx))
        for s in both:
            a_send(s, 1, NX - dx)

    def b_send(s, k):
        if (s, k) in b1:
            piece = buf.at[zz(-s * (k - 1)), x, c, hi]
            links.put(piece, piece, g_b1, b1[s, k], sp_0=zz(s))

    def b_spread(d):
        piece = buf.at[zz(d), x, c, hi]
        for dx in (1, 3, 2):
            links.put(piece, piece, g_b2, b2[d], sp_1=xx(dx))

    def b_hop(s, k):
        if (s, k) in b1:
            links.got(buf.at[zz(-s * k), x, c, hi], b1[s, k], sp_0=zz(s))
            b_send(s, k + 1)
            b_spread(-s * k if k < 4 else 4)

    def row_done(d):
        links.got(buf.at[zz(d), pl.ds(0, 3), c, hi], b2[d], sp_1=xx(1))
        row = buf.at[zz(d), pl.ds(0, NX), c]
        links.put(row, row, g_dd, dd, **other)

    def first():
        own = buf.at[z, x, c, lo]
        for dx in (1, 3, 2):
            links.put(own, own, g_a1, a1[dx], sp_1=xx(dx))
        for s in both:
            b_send(s, 1)
            a_send(s, 1, 0)

    def arrived():
        links.got(buf.at[pl.ds(0, NZ), pl.ds(0, NX), 1 - c], dd, **other)

    def at(f, *args):
        return functools.partial(f, *args)

    along_b = [[at(b_spread, 0)]] + [[at(b_hop, s, k) for s in both] for k in range(1, 5)]
    along_a = [[first], [at(a_side, 1), at(a_side, 3)]]
    along_a[1] += [at(a_hop, s, 1, 0) for s in both] + [at(a_side, 2)]
    for k in range(2, 6):
        along_a.append(
            [at(a_hop, s, k, 0) for s in both]
            + [at(a_hop, s, k - 1, e) for e in (3, 1, 2) for s in both]
        )
    rows = [[at(row_done, d) for d in ds] for ds in ((0,), (-1, 1), (-2, 2), (-3, 3), (4,))]
    return along_a, along_b, rows, arrived


def logistic(v):
    return 1.0 / (1.0 + jnp.exp(-v))


def one_minus_exp(y, e):
    series = y * (-1.0 / 720.0) - 1.0 / 120.0
    for n in (24.0, 6.0, 2.0, 1.0):
        series = y * series - 1.0 / n
    return jnp.where(y > -0.125, y * series, 1.0 - e)


def root(v):
    return v * lax.rsqrt(jnp.maximum(v, 1e-37))


def layer(
    tokens, gain, wpi, wli, pmix, taps, rgate, igate, decay, logd, start, wop, wol, own, rs1, rs3,
    tok, nrm, win, wout, pmv, rgv, igv, ldb, box, rcp, ulb, ulf, hb, cvb, pext, pdf, gs, aa, bb,
    sg, ex, c1, c2, ycat, part, rs2, mg, send, recv, local,
):
    z, x, c = (lax.axis_index(n) for n in SP)
    y = lax.axis_index("tp")
    s = (z * NX + x) * NC + c
    links = Links(send, recv)

    def zz(d):
        return lax.rem(z + (d + NZ), NZ)

    def xx(d):
        return lax.rem(x + (d + NX), NX)

    def yy(d):
        return lax.rem(y + (d + NY), NY)

    def run_dev(d):
        t = lax.rem(s + (d + NZ * NX * NC), NZ * NX * NC)
        return {"sp_0": t // (NX * NC), "sp_1": lax.rem(t // NC, NX), "sp_2": lax.rem(t, NC)}

    after, before = run_dev(1), run_dev(-1)

    loads = [
        pltpu.make_async_copy(tokens, tok.at[y], local.at[0]),
        pltpu.make_async_copy(wpi, win.at[z, x, c, :, pl.ds(0, CH)], local.at[1]),
        pltpu.make_async_copy(wli, win.at[z, x, c, :, pl.ds(CH, CH)], local.at[2]),
        pltpu.make_async_copy(pmix, pmv, local.at[3]),
        pltpu.make_async_copy(rgate, rgv, local.at[4]),
        pltpu.make_async_copy(igate, igv, local.at[5]),
        pltpu.make_async_copy(wop, wout.at[z, x, c, :, pl.ds(0, CH)], local.at[6]),
        pltpu.make_async_copy(wol, wout.at[z, x, c, :, pl.ds(CH, CH)], local.at[7]),
    ]
    for load in loads:
        load.start()

    barrier = pltpu.get_barrier_semaphore()
    peers = [{"tp": yy(1)}, {"tp": yy(-1)}, after, before]
    peers += [{"sp_0": zz(d)} for d in range(1, NZ)]
    around = [(dx, dc) for dx in range(NX) for dc in range(NC) if dx or dc]
    for dx, dc in around:
        peers.append({"sp_1": xx(dx), "sp_2": lax.rem(c + dc, NC)})
    for peer in peers:
        pl.semaphore_signal(barrier, inc=1, device_id=peer, device_id_type=pl.DeviceIdType.MESH)

    for d in range(2):
        for i in range(TOK // 128):
            rows = slice(i * 128, (i + 1) * 128)
            ldb[d, rows, :] = jnp.broadcast_to(logd[d : d + 1, rows], (128, 128)).T
    half = lax.shift_left(jnp.int32(1), y)
    grid_rows = TOK // GRID_W
    row_count = grid_rows * NZ * NX * NC
    first_row = s * grid_rows

    def boxes(i, _):
        at = pl.multiple_of(i * 32, 32)
        er = lax.shift_right_logical(lax.broadcasted_iota(jnp.int32, (32, EXT), 1), 5)
        ec = lax.broadcasted_iota(jnp.int32, (32, EXT), 1) & (GRID_W - 1)
        col = lax.broadcasted_iota(jnp.int32, (32, EXT), 0)
        low = jnp.maximum(i - half, -first_row) + REACH
        high = jnp.minimum(i + half, row_count - first_row) + REACH
        inside = (er >= low) & (er < high) & (ec >= col - half) & (ec < col + half)
        box[pl.ds(at, 32), :] = jnp.where(inside, 1.0, 0.0).astype(BF16)
        cc = lax.broadcasted_iota(jnp.int32, (32, 128), 0)
        cols = jnp.minimum(cc + half, GRID_W) - jnp.maximum(cc - half, 0)
        rcp[pl.ds(at, 32), :] = 1.0 / (cols * (high - low)).astype(F32)
        return 0

    lax.fori_loop(0, grid_rows, boxes, 0)

    pl.semaphore_wait(barrier, len(peers))
    for load in loads[:3] + loads[6:]:
        load.wait()

    halves = (pl.ds(0, TOK // 2), pl.ds(TOK // 2, TOK // 2))
    g_t1 = links.group(tok.at[pl.ds(0, 2)])
    g_t2 = links.group(tok.at[0])
    t1 = {(d, h): links.slot() for d in (1, -1) for h in (0, 1)}
    t2 = {d: links.slot() for d in (1, -1)}
    for i in (0, 1):
        for d in (1, -1):
            h = i if d == 1 else 1 - i
            piece = tok.at[y, halves[h]]
            links.put(piece, piece, g_t1, t1[d, h], tp=yy(d))
    in_a, in_b, in_rows, in_arrived = weight_gather(links, win, z, x, c)
    out_a, out_b, out_rows, out_arrived = weight_gather(links, wout, z, x, c)

    def serve(*rounds):
        for turn in rounds:
            for step in turn:
                step()

    serve(in_a[0], in_b[0], out_a[0])

    def token_relay():
        for d, h in ((1, 0), (-1, 1)):
            piece = tok.at[yy(-d), halves[h]]
            links.got(piece, t1[d, h], tp=yy(d))
            links.put(piece, piece, g_t2, t2[d], tp=yy(d))

    serve(in_a[1][:2], in_b[1], in_a[1][2:])
    serve(in_b[2], in_a[2], in_rows[0])
    token_relay()
    serve(out_b[0])
    serve(in_b[3], in_a[3], in_rows[1])
    serve(in_b[4], in_a[4], in_rows[2])
    serve(out_b[1], out_a[1])
    serve(in_a[5], in_rows[3], in_rows[4])
    for d, h in ((1, 1), (-1, 0)):
        links.got(tok.at[yy(-d), halves[h]], t1[d, h], tp=yy(d))
    for d, h in ((1, 0), (-1, 1)):
        links.got(tok.at[yy(2), halves[h]], t2[d], tp=yy(d))

    def norm(i, _):
        rows = pl.ds(pl.multiple_of(i * 32, 32), 32)
        total = jnp.zeros((32, 1), F32)
        for k in range(NY):
            v = tok[k, rows, :].astype(F32)
            total = total + jnp.sum(v * v, axis=1, keepdims=True)
        scale = lax.rsqrt(total * (1.0 / D) + EPS)
        for k in range(NY):
            cols = slice(k * CH, (k + 1) * CH)
            v = tok[k, rows, :].astype(F32)
            nrm[rows, cols] = (v * scale * gain[:, cols]).astype(BF16)
        return 0

    serve(out_b[2])
    lax.fori_loop(0, TOK // 32, norm, 0)
    in_arrived()

    def project(col):
        w = win[:, :, :, :, col : col + 256].reshape(D, 256)
        return jnp.dot(nrm[...], w, preferred_element_type=F32).astype(BF16)

    for n in range(2):
        u = project(CH + n * 256)
        ulb[:, n * 256 : (n + 1) * 256] = u
        for k in range(2):
            ulf[2 * n + k, PAD : PAD + TOK, :] = u[:, k * 128 : (k + 1) * 128].astype(F32)
    g_ch = links.group(hb)
    ch = {d: links.slot() for d in (1, -1)}
    links.put(ulb.at[pl.ds(TOK - PAD, PAD)], hb.at[0], g_ch, ch[1], **after)
    links.put(ulb.at[pl.ds(0, PAD)], hb.at[1], g_ch, ch[-1], **before)
    serve(out_b[3], out_a[2])
    for n in range(2):
        pext[OWN : OWN + TOK, n * 256 : (n + 1) * 256] = project(n * 256)
    g_ph = links.group(pext.at[pl.ds(0, 2 * OWN)])
    ph = {d: links.slot() for d in (1, -1)}
    links.put(pext.at[pl.ds(TOK, OWN)], pext.at[pl.ds(0, OWN)], g_ph, ph[1], **after)
    links.put(pext.at[pl.ds(OWN, OWN)], pext.at[pl.ds(OWN + TOK, OWN)], g_ph, ph[-1], **before)

    serve(out_rows[0])
    links.got(hb.at[0], ch[1], **after)
    links.got(hb.at[1], ch[-1], **before)
    has_before = jnp.where(s > 0, 1.0, 0.0).astype(F32)
    has_after = jnp.where(s < NZ * NX * NC - 1, 1.0, 0.0).astype(F32)
    for b in range(4):
        lanes = slice(b * 128, (b + 1) * 128)
        ulf[b, 0:PAD, :] = hb[0, :, lanes].astype(F32) * has_before
        ulf[b, PAD + TOK :, :] = hb[1, :, lanes].astype(F32) * has_after
    for load in loads[4:6]:
        load.wait()

    def block(b):
        lanes = slice(b * 128, (b + 1) * 128)
        tap = taps[:, lanes].astype(F32)
        acc = ulf[b, PAD - 2 : PAD - 2 + TOK, :] * tap[0:1]
        for k in range(1, 4):
            acc = acc + ulf[b, PAD - 2 + k : PAD - 2 + k + TOK, :] * tap[k : k + 1]
        conv = acc.astype(BF16)
        cvb[...] = conv.astype(F32)
        for d in range(2):
            gs[2 * d] = jnp.dot(conv, rgv[d, b], preferred_element_type=F32)
            gs[2 * d + 1] = jnp.dot(conv, igv[d, b], preferred_element_type=F32)

        for j in range(SEGS):
            rows, padded = slice(j * SEG, (j + 1) * SEG), slice(j * STEP, j * STEP + SEG)
            value = cvb[rows, :]
            for d in range(2):
                rate = logistic(gs[2 * d, rows, :])
                gate = logistic(gs[2 * d + 1, rows, :])
                keep_log = -8.0 * rate * decay[d : d + 1, lanes] + ldb[d, rows, :]
                keep = jnp.exp(keep_log)
                rest = one_minus_exp(2.0 * keep_log, keep * keep)
                aa[d, b, padded, :] = keep
                bb[d, b, padded, :] = root(rest) * gate * value

    block(0)
    block(1)
    serve(out_b[4], out_a[3])
    block(2)
    block(3)

    def scan_step(t, carry):
        new = []
        for d in range(2):
            at = pl.ds(t if d == 0 else SEG - 1 - t, SEGS, stride=STEP)
            for b in range(4):
                prod, state = carry[2 * (4 * d + b)], carry[2 * (4 * d + b) + 1]
                keep = aa[d, b, at, :]
                state = keep * state + bb[d, b, at, :]
                prod = prod * keep
                aa[d, b, at, :] = prod
                bb[d, b, at, :] = state
                new += [prod, state]
        return tuple(new)

    ones, zeros = jnp.ones((SEGS, 128), F32), jnp.zeros((SEGS, 128), F32)
    ends = lax.fori_loop(0, SEG, scan_step, (ones, zeros) * 8, unroll=2)
    for d in range(2):
        for b in range(4):
            for k in range(2):
                sg[k, d, :, b * 128 : (b + 1) * 128] = ends[2 * (4 * d + b) + k]
    me = x * NC + c
    for d in range(2):
        prod, state = jnp.ones((1, CH), F32), jnp.zeros((1, CH), F32)
        for j in range(SEGS) if d == 0 else reversed(range(SEGS)):
            ex[0, d, j : j + 1, :] = prod
            ex[1, d, j : j + 1, :] = state
            keep = sg[0, d, j : j + 1, :]
            state = keep * state + sg[1, d, j : j + 1, :]
            prod = prod * keep
        c1[me, 2 * d : 2 * d + 1, :] = prod
        c1[me, 2 * d + 1 : 2 * d + 2, :] = state
    g_k1, k1 = links.group(c1.at[pl.ds(0, 7)]), links.slot()
    for dx, dc in around:
        links.put(c1.at[me], c1.at[me], g_k1, k1, sp_1=xx(dx), sp_2=lax.rem(c + dc, NC))

    loads[3].wait()
    links.got(pext.at[pl.ds(0, OWN)], ph[1], **after)
    links.got(pext.at[pl.ds(OWN + TOK, OWN)], ph[-1], **before)

    def combine(table, mine):
        full, inside = [], []
        for d in range(2):
            count = NZ
            prod, state = jnp.ones((1, CH), F32), jnp.zeros((1, CH), F32)
            in_p, in_s = prod, state
            for k in range(count) if d == 0 else reversed(range(count)):
                keep = table[k, 2 * d : 2 * d + 1, :]
                state = keep * state + table[k, 2 * d + 1 : 2 * d + 2, :]
                prod = prod * keep
                passed = (k < mine) if d == 0 else (k > mine)
                in_p = jnp.where(passed, prod, in_p)
                in_s = jnp.where(passed, state, in_s)
            full.append((prod, state))
            inside.append((in_p, in_s))
        return full, inside

    def pooled(n):
        cols = slice(n * 256, (n + 1) * 256)
        total = jnp.dot(box[...], pext[:, cols], preferred_element_type=F32)
        own = pext[OWN : OWN + TOK, cols].astype(F32)
        scale = jnp.concatenate([rcp[...], rcp[...]], axis=1)
        pdf[:, cols] = (total * scale - own).astype(BF16)

    for n in range(2):
        pooled(n)

    serve(out_rows[1], out_a[4])
    links.got(c1.at[pl.ds(0, 7)], k1, **after)
    full, near = combine(c1, me)
    for d in range(2):
        c2[z, 2 * d : 2 * d + 1, :] = full[d][0]
        c2[z, 2 * d + 1 : 2 * d + 2, :] = full[d][1]
    g_k2, k2 = links.group(c2.at[pl.ds(0, 7)]), links.slot()
    for d in range(1, NZ):
        links.put(c2.at[z], c2.at[z], g_k2, k2, sp_0=zz(d))

    for n in range(2):
        cols = slice(n * 256, (n + 1) * 256)
        ycat[:, cols] = jnp.dot(pdf[...], pmv[0, :, cols], preferred_element_type=F32).astype(BF16)

    serve(out_rows[2], out_a[5], out_rows[3], out_rows[4])
    links.got(c2.at[pl.ds(0, 7)], k2, **after)
    _, far = combine(c2, z)
    for d in range(2):
        (np_, ns_), (fp_, fs_) = near[d], far[d]
        enter = np_ * fs_ + ns_ + (np_ * fp_) * start[d : d + 1, :]
        ex[0, d] = ex[1, d] + ex[0, d] * enter
    for j in range(SEGS):
        rows, padded = slice(j * SEG, (j + 1) * SEG), slice(j * STEP, j * STEP + SEG)
        for b in range(4):
            lanes = slice(b * 128, (b + 1) * 128)
            h0 = bb[0, b, padded, :] + aa[0, b, padded, :] * ex[0, 0, j : j + 1, lanes]
            h1 = bb[1, b, padded, :] + aa[1, b, padded, :] * ex[0, 1, j : j + 1, lanes]
            ycat[rows, CH + b * 128 : CH + (b + 1) * 128] = (h0 + h1).astype(BF16)
    out_arrived()

    g_q1, g_q2, g_q3 = links.group(rs1), links.group(rs2), links.group(rs3)
    q1, q3 = links.slot(), links.slot()
    q2 = [links.slot() for _ in range(NZ)]

    def relay(n):
        cols = slice(n * 256, (n + 1) * 256)
        d = 1 if n % 2 == 0 else -1
        at = rs2.at[:, pl.ds(n * 256, 256)]
        links.got(at, q2[n], tp=yy(d))
        mg[:, cols] = (rs2[:, cols].astype(F32) + part[yy(d), :, cols].astype(F32)).astype(BF16)
        there = pl.ds(n * 256, 256)
        links.put(mg.at[:, there], rs3.at[:, there], g_q3, q3, tp=yy(d))

    for n in range(NZ):
        cols = slice(n * 256, (n + 1) * 256)
        there = pl.ds(n * 256, 256)
        w = wout[n].reshape(256, 2 * CH)
        acc = lax.dot_general(ycat[...], w, NT, preferred_element_type=F32)
        for k in range(NY):
            part[k, :, cols] = acc[k * OUT_ROWS : (k + 1) * OUT_ROWS].astype(BF16)
        d = 1 if n % 2 == 0 else -1
        links.put(part.at[yy(2), :, there], rs2.at[:, there], g_q2, q2[n], tp=yy(d))
        links.put(part.at[yy(-d), :, there], rs1.at[:, there], g_q1, q1, tp=yy(-d))
        if n >= 5:
            relay(n - 5)
    keep_own = pltpu.make_async_copy(part.at[y], own, local.at[0])
    keep_own.start()
    for n in range(3, NZ):
        relay(n)
    links.got(rs1, q1, **after)
    links.got(rs3, q3, **after)
    keep_own.wait()
    links.drain(**after)


def per_device(
    tokens, norm_gain, w_pool_in, w_lru_in, pool_mix, conv_taps, rec_gate, in_gate, decay_rate,
    log_decay, start_state, w_out_pool, w_out_lru,
):
    anywhere = pl.BlockSpec(memory_space=pl.ANY)
    near = pl.BlockSpec(memory_space=pltpu.VMEM)
    buf = pltpu.VMEM
    own, near_sum, far_sum = pl.pallas_call(
        layer,
        out_shape=[jax.ShapeDtypeStruct((OUT_ROWS, D), BF16)] * 3,
        in_specs=[
            anywhere, near, anywhere, anywhere, anywhere, near, anywhere, anywhere, near, near,
            near, anywhere, anywhere,
        ],
        out_specs=[anywhere] * 3,
        scratch_shapes=[
            buf((NY, TOK, CH), BF16),
            buf((TOK, D), BF16),
            buf((NZ, NX, NC, 32, 2 * CH), BF16),
            buf((NZ, NX, NC, 32, 2 * CH), BF16),
            buf((1, CH, CH), BF16),
            buf((2, 4, 128, 128), BF16),
            buf((2, 4, 128, 128), BF16),
            buf((2, TOK, 128), F32),
            buf((TOK, EXT), BF16),
            buf((TOK, 128), F32),
            buf((TOK, CH), BF16),
            buf((4, TOK + 2 * PAD, 128), F32),
            buf((2, PAD, CH), BF16),
            buf((TOK, 128), F32),
            buf((EXT, CH), BF16),
            buf((TOK, CH), BF16),
            buf((4, TOK, 128), F32),
            buf((2, 4, SEGS * STEP, 128), F32),
            buf((2, 4, SEGS * STEP, 128), F32),
            buf((2, 2, SEGS, CH), F32),
            buf((2, 2, SEGS, CH), F32),
            buf((NX * NC, 4, CH), F32),
            buf((NZ, 4, CH), F32),
            buf((TOK, 2 * CH), BF16),
            buf((NY, OUT_ROWS, D), BF16),
            buf((OUT_ROWS, D), BF16),
            buf((OUT_ROWS, D), BF16),
            pltpu.SemaphoreType.DMA((N_SEND,)),
            pltpu.SemaphoreType.DMA((N_RECV,)),
            pltpu.SemaphoreType.DMA((N_LOCAL,)),
        ],
        compiler_params=pltpu.CompilerParams(
            collective_id=0, has_side_effects=True, vmem_limit_bytes=60 * 1024 * 1024
        ),
        name="layer",
    )(
        tokens, norm_gain.reshape(1, D), w_pool_in, w_lru_in, pool_mix, conv_taps, rec_gate,
        in_gate, decay_rate, log_decay, start_state, w_out_pool.T, w_out_lru.T,
    )
    total = own.astype(F32) + near_sum.astype(F32) + far_sum.astype(F32)
    return total.astype(BF16)


def solution(mesh):
    torus = Mesh(mesh.devices.reshape(NZ, NX, NC, mesh.shape["tp"]), SP_TP)
    in_specs = (
        P(SP, "tp"),
        P(),
        P(SP, "tp"),
        P(SP, "tp"),
        P("tp", None, None),
        P(None, "tp"),
        P(None, "tp", None, None),
        P(None, "tp", None, None),
        P(None, "tp"),
        P(None, SP),
        P(None, "tp"),
        P("tp", SP),
        P("tp", SP),
    )
    return jax.shard_map(
        per_device, mesh=torus, in_specs=in_specs, out_specs=P(SP_TP, None), check_vma=False
    )
```

```python
import functools

import jax
import jax.numpy as jnp
from jax import lax
from jax.experimental import pallas as pl
from jax.experimental.pallas import tpu as pltpu
from jax.sharding import Mesh
from jax.sharding import PartitionSpec as P

GRID_W = 32
REACH = 8
EPS = 1e-06
SP = ("sp_0", "sp_1", "sp_2")
SP_TP = ("sp_0", "sp_1", "sp_2", "tp")
NZ, NX, NC, NY = 8, 4, 2, 4
TOK = 384
D = 2048
CH = 512
SEGS = 8
SEG = TOK // SEGS
STEP = SEG + 1
OWN = REACH * GRID_W
EXT = TOK + 2 * OWN
PAD = 16
OUT_ROWS = TOK // NY
N_SEND = 19
N_RECV = 123
N_LOCAL = 8
F32 = jnp.float32
BF16 = jnp.bfloat16
NT = (((1,), (1,)), ((), ()))


class Links:
    def __init__(self, send, recv):
        self.send, self.recv, self.groups, self.used = send, recv, [], 0

    def slot(self):
        self.used += 1
        return self.used - 1

    def group(self, region):
        self.groups.append(region)
        return len(self.groups) - 1

    def copy(self, src, dst, group, slot, dev):
        return pltpu.make_async_remote_copy(
            src_ref=src,
            dst_ref=dst,
            send_sem=self.send.at[group],
            recv_sem=self.recv.at[slot],
            device_id=dev,
            device_id_type=pl.DeviceIdType.MESH,
        )

    def put(self, src, dst, group, slot, **dev):
        self.copy(src, dst, group, slot, dev).start()

    def got(self, region, slot, **dev):
        self.copy(region, region, 0, slot, dev).wait_recv()

    def drain(self, **dev):
        for group, region in enumerate(self.groups):
            self.copy(region, region, group, 0, dev).wait_send()


def weight_gather(links, buf, z, x, c, by_row):
    lo, hi = pl.ds(0, 16), pl.ds(16, 16)

    def zz(d):
        return lax.rem(z + (d + NZ), NZ)

    def xx(d):
        return lax.rem(x + (d + NX), NX)

    other = {"sp_2": 1 - c}
    both = (1, -1)
    rel = [0, -1, 1, -2, 2, -3, 3, 4]
    a1 = {dx: links.slot() for dx in (1, 3, 2)}
    a2 = {
        (s, k, e): links.slot()
        for s in both
        for e in range(NX)
        for k in range(1, 5 if (s == 1) == (e < 2) else 4)
    }
    b1 = {(s, k): links.slot() for s in both for k in range(1, 5 if s == 1 else 4)}
    b2 = {d: links.slot() for d in rel}
    dd = {d: links.slot() for d in rel} if by_row else dict.fromkeys(rel, links.slot())
    g_a1 = links.group(buf.at[0, pl.ds(0, 3), c, lo])
    g_a2 = links.group(buf.at[pl.ds(0, 7), pl.ds(0, NX), c, lo])
    g_b1 = links.group(buf.at[pl.ds(0, 7), 0, c, lo])
    g_b2 = links.group(buf.at[pl.ds(0, NZ), pl.ds(0, 3), c, lo])
    g_dd = links.group(buf.at[pl.ds(0, NZ), pl.ds(0, NX), c])

    def a_send(s, k, e):
        if (s, k, e) in a2:
            piece = buf.at[zz(-s * (k - 1)), xx(e), c, lo]
            links.put(piece, piece, g_a2, a2[s, k, e], sp_0=zz(s))

    def a_hop(s, k, e):
        if (s, k, e) in a2:
            links.got(buf.at[zz(-s * k), xx(e), c, lo], a2[s, k, e], sp_0=zz(s))
            a_send(s, k + 1, e)

    def a_side(dx):
        links.got(buf.at[z, xx(-dx), c, lo], a1[dx], sp_1=xx(dx))
        for s in both:
            a_send(s, 1, NX - dx)

    def b_send(s, k):
        if (s, k) in b1:
            piece = buf.at[zz(-s * (k - 1)), x, c, hi]
            links.put(piece, piece, g_b1, b1[s, k], sp_0=zz(s))

    def b_spread(d):
        piece = buf.at[zz(d), x, c, hi]
        for dx in (1, 3, 2):
            links.put(piece, piece, g_b2, b2[d], sp_1=xx(dx))

    def b_hop(s, k):
        if (s, k) in b1:
            links.got(buf.at[zz(-s * k), x, c, hi], b1[s, k], sp_0=zz(s))
            b_send(s, k + 1)
            b_spread(-s * k if k < 4 else 4)

    def row_done(d):
        links.got(buf.at[zz(d), pl.ds(0, 3), c, hi], b2[d], sp_1=xx(1))
        row = buf.at[zz(d), pl.ds(0, NX), c]
        links.put(row, row, g_dd, dd[d], **other)

    def first():
        own = buf.at[z, x, c, lo]
        for dx in (1, 3, 2):
            links.put(own, own, g_a1, a1[dx], sp_1=xx(dx))
        for s in both:
            b_send(s, 1)
            a_send(s, 1, 0)

    def arrived(d):
        of = zz(d) if by_row else pl.ds(0, NZ)
        links.got(buf.at[of, pl.ds(0, NX), 1 - c], dd[d], **other)

    def at(f, *args):
        return functools.partial(f, *args)

    along_b = [[at(b_spread, 0)]] + [[at(b_hop, s, k) for s in both] for k in range(1, 5)]
    along_a = [[first], [at(a_side, 1), at(a_side, 3)]]
    along_a[1] += [at(a_hop, s, 1, 0) for s in both] + [at(a_side, 2)]
    for k in range(2, 6):
        along_a.append(
            [at(a_hop, s, k, 0) for s in both]
            + [at(a_hop, s, k - 1, e) for e in (3, 1, 2) for s in both]
        )
    rows = [[at(row_done, d) for d in ds] for ds in ((0,), (-1, 1), (-2, 2), (-3, 3), (4,))]
    return along_a, along_b, rows, arrived


def logistic(v):
    return 1.0 / (1.0 + jnp.exp(-v))


def one_minus_exp(y, e):
    series = y * (-1.0 / 720.0) - 1.0 / 120.0
    for n in (24.0, 6.0, 2.0, 1.0):
        series = y * series - 1.0 / n
    return jnp.where(y > -0.125, y * series, 1.0 - e)


def root(v):
    return v * lax.rsqrt(jnp.maximum(v, 1e-37))


def layer(
    tokens, gain, wpi, wli, pmix, taps, rgate, igate, decay, logd, start, wop, wol, own, rs1, rs3,
    tok, nrm, win, wout, pmv, rgv, igv, ldb, box, rcp, ulb, ulf, hb, cvb, pext, pdf, gs, aa, bb,
    sg, ex, c1, c2, ycat, part, rs2, mg, send, recv, local,
):
    z, x, c = (lax.axis_index(n) for n in SP)
    y = lax.axis_index("tp")
    s = (z * NX + x) * NC + c
    links = Links(send, recv)

    def zz(d):
        return lax.rem(z + (d + NZ), NZ)

    def xx(d):
        return lax.rem(x + (d + NX), NX)

    def yy(d):
        return lax.rem(y + (d + NY), NY)

    def run_dev(d):
        t = lax.rem(s + (d + NZ * NX * NC), NZ * NX * NC)
        return {"sp_0": t // (NX * NC), "sp_1": lax.rem(t // NC, NX), "sp_2": lax.rem(t, NC)}

    after, before = run_dev(1), run_dev(-1)

    loads = [
        pltpu.make_async_copy(tokens, tok.at[y], local.at[0]),
        pltpu.make_async_copy(wpi, win.at[z, x, c, :, pl.ds(0, CH)], local.at[1]),
        pltpu.make_async_copy(wli, win.at[z, x, c, :, pl.ds(CH, CH)], local.at[2]),
        pltpu.make_async_copy(pmix, pmv, local.at[3]),
        pltpu.make_async_copy(rgate, rgv, local.at[4]),
        pltpu.make_async_copy(igate, igv, local.at[5]),
        pltpu.make_async_copy(wop, wout.at[z, x, c, :, pl.ds(0, CH)], local.at[6]),
        pltpu.make_async_copy(wol, wout.at[z, x, c, :, pl.ds(CH, CH)], local.at[7]),
    ]
    for load in loads:
        load.start()

    barrier = pltpu.get_barrier_semaphore()
    peers = [{"tp": yy(1)}, {"tp": yy(-1)}, after, before]
    peers += [{"sp_0": zz(d)} for d in range(1, NZ)]
    around = [(dx, dc) for dx in range(NX) for dc in range(NC) if dx or dc]
    for dx, dc in around:
        peers.append({"sp_1": xx(dx), "sp_2": lax.rem(c + dc, NC)})
    for peer in peers:
        pl.semaphore_signal(barrier, inc=1, device_id=peer, device_id_type=pl.DeviceIdType.MESH)

    for d in range(2):
        for i in range(TOK // 128):
            rows = slice(i * 128, (i + 1) * 128)
            ldb[d, rows, :] = jnp.broadcast_to(logd[d : d + 1, rows], (128, 128)).T
    half = lax.shift_left(jnp.int32(1), y)
    grid_rows = TOK // GRID_W
    row_count = grid_rows * NZ * NX * NC
    first_row = s * grid_rows

    def boxes(i, _):
        at = pl.multiple_of(i * 32, 32)
        er = lax.shift_right_logical(lax.broadcasted_iota(jnp.int32, (32, EXT), 1), 5)
        ec = lax.broadcasted_iota(jnp.int32, (32, EXT), 1) & (GRID_W - 1)
        col = lax.broadcasted_iota(jnp.int32, (32, EXT), 0)
        low = jnp.maximum(i - half, -first_row) + REACH
        high = jnp.minimum(i + half, row_count - first_row) + REACH
        inside = (er >= low) & (er < high) & (ec >= col - half) & (ec < col + half)
        box[pl.ds(at, 32), :] = jnp.where(inside, 1.0, 0.0).astype(BF16)
        cc = lax.broadcasted_iota(jnp.int32, (32, 128), 0)
        cols = jnp.minimum(cc + half, GRID_W) - jnp.maximum(cc - half, 0)
        rcp[pl.ds(at, 32), :] = 1.0 / (cols * (high - low)).astype(F32)
        return 0

    lax.fori_loop(0, grid_rows, boxes, 0)

    pl.semaphore_wait(barrier, len(peers))
    for load in loads[:3] + loads[6:]:
        load.wait()

    halves = (pl.ds(0, TOK // 2), pl.ds(TOK // 2, TOK // 2))
    g_t1 = links.group(tok.at[pl.ds(0, 2)])
    g_t2 = links.group(tok.at[0])
    t1 = {(d, h): links.slot() for d in (1, -1) for h in (0, 1)}
    t2 = {d: links.slot() for d in (1, -1)}
    for i in (0, 1):
        for d in (1, -1):
            h = i if d == 1 else 1 - i
            piece = tok.at[y, halves[h]]
            links.put(piece, piece, g_t1, t1[d, h], tp=yy(d))
    in_a, in_b, in_rows, in_arrived = weight_gather(links, win, z, x, c, False)
    out_a, out_b, out_rows, out_arrived = weight_gather(links, wout, z, x, c, True)

    def serve(*rounds):
        for turn in rounds:
            for step in turn:
                step()

    serve(in_a[0], in_b[0], out_a[0])

    def token_relay():
        for d, h in ((1, 0), (-1, 1)):
            piece = tok.at[yy(-d), halves[h]]
            links.got(piece, t1[d, h], tp=yy(d))
            links.put(piece, piece, g_t2, t2[d], tp=yy(d))

    serve(in_a[1][:2], in_b[1], in_a[1][2:])
    serve(in_b[2], in_a[2], in_rows[0])
    token_relay()
    serve(out_b[0])
    serve(in_b[3], in_a[3], in_rows[1])
    serve(in_b[4], in_a[4], in_rows[2])
    serve(out_b[1], out_a[1])
    serve(in_a[5], in_rows[3], in_rows[4])
    for d, h in ((1, 1), (-1, 0)):
        links.got(tok.at[yy(-d), halves[h]], t1[d, h], tp=yy(d))
    for d, h in ((1, 0), (-1, 1)):
        links.got(tok.at[yy(2), halves[h]], t2[d], tp=yy(d))

    def norm(i, _):
        rows = pl.ds(pl.multiple_of(i * 32, 32), 32)
        total = jnp.zeros((32, 1), F32)
        for k in range(NY):
            v = tok[k, rows, :].astype(F32)
            total = total + jnp.sum(v * v, axis=1, keepdims=True)
        scale = lax.rsqrt(total * (1.0 / D) + EPS)
        for k in range(NY):
            cols = slice(k * CH, (k + 1) * CH)
            v = tok[k, rows, :].astype(F32)
            nrm[rows, cols] = (v * scale * gain[:, cols]).astype(BF16)
        return 0

    serve(out_b[2])
    lax.fori_loop(0, TOK // 32, norm, 0)
    in_arrived(0)

    def project(col):
        w = win[:, :, :, :, col : col + 256].reshape(D, 256)
        return jnp.dot(nrm[...], w, preferred_element_type=F32).astype(BF16)

    for n in range(2):
        u = project(CH + n * 256)
        ulb[:, n * 256 : (n + 1) * 256] = u
        for k in range(2):
            ulf[2 * n + k, PAD : PAD + TOK, :] = u[:, k * 128 : (k + 1) * 128].astype(F32)
    g_ch = links.group(hb)
    ch = {d: links.slot() for d in (1, -1)}
    links.put(ulb.at[pl.ds(TOK - PAD, PAD)], hb.at[0], g_ch, ch[1], **after)
    links.put(ulb.at[pl.ds(0, PAD)], hb.at[1], g_ch, ch[-1], **before)
    serve(out_b[3], out_a[2])
    for n in range(2):
        pext[OWN : OWN + TOK, n * 256 : (n + 1) * 256] = project(n * 256)
    g_ph = links.group(pext.at[pl.ds(0, 2 * OWN)])
    ph = {d: links.slot() for d in (1, -1)}
    links.put(pext.at[pl.ds(TOK, OWN)], pext.at[pl.ds(0, OWN)], g_ph, ph[1], **after)
    links.put(pext.at[pl.ds(OWN, OWN)], pext.at[pl.ds(OWN + TOK, OWN)], g_ph, ph[-1], **before)

    serve(out_rows[0])
    links.got(hb.at[0], ch[1], **after)
    links.got(hb.at[1], ch[-1], **before)
    has_before = jnp.where(s > 0, 1.0, 0.0).astype(F32)
    has_after = jnp.where(s < NZ * NX * NC - 1, 1.0, 0.0).astype(F32)
    for b in range(4):
        lanes = slice(b * 128, (b + 1) * 128)
        ulf[b, 0:PAD, :] = hb[0, :, lanes].astype(F32) * has_before
        ulf[b, PAD + TOK :, :] = hb[1, :, lanes].astype(F32) * has_after
    for load in loads[4:6]:
        load.wait()

    def block(b):
        lanes = slice(b * 128, (b + 1) * 128)
        tap = taps[:, lanes].astype(F32)
        acc = ulf[b, PAD - 2 : PAD - 2 + TOK, :] * tap[0:1]
        for k in range(1, 4):
            acc = acc + ulf[b, PAD - 2 + k : PAD - 2 + k + TOK, :] * tap[k : k + 1]
        conv = acc.astype(BF16)
        cvb[...] = conv.astype(F32)
        for d in range(2):
            gs[2 * d] = jnp.dot(conv, rgv[d, b], preferred_element_type=F32)
            gs[2 * d + 1] = jnp.dot(conv, igv[d, b], preferred_element_type=F32)

        for j in range(SEGS):
            rows, padded = slice(j * SEG, (j + 1) * SEG), slice(j * STEP, j * STEP + SEG)
            value = cvb[rows, :]
            for d in range(2):
                rate = logistic(gs[2 * d, rows, :])
                gate = logistic(gs[2 * d + 1, rows, :])
                keep_log = -8.0 * rate * decay[d : d + 1, lanes] + ldb[d, rows, :]
                keep = jnp.exp(keep_log)
                rest = one_minus_exp(2.0 * keep_log, keep * keep)
                aa[d, b, padded, :] = keep
                bb[d, b, padded, :] = root(rest) * gate * value

    block(0)
    block(1)
    block(2)
    block(3)

    def scan_step(t, carry):
        new = []
        for d in range(2):
            at = pl.ds(t if d == 0 else SEG - 1 - t, SEGS, stride=STEP)
            for b in range(4):
                prod, state = carry[2 * (4 * d + b)], carry[2 * (4 * d + b) + 1]
                keep = aa[d, b, at, :]
                state = keep * state + bb[d, b, at, :]
                prod = prod * keep
                aa[d, b, at, :] = prod
                bb[d, b, at, :] = state
                new += [prod, state]
        return tuple(new)

    ones, zeros = jnp.ones((SEGS, 128), F32), jnp.zeros((SEGS, 128), F32)
    ends = lax.fori_loop(0, SEG, scan_step, (ones, zeros) * 8, unroll=2)
    for d in range(2):
        for b in range(4):
            for k in range(2):
                sg[k, d, :, b * 128 : (b + 1) * 128] = ends[2 * (4 * d + b) + k]
    me = x * NC + c
    for d in range(2):
        prod, state = jnp.ones((1, CH), F32), jnp.zeros((1, CH), F32)
        for j in range(SEGS) if d == 0 else reversed(range(SEGS)):
            ex[0, d, j : j + 1, :] = prod
            ex[1, d, j : j + 1, :] = state
            keep = sg[0, d, j : j + 1, :]
            state = keep * state + sg[1, d, j : j + 1, :]
            prod = prod * keep
        c1[me, 2 * d : 2 * d + 1, :] = prod
        c1[me, 2 * d + 1 : 2 * d + 2, :] = state
    g_k1, k1 = links.group(c1.at[pl.ds(0, 7)]), links.slot()
    for dx, dc in around:
        links.put(c1.at[me], c1.at[me], g_k1, k1, sp_1=xx(dx), sp_2=lax.rem(c + dc, NC))

    serve(out_b[4], out_a[3])

    def combine(table, mine):
        full, inside = [], []
        for d in range(2):
            count = NZ
            prod, state = jnp.ones((1, CH), F32), jnp.zeros((1, CH), F32)
            in_p, in_s = prod, state
            for k in range(count) if d == 0 else reversed(range(count)):
                keep = table[k, 2 * d : 2 * d + 1, :]
                state = keep * state + table[k, 2 * d + 1 : 2 * d + 2, :]
                prod = prod * keep
                passed = (k < mine) if d == 0 else (k > mine)
                in_p = jnp.where(passed, prod, in_p)
                in_s = jnp.where(passed, state, in_s)
            full.append((prod, state))
            inside.append((in_p, in_s))
        return full, inside

    def pooled(n):
        cols = slice(n * 256, (n + 1) * 256)
        total = jnp.dot(box[...], pext[:, cols], preferred_element_type=F32)
        own = pext[OWN : OWN + TOK, cols].astype(F32)
        scale = jnp.concatenate([rcp[...], rcp[...]], axis=1)
        pdf[:, cols] = (total * scale - own).astype(BF16)

    links.got(c1.at[pl.ds(0, 7)], k1, **after)
    full, near = combine(c1, me)
    for d in range(2):
        c2[z, 2 * d : 2 * d + 1, :] = full[d][0]
        c2[z, 2 * d + 1 : 2 * d + 2, :] = full[d][1]
    g_k2, k2 = links.group(c2.at[pl.ds(0, 7)]), links.slot()
    for d in range(1, NZ):
        links.put(c2.at[z], c2.at[z], g_k2, k2, sp_0=zz(d))

    serve(out_rows[1], out_rows[2], out_a[4])
    loads[3].wait()
    links.got(pext.at[pl.ds(0, OWN)], ph[1], **after)
    links.got(pext.at[pl.ds(OWN + TOK, OWN)], ph[-1], **before)
    for n in range(2):
        pooled(n)
    for n in range(2):
        cols = slice(n * 256, (n + 1) * 256)
        ycat[:, cols] = jnp.dot(pdf[...], pmv[0, :, cols], preferred_element_type=F32).astype(BF16)

    serve(out_rows[3])
    links.got(c2.at[pl.ds(0, 7)], k2, **after)
    _, far = combine(c2, z)
    for d in range(2):
        (np_, ns_), (fp_, fs_) = near[d], far[d]
        enter = np_ * fs_ + ns_ + (np_ * fp_) * start[d : d + 1, :]
        ex[0, d] = ex[1, d] + ex[0, d] * enter
    for j in range(SEGS):
        rows, padded = slice(j * SEG, (j + 1) * SEG), slice(j * STEP, j * STEP + SEG)
        for b in range(4):
            lanes = slice(b * 128, (b + 1) * 128)
            h0 = bb[0, b, padded, :] + aa[0, b, padded, :] * ex[0, 0, j : j + 1, lanes]
            h1 = bb[1, b, padded, :] + aa[1, b, padded, :] * ex[0, 1, j : j + 1, lanes]
            ycat[rows, CH + b * 128 : CH + (b + 1) * 128] = (h0 + h1).astype(BF16)
    g_q1, g_q2, g_q3 = links.group(rs1), links.group(rs2), links.group(rs3)
    q1, q3 = links.slot(), links.slot()
    q2 = [links.slot() for _ in range(NZ)]

    def tile(n):
        turn = (0, -1, 1, -2, 2, -3, 3, 4)[n]
        return pl.ds(pl.multiple_of(zz(turn) * 256, 256), 256)

    def relay(n):
        cols = slice(n * 256, (n + 1) * 256)
        d = 1 if n % 2 == 0 else -1
        at = rs2.at[:, pl.ds(n * 256, 256)]
        links.got(at, q2[n], tp=yy(d))
        mg[:, cols] = (rs2[:, cols].astype(F32) + part[yy(d), :, cols].astype(F32)).astype(BF16)
        there = pl.ds(n * 256, 256)
        links.put(mg.at[:, there], rs3.at[:, tile(n)], g_q3, q3, tp=yy(d))

    for n, turn in enumerate((0, -1, 1, -2, 2, -3, 3, 4)):
        cols = slice(n * 256, (n + 1) * 256)
        here = pl.ds(n * 256, 256)
        out_arrived(turn)
        w = wout[zz(turn)].reshape(256, 2 * CH)
        acc = lax.dot_general(ycat[...], w, NT, preferred_element_type=F32)
        for k in range(NY):
            part[k, :, cols] = acc[k * OUT_ROWS : (k + 1) * OUT_ROWS].astype(BF16)
        d = 1 if n % 2 == 0 else -1
        links.put(part.at[yy(2), :, here], rs2.at[:, here], g_q2, q2[n], tp=yy(d))
        links.put(part.at[yy(-d), :, here], rs1.at[:, tile(n)], g_q1, q1, tp=yy(-d))
        pltpu.make_async_copy(part.at[y, :, here], own.at[:, tile(n)], local.at[0]).start()
        if n == 2:
            serve(out_a[5], out_rows[4])
        if n >= 5:
            relay(n - 5)
    for n in range(3, NZ):
        relay(n)
    links.got(rs1, q1, **after)
    links.got(rs3, q3, **after)
    pltpu.make_async_copy(rs1, own, local.at[0]).wait()
    links.drain(**after)


def per_device(
    tokens, norm_gain, w_pool_in, w_lru_in, pool_mix, conv_taps, rec_gate, in_gate, decay_rate,
    log_decay, start_state, w_out_pool, w_out_lru,
):
    anywhere = pl.BlockSpec(memory_space=pl.ANY)
    near = pl.BlockSpec(memory_space=pltpu.VMEM)
    buf = pltpu.VMEM
    own, near_sum, far_sum = pl.pallas_call(
        layer,
        out_shape=[jax.ShapeDtypeStruct((OUT_ROWS, D), BF16)] * 3,
        in_specs=[
            anywhere, near, anywhere, anywhere, anywhere, near, anywhere, anywhere, near, near,
            near, anywhere, anywhere,
        ],
        out_specs=[anywhere] * 3,
        scratch_shapes=[
            buf((NY, TOK, CH), BF16),
            buf((TOK, D), BF16),
            buf((NZ, NX, NC, 32, 2 * CH), BF16),
            buf((NZ, NX, NC, 32, 2 * CH), BF16),
            buf((1, CH, CH), BF16),
            buf((2, 4, 128, 128), BF16),
            buf((2, 4, 128, 128), BF16),
            buf((2, TOK, 128), F32),
            buf((TOK, EXT), BF16),
            buf((TOK, 128), F32),
            buf((TOK, CH), BF16),
            buf((4, TOK + 2 * PAD, 128), F32),
            buf((2, PAD, CH), BF16),
            buf((TOK, 128), F32),
            buf((EXT, CH), BF16),
            buf((TOK, CH), BF16),
            buf((4, TOK, 128), F32),
            buf((2, 4, SEGS * STEP, 128), F32),
            buf((2, 4, SEGS * STEP, 128), F32),
            buf((2, 2, SEGS, CH), F32),
            buf((2, 2, SEGS, CH), F32),
            buf((NX * NC, 4, CH), F32),
            buf((NZ, 4, CH), F32),
            buf((TOK, 2 * CH), BF16),
            buf((NY, OUT_ROWS, D), BF16),
            buf((OUT_ROWS, D), BF16),
            buf((OUT_ROWS, D), BF16),
            pltpu.SemaphoreType.DMA((N_SEND,)),
            pltpu.SemaphoreType.DMA((N_RECV,)),
            pltpu.SemaphoreType.DMA((N_LOCAL,)),
        ],
        compiler_params=pltpu.CompilerParams(
            collective_id=0, has_side_effects=True, vmem_limit_bytes=60 * 1024 * 1024
        ),
        name="layer",
    )(
        tokens, norm_gain.reshape(1, D), w_pool_in, w_lru_in, pool_mix, conv_taps, rec_gate,
        in_gate, decay_rate, log_decay, start_state, w_out_pool.T, w_out_lru.T,
    )
    total = own.astype(F32) + near_sum.astype(F32) + far_sum.astype(F32)
    return total.astype(BF16)


def solution(mesh):
    torus = Mesh(mesh.devices.reshape(NZ, NX, NC, mesh.shape["tp"]), SP_TP)
    in_specs = (
        P(SP, "tp"),
        P(),
        P(SP, "tp"),
        P(SP, "tp"),
        P("tp", None, None),
        P(None, "tp"),
        P(None, "tp", None, None),
        P(None, "tp", None, None),
        P(None, "tp"),
        P(None, SP),
        P(None, "tp"),
        P("tp", SP),
        P("tp", SP),
    )
    return jax.shard_map(
        per_device, mesh=torus, in_specs=in_specs, out_specs=P(SP_TP, None), check_vma=False
    )
```

```python
import functools

import jax
import jax.numpy as jnp
from jax import lax
from jax.experimental import pallas as pl
from jax.experimental.pallas import tpu as pltpu
from jax.sharding import Mesh
from jax.sharding import PartitionSpec as P

GRID_W = 32
REACH = 8
EPS = 1e-06
SP = ("sp_0", "sp_1", "sp_2")
SP_TP = ("sp_0", "sp_1", "sp_2", "tp")
NZ, NX, NC, NY = 8, 4, 2, 4
TOK = 384
D = 2048
CH = 512
SEGS = 8
SEG = TOK // SEGS
STEP = SEG + 1
OWN = REACH * GRID_W
EXT = TOK + 2 * OWN
PAD = 16
OUT_ROWS = TOK // NY
N_SEND = 20
N_RECV = 124
N_LOCAL = 8
F32 = jnp.float32
BF16 = jnp.bfloat16
NT = (((1,), (1,)), ((), ()))


class Links:
    def __init__(self, send, recv):
        self.send, self.recv, self.groups, self.used = send, recv, [], 0

    def slot(self):
        self.used += 1
        return self.used - 1

    def group(self, region):
        self.groups.append(region)
        return len(self.groups) - 1

    def copy(self, src, dst, group, slot, dev):
        return pltpu.make_async_remote_copy(
            src_ref=src,
            dst_ref=dst,
            send_sem=self.send.at[group],
            recv_sem=self.recv.at[slot],
            device_id=dev,
            device_id_type=pl.DeviceIdType.MESH,
        )

    def put(self, src, dst, group, slot, **dev):
        self.copy(src, dst, group, slot, dev).start()

    def got(self, region, slot, **dev):
        self.copy(region, region, 0, slot, dev).wait_recv()

    def drain(self, **dev):
        for group, region in enumerate(self.groups):
            self.copy(region, region, group, 0, dev).wait_send()


def weight_gather(links, buf, z, x, c, by_row):
    lo, hi = pl.ds(0, 16), pl.ds(16, 16)

    def zz(d):
        return lax.rem(z + (d + NZ), NZ)

    def xx(d):
        return lax.rem(x + (d + NX), NX)

    other = {"sp_2": 1 - c}
    both = (1, -1)
    rel = [0, -1, 1, -2, 2, -3, 3, 4]
    a1 = {dx: links.slot() for dx in (1, 3, 2)}
    a2 = {
        (s, k, e): links.slot()
        for s in both
        for e in range(NX)
        for k in range(1, 5 if (s == 1) == (e < 2) else 4)
    }
    b1 = {(s, k): links.slot() for s in both for k in range(1, 5 if s == 1 else 4)}
    b2 = {d: links.slot() for d in rel}
    dd = {d: links.slot() for d in rel} if by_row else dict.fromkeys(rel, links.slot())
    g_a1 = links.group(buf.at[0, pl.ds(0, 3), c, lo])
    g_a2 = links.group(buf.at[pl.ds(0, 7), pl.ds(0, NX), c, lo])
    g_b1 = links.group(buf.at[pl.ds(0, 7), 0, c, lo])
    g_b2 = links.group(buf.at[pl.ds(0, NZ), pl.ds(0, 3), c, lo])
    g_dd = links.group(buf.at[pl.ds(0, NZ), pl.ds(0, NX), c])

    def a_send(s, k, e):
        if (s, k, e) in a2:
            piece = buf.at[zz(-s * (k - 1)), xx(e), c, lo]
            links.put(piece, piece, g_a2, a2[s, k, e], sp_0=zz(s))

    def a_hop(s, k, e):
        if (s, k, e) in a2:
            links.got(buf.at[zz(-s * k), xx(e), c, lo], a2[s, k, e], sp_0=zz(s))
            a_send(s, k + 1, e)

    def a_side(dx):
        links.got(buf.at[z, xx(-dx), c, lo], a1[dx], sp_1=xx(dx))
        for s in both:
            a_send(s, 1, NX - dx)

    def b_send(s, k):
        if (s, k) in b1:
            piece = buf.at[zz(-s * (k - 1)), x, c, hi]
            links.put(piece, piece, g_b1, b1[s, k], sp_0=zz(s))

    def b_spread(d):
        piece = buf.at[zz(d), x, c, hi]
        for dx in (1, 3, 2):
            links.put(piece, piece, g_b2, b2[d], sp_1=xx(dx))

    def b_hop(s, k):
        if (s, k) in b1:
            links.got(buf.at[zz(-s * k), x, c, hi], b1[s, k], sp_0=zz(s))
            b_send(s, k + 1)
            b_spread(-s * k if k < 4 else 4)

    def row_done(d):
        links.got(buf.at[zz(d), pl.ds(0, 3), c, hi], b2[d], sp_1=xx(1))
        row = buf.at[zz(d), pl.ds(0, NX), c]
        links.put(row, row, g_dd, dd[d], **other)

    def first():
        own = buf.at[z, x, c, lo]
        for dx in (1, 3, 2):
            links.put(own, own, g_a1, a1[dx], sp_1=xx(dx))
        for s in both:
            b_send(s, 1)
            a_send(s, 1, 0)

    def arrived(d):
        of = zz(d) if by_row else pl.ds(0, NZ)
        links.got(buf.at[of, pl.ds(0, NX), 1 - c], dd[d], **other)

    def at(f, *args):
        return functools.partial(f, *args)

    along_b = [[at(b_spread, 0)]] + [[at(b_hop, s, k) for s in both] for k in range(1, 5)]
    along_a = [[first], [at(a_side, 1), at(a_side, 3)]]
    along_a[1] += [at(a_hop, s, 1, 0) for s in both] + [at(a_side, 2)]
    for k in range(2, 6):
        along_a.append(
            [at(a_hop, s, k, 0) for s in both]
            + [at(a_hop, s, k - 1, e) for e in (3, 1, 2) for s in both]
        )
    rows = [[at(row_done, d) for d in ds] for ds in ((0,), (-1, 1), (-2, 2), (-3, 3), (4,))]
    return along_a, along_b, rows, arrived


def logistic(v):
    return 1.0 / (1.0 + jnp.exp(-v))


def one_minus_exp(y, e):
    series = y * (-1.0 / 720.0) - 1.0 / 120.0
    for n in (24.0, 6.0, 2.0, 1.0):
        series = y * series - 1.0 / n
    return jnp.where(y > -0.125, y * series, 1.0 - e)


def root(v):
    return v * lax.rsqrt(jnp.maximum(v, 1e-37))


def layer(
    tokens, gain, wpi, wli, pmix, taps, rgate, igate, decay, logd, start, wop, wol, own, rs1, rs3,
    tok, nrm, win, wout, pmv, rgv, igv, ldb, box, rcp, ulf, hal, cvb, pext, pdf, gs, aa, bb,
    sg, ex, c1, c2, ycat, part, rs2, mg, send, recv, local,
):
    z, x, c = (lax.axis_index(n) for n in SP)
    y = lax.axis_index("tp")
    s = (z * NX + x) * NC + c
    links = Links(send, recv)

    def zz(d):
        return lax.rem(z + (d + NZ), NZ)

    def xx(d):
        return lax.rem(x + (d + NX), NX)

    def yy(d):
        return lax.rem(y + (d + NY), NY)

    def run_dev(d):
        t = lax.rem(s + (d + NZ * NX * NC), NZ * NX * NC)
        return {"sp_0": t // (NX * NC), "sp_1": lax.rem(t // NC, NX), "sp_2": lax.rem(t, NC)}

    after, before = run_dev(1), run_dev(-1)

    loads = [
        pltpu.make_async_copy(tokens, tok.at[y], local.at[0]),
        pltpu.make_async_copy(wpi, win.at[z, x, c, :, pl.ds(0, CH)], local.at[1]),
        pltpu.make_async_copy(wli, win.at[z, x, c, :, pl.ds(CH, CH)], local.at[2]),
        pltpu.make_async_copy(pmix, pmv, local.at[3]),
        pltpu.make_async_copy(rgate, rgv, local.at[4]),
        pltpu.make_async_copy(igate, igv, local.at[5]),
        pltpu.make_async_copy(wop, wout.at[z, x, c, :, pl.ds(0, CH)], local.at[6]),
        pltpu.make_async_copy(wol, wout.at[z, x, c, :, pl.ds(CH, CH)], local.at[7]),
    ]
    for load in loads:
        load.start()

    barrier = pltpu.get_barrier_semaphore()
    peers = [{"tp": yy(1)}, {"tp": yy(-1)}, {"tp": yy(2)}, after, before]
    peers += [{"sp_0": zz(d)} for d in range(1, NZ)]
    around = [(dx, dc) for dx in range(NX) for dc in range(NC) if dx or dc]
    for dx, dc in around:
        peers.append({"sp_1": xx(dx), "sp_2": lax.rem(c + dc, NC)})
    for peer in peers:
        pl.semaphore_signal(barrier, inc=1, device_id=peer, device_id_type=pl.DeviceIdType.MESH)

    for d in range(2):
        for i in range(TOK // 128):
            rows = slice(i * 128, (i + 1) * 128)
            ldb[d, rows, :] = jnp.broadcast_to(logd[d : d + 1, rows], (128, 128)).T
    half = lax.shift_left(jnp.int32(1), y)
    grid_rows = TOK // GRID_W
    row_count = grid_rows * NZ * NX * NC
    first_row = s * grid_rows

    def boxes(i, _):
        at = pl.multiple_of(i * 32, 32)
        er = lax.shift_right_logical(lax.broadcasted_iota(jnp.int32, (32, EXT), 1), 5)
        ec = lax.broadcasted_iota(jnp.int32, (32, EXT), 1) & (GRID_W - 1)
        col = lax.broadcasted_iota(jnp.int32, (32, EXT), 0)
        low = jnp.maximum(i - half, -first_row) + REACH
        high = jnp.minimum(i + half, row_count - first_row) + REACH
        inside = (er >= low) & (er < high) & (ec >= col - half) & (ec < col + half)
        box[pl.ds(at, 32), :] = jnp.where(inside, 1.0, 0.0).astype(BF16)
        cc = lax.broadcasted_iota(jnp.int32, (32, 128), 0)
        cols = jnp.minimum(cc + half, GRID_W) - jnp.maximum(cc - half, 0)
        rcp[pl.ds(at, 32), :] = 1.0 / (cols * (high - low)).astype(F32)
        return 0

    lax.fori_loop(0, grid_rows, boxes, 0)

    pl.semaphore_wait(barrier, len(peers))
    for load in loads[:3] + loads[6:]:
        load.wait()

    halves = (pl.ds(0, TOK // 2), pl.ds(TOK // 2, TOK // 2))
    g_t1 = links.group(tok.at[pl.ds(0, 2)])
    g_t2 = links.group(tok.at[0])
    t1 = {(d, h): links.slot() for d in (1, -1) for h in (0, 1)}
    t2 = {d: links.slot() for d in (1, -1)}
    for i in (0, 1):
        for d in (1, -1):
            h = i if d == 1 else 1 - i
            piece = tok.at[y, halves[h]]
            links.put(piece, piece, g_t1, t1[d, h], tp=yy(d))
    g_ch, g_hs = links.group(hal.at[0]), links.group(hal.at[pl.ds(0, 3)])
    ch, hs = {d: links.slot() for d in (1, -1)}, links.slot()
    links.put(tok.at[y, pl.ds(TOK - PAD, PAD)], hal.at[y, 0], g_ch, ch[1], **after)
    links.put(tok.at[y, pl.ds(0, PAD)], hal.at[y, 1], g_ch, ch[-1], **before)
    in_a, in_b, in_rows, in_arrived = weight_gather(links, win, z, x, c, False)
    out_a, out_b, out_rows, out_arrived = weight_gather(links, wout, z, x, c, True)

    def serve(*rounds):
        for turn in rounds:
            for step in turn:
                step()

    serve(in_a[0], in_b[0], out_a[0])

    def token_relay():
        for d, h in ((1, 0), (-1, 1)):
            piece = tok.at[yy(-d), halves[h]]
            links.got(piece, t1[d, h], tp=yy(d))
            links.put(piece, piece, g_t2, t2[d], tp=yy(d))

    serve(in_a[1][:2], in_b[1], in_a[1][2:])
    links.got(hal.at[y, 0], ch[1], **after)
    links.got(hal.at[y, 1], ch[-1], **before)
    for d in (1, -1, 2):
        links.put(hal.at[y], hal.at[y], g_hs, hs, tp=yy(d))
    serve(in_b[2], in_a[2], in_rows[0])
    token_relay()
    serve(out_b[0])
    serve(in_b[3], in_a[3], in_rows[1])
    serve(in_b[4], in_a[4], in_rows[2])
    serve(out_b[1], out_a[1])
    serve(in_a[5], in_rows[3], in_rows[4])
    for d, h in ((1, 1), (-1, 0)):
        links.got(tok.at[yy(-d), halves[h]], t1[d, h], tp=yy(d))
    for d, h in ((1, 0), (-1, 1)):
        links.got(tok.at[yy(2), halves[h]], t2[d], tp=yy(d))

    links.got(hal.at[pl.ds(0, 3)], hs, tp=yy(1))

    def normed(parts, rows):
        total = jnp.zeros((32, 1), F32)
        for k in range(NY):
            v = parts(k).astype(F32)
            total = total + jnp.sum(v * v, axis=1, keepdims=True)
        scale = lax.rsqrt(total * (1.0 / D) + EPS)
        for k in range(NY):
            cols = slice(k * CH, (k + 1) * CH)
            v = parts(k).astype(F32)
            nrm[rows, cols] = (v * scale * gain[:, cols]).astype(BF16)

    def norm(i, _):
        rows = pl.ds(pl.multiple_of(i * 32, 32), 32)
        normed(lambda k: tok[k, rows, :], rows)
        return 0

    serve(out_b[2])
    lax.fori_loop(0, TOK // 32, norm, 0)
    normed(lambda k: hal[k].reshape(2 * PAD, CH), pl.ds(TOK, 2 * PAD))
    in_arrived(0)

    has_before = jnp.where(s > 0, 1.0, 0.0).astype(F32)
    has_after = jnp.where(s < NZ * NX * NC - 1, 1.0, 0.0).astype(F32)

    def project(col, rows):
        w = win[:, :, :, :, col : col + 256].reshape(D, 256)
        return jnp.dot(nrm[:rows, :], w, preferred_element_type=F32).astype(BF16)

    for n in range(2):
        u = project(CH + n * 256, TOK + 2 * PAD)
        for k in range(2):
            v = u[:, k * 128 : (k + 1) * 128].astype(F32)
            ulf[2 * n + k, PAD : PAD + TOK, :] = v[:TOK]
            ulf[2 * n + k, 0:PAD, :] = v[TOK : TOK + PAD] * has_before
            ulf[2 * n + k, PAD + TOK :, :] = v[TOK + PAD :] * has_after
    serve(out_b[3], out_a[2])
    serve(out_rows[0])
    for load in loads[4:6]:
        load.wait()

    def block(b):
        lanes = slice(b * 128, (b + 1) * 128)
        tap = taps[:, lanes].astype(F32)
        acc = ulf[b, PAD - 2 : PAD - 2 + TOK, :] * tap[0:1]
        for k in range(1, 4):
            acc = acc + ulf[b, PAD - 2 + k : PAD - 2 + k + TOK, :] * tap[k : k + 1]
        conv = acc.astype(BF16)
        cvb[...] = conv.astype(F32)
        for d in range(2):
            gs[2 * d] = jnp.dot(conv, rgv[d, b], preferred_element_type=F32)
            gs[2 * d + 1] = jnp.dot(conv, igv[d, b], preferred_element_type=F32)

        for j in range(SEGS):
            rows, padded = slice(j * SEG, (j + 1) * SEG), slice(j * STEP, j * STEP + SEG)
            value = cvb[rows, :]
            for d in range(2):
                rate = logistic(gs[2 * d, rows, :])
                gate = logistic(gs[2 * d + 1, rows, :])
                keep_log = -8.0 * rate * decay[d : d + 1, lanes] + ldb[d, rows, :]
                keep = jnp.exp(keep_log)
                rest = one_minus_exp(2.0 * keep_log, keep * keep)
                aa[d, b, padded, :] = keep
                bb[d, b, padded, :] = root(rest) * gate * value

    block(0)
    block(1)
    block(2)
    block(3)

    def scan_step(t, carry):
        new = []
        for d in range(2):
            at = pl.ds(t if d == 0 else SEG - 1 - t, SEGS, stride=STEP)
            for b in range(4):
                prod, state = carry[2 * (4 * d + b)], carry[2 * (4 * d + b) + 1]
                keep = aa[d, b, at, :]
                state = keep * state + bb[d, b, at, :]
                prod = prod * keep
                aa[d, b, at, :] = prod
                bb[d, b, at, :] = state
                new += [prod, state]
        return tuple(new)

    ones, zeros = jnp.ones((SEGS, 128), F32), jnp.zeros((SEGS, 128), F32)
    ends = lax.fori_loop(0, SEG, scan_step, (ones, zeros) * 8, unroll=2)
    for d in range(2):
        for b in range(4):
            for k in range(2):
                sg[k, d, :, b * 128 : (b + 1) * 128] = ends[2 * (4 * d + b) + k]
    me = x * NC + c
    for d in range(2):
        prod, state = jnp.ones((1, CH), F32), jnp.zeros((1, CH), F32)
        for j in range(SEGS) if d == 0 else reversed(range(SEGS)):
            ex[0, d, j : j + 1, :] = prod
            ex[1, d, j : j + 1, :] = state
            keep = sg[0, d, j : j + 1, :]
            state = keep * state + sg[1, d, j : j + 1, :]
            prod = prod * keep
        c1[me, 2 * d : 2 * d + 1, :] = prod
        c1[me, 2 * d + 1 : 2 * d + 2, :] = state
    g_k1, k1 = links.group(c1.at[pl.ds(0, 7)]), links.slot()
    for dx, dc in around:
        links.put(c1.at[me], c1.at[me], g_k1, k1, sp_1=xx(dx), sp_2=lax.rem(c + dc, NC))

    for n in range(2):
        pext[OWN : OWN + TOK, n * 256 : (n + 1) * 256] = project(n * 256, TOK)
    g_ph = links.group(pext.at[pl.ds(0, 2 * OWN)])
    ph = {d: links.slot() for d in (1, -1)}
    links.put(pext.at[pl.ds(TOK, OWN)], pext.at[pl.ds(0, OWN)], g_ph, ph[1], **after)
    links.put(pext.at[pl.ds(OWN, OWN)], pext.at[pl.ds(OWN + TOK, OWN)], g_ph, ph[-1], **before)
    serve(out_b[4], out_a[3])

    def combine(table, mine):
        full, inside = [], []
        for d in range(2):
            count = NZ
            prod, state = jnp.ones((1, CH), F32), jnp.zeros((1, CH), F32)
            in_p, in_s = prod, state
            for k in range(count) if d == 0 else reversed(range(count)):
                keep = table[k, 2 * d : 2 * d + 1, :]
                state = keep * state + table[k, 2 * d + 1 : 2 * d + 2, :]
                prod = prod * keep
                passed = (k < mine) if d == 0 else (k > mine)
                in_p = jnp.where(passed, prod, in_p)
                in_s = jnp.where(passed, state, in_s)
            full.append((prod, state))
            inside.append((in_p, in_s))
        return full, inside

    def pooled(n):
        cols = slice(n * 256, (n + 1) * 256)
        total = jnp.dot(box[...], pext[:, cols], preferred_element_type=F32)
        own = pext[OWN : OWN + TOK, cols].astype(F32)
        scale = jnp.concatenate([rcp[...], rcp[...]], axis=1)
        pdf[:, cols] = (total * scale - own).astype(BF16)

    links.got(c1.at[pl.ds(0, 7)], k1, **after)
    full, near = combine(c1, me)
    for d in range(2):
        c2[z, 2 * d : 2 * d + 1, :] = full[d][0]
        c2[z, 2 * d + 1 : 2 * d + 2, :] = full[d][1]
    g_k2, k2 = links.group(c2.at[pl.ds(0, 7)]), links.slot()
    for d in range(1, NZ):
        links.put(c2.at[z], c2.at[z], g_k2, k2, sp_0=zz(d))

    serve(out_rows[1], out_rows[2], out_a[4])
    loads[3].wait()
    links.got(pext.at[pl.ds(0, OWN)], ph[1], **after)
    links.got(pext.at[pl.ds(OWN + TOK, OWN)], ph[-1], **before)
    for n in range(2):
        pooled(n)
    for n in range(2):
        cols = slice(n * 256, (n + 1) * 256)
        ycat[:, cols] = jnp.dot(pdf[...], pmv[0, :, cols], preferred_element_type=F32).astype(BF16)

    serve(out_rows[3])
    links.got(c2.at[pl.ds(0, 7)], k2, **after)
    _, far = combine(c2, z)
    for d in range(2):
        (np_, ns_), (fp_, fs_) = near[d], far[d]
        enter = np_ * fs_ + ns_ + (np_ * fp_) * start[d : d + 1, :]
        ex[0, d] = ex[1, d] + ex[0, d] * enter
    for j in range(SEGS):
        rows, padded = slice(j * SEG, (j + 1) * SEG), slice(j * STEP, j * STEP + SEG)
        for b in range(4):
            lanes = slice(b * 128, (b + 1) * 128)
            h0 = bb[0, b, padded, :] + aa[0, b, padded, :] * ex[0, 0, j : j + 1, lanes]
            h1 = bb[1, b, padded, :] + aa[1, b, padded, :] * ex[0, 1, j : j + 1, lanes]
            ycat[rows, CH + b * 128 : CH + (b + 1) * 128] = (h0 + h1).astype(BF16)
    g_q1, g_q2, g_q3 = links.group(rs1), links.group(rs2), links.group(rs3)
    q1, q3 = links.slot(), links.slot()
    q2 = [links.slot() for _ in range(NZ)]

    def tile(n):
        turn = (0, -1, 1, -2, 2, -3, 3, 4)[n]
        return pl.ds(pl.multiple_of(zz(turn) * 256, 256), 256)

    def relay(n):
        cols = slice(n * 256, (n + 1) * 256)
        d = 1 if n % 2 == 0 else -1
        at = rs2.at[:, pl.ds(n * 256, 256)]
        links.got(at, q2[n], tp=yy(d))
        mg[:, cols] = (rs2[:, cols].astype(F32) + part[yy(d), :, cols].astype(F32)).astype(BF16)
        there = pl.ds(n * 256, 256)
        links.put(mg.at[:, there], rs3.at[:, tile(n)], g_q3, q3, tp=yy(d))

    for n, turn in enumerate((0, -1, 1, -2, 2, -3, 3, 4)):
        cols = slice(n * 256, (n + 1) * 256)
        here = pl.ds(n * 256, 256)
        out_arrived(turn)
        w = wout[zz(turn)].reshape(256, 2 * CH)
        acc = lax.dot_general(ycat[...], w, NT, preferred_element_type=F32)
        for k in range(NY):
            part[k, :, cols] = acc[k * OUT_ROWS : (k + 1) * OUT_ROWS].astype(BF16)
        d = 1 if n % 2 == 0 else -1
        links.put(part.at[yy(2), :, here], rs2.at[:, here], g_q2, q2[n], tp=yy(d))
        links.put(part.at[yy(-d), :, here], rs1.at[:, tile(n)], g_q1, q1, tp=yy(-d))
        pltpu.make_async_copy(part.at[y, :, here], own.at[:, tile(n)], local.at[0]).start()
        if n == 2:
            serve(out_a[5], out_rows[4])
        if n >= 5:
            relay(n - 5)
    for n in range(3, NZ):
        relay(n)
    links.got(rs1, q1, **after)
    links.got(rs3, q3, **after)
    pltpu.make_async_copy(rs1, own, local.at[0]).wait()
    links.drain(**after)


def per_device(
    tokens, norm_gain, w_pool_in, w_lru_in, pool_mix, conv_taps, rec_gate, in_gate, decay_rate,
    log_decay, start_state, w_out_pool, w_out_lru,
):
    anywhere = pl.BlockSpec(memory_space=pl.ANY)
    near = pl.BlockSpec(memory_space=pltpu.VMEM)
    buf = pltpu.VMEM
    own, near_sum, far_sum = pl.pallas_call(
        layer,
        out_shape=[jax.ShapeDtypeStruct((OUT_ROWS, D), BF16)] * 3,
        in_specs=[
            anywhere, near, anywhere, anywhere, anywhere, near, anywhere, anywhere, near, near,
            near, anywhere, anywhere,
        ],
        out_specs=[anywhere] * 3,
        scratch_shapes=[
            buf((NY, TOK, CH), BF16),
            buf((TOK + 2 * PAD, D), BF16),
            buf((NZ, NX, NC, 32, 2 * CH), BF16),
            buf((NZ, NX, NC, 32, 2 * CH), BF16),
            buf((1, CH, CH), BF16),
            buf((2, 4, 128, 128), BF16),
            buf((2, 4, 128, 128), BF16),
            buf((2, TOK, 128), F32),
            buf((TOK, EXT), BF16),
            buf((TOK, 128), F32),
            buf((4, TOK + 2 * PAD, 128), F32),
            buf((NY, 2, PAD, CH), BF16),
            buf((TOK, 128), F32),
            buf((EXT, CH), BF16),
            buf((TOK, CH), BF16),
            buf((4, TOK, 128), F32),
            buf((2, 4, SEGS * STEP + SEG, 128), F32),
            buf((2, 4, SEGS * STEP + SEG, 128), F32),
            buf((2, 2, SEGS, CH), F32),
            buf((2, 2, SEGS, CH), F32),
            buf((NX * NC, 4, CH), F32),
            buf((NZ, 4, CH), F32),
            buf((TOK, 2 * CH), BF16),
            buf((NY, OUT_ROWS, D), BF16),
            buf((OUT_ROWS, D), BF16),
            buf((OUT_ROWS, D), BF16),
            pltpu.SemaphoreType.DMA((N_SEND,)),
            pltpu.SemaphoreType.DMA((N_RECV,)),
            pltpu.SemaphoreType.DMA((N_LOCAL,)),
        ],
        compiler_params=pltpu.CompilerParams(
            collective_id=0, has_side_effects=True, vmem_limit_bytes=60 * 1024 * 1024
        ),
        name="layer",
    )(
        tokens, norm_gain.reshape(1, D), w_pool_in, w_lru_in, pool_mix, conv_taps, rec_gate,
        in_gate, decay_rate, log_decay, start_state, w_out_pool.T, w_out_lru.T,
    )
    total = own.astype(F32) + near_sum.astype(F32) + far_sum.astype(F32)
    return total.astype(BF16)


def solution(mesh):
    torus = Mesh(mesh.devices.reshape(NZ, NX, NC, mesh.shape["tp"]), SP_TP)
    in_specs = (
        P(SP, "tp"),
        P(),
        P(SP, "tp"),
        P(SP, "tp"),
        P("tp", None, None),
        P(None, "tp"),
        P(None, "tp", None, None),
        P(None, "tp", None, None),
        P(None, "tp"),
        P(None, SP),
        P(None, "tp"),
        P("tp", SP),
        P("tp", SP),
    )
    return jax.shard_map(
        per_device, mesh=torus, in_specs=in_specs, out_specs=P(SP_TP, None), check_vma=False
    )
```

```python
import functools

import jax
import jax.numpy as jnp
from jax import lax
from jax.experimental import pallas as pl
from jax.experimental.pallas import tpu as pltpu
from jax.sharding import Mesh
from jax.sharding import PartitionSpec as P

GRID_W = 32
REACH = 8
EPS = 1e-06
SP = ("sp_0", "sp_1", "sp_2")
SP_TP = ("sp_0", "sp_1", "sp_2", "tp")
NZ, NX, NC, NY = 8, 4, 2, 4
TOK = 384
D = 2048
CH = 512
SEGS = 8
SEG = TOK // SEGS
STEP = SEG + 1
OWN = REACH * GRID_W
EXT = TOK + 2 * OWN
PAD = 16
OUT_ROWS = TOK // NY
N_SEND = 25
N_RECV = 171
N_LOCAL = 8
F32 = jnp.float32
BF16 = jnp.bfloat16
NT = (((1,), (1,)), ((), ()))


class Links:
    def __init__(self, send, recv):
        self.send, self.recv, self.groups, self.used = send, recv, [], 0

    def slot(self):
        self.used += 1
        return self.used - 1

    def group(self, region):
        self.groups.append(region)
        return len(self.groups) - 1

    def copy(self, src, dst, group, slot, dev):
        return pltpu.make_async_remote_copy(
            src_ref=src,
            dst_ref=dst,
            send_sem=self.send.at[group],
            recv_sem=self.recv.at[slot],
            device_id=dev,
            device_id_type=pl.DeviceIdType.MESH,
        )

    def put(self, src, dst, group, slot, **dev):
        self.copy(src, dst, group, slot, dev).start()

    def got(self, region, slot, **dev):
        self.copy(region, region, 0, slot, dev).wait_recv()

    def drain(self, **dev):
        for group, region in enumerate(self.groups):
            self.copy(region, region, group, 0, dev).wait_send()


def weight_gather(links, buf, z, x, c, by_row):
    lo, hi = pl.ds(0, 16), pl.ds(16, 16)

    def zz(d):
        return lax.rem(z + (d + NZ), NZ)

    def xx(d):
        return lax.rem(x + (d + NX), NX)

    other = {"sp_2": 1 - c}
    both = (1, -1)
    rel = [0, -1, 1, -2, 2, -3, 3, 4]
    a1 = {dx: links.slot() for dx in (1, 3, 2)}
    a2 = {
        (s, k, e): links.slot()
        for s in both
        for e in range(NX)
        for k in range(1, 5 if (s == 1) == (e < 2) else 4)
    }
    b1 = {(s, k): links.slot() for s in both for k in range(1, 5 if s == 1 else 4)}
    b2 = {d: links.slot() for d in rel}
    dd = {d: links.slot() for d in rel} if by_row else dict.fromkeys(rel, links.slot())
    g_a1 = links.group(buf.at[0, pl.ds(0, 3), c, lo])
    g_a2 = links.group(buf.at[pl.ds(0, 7), pl.ds(0, NX), c, lo])
    g_b1 = links.group(buf.at[pl.ds(0, 7), 0, c, lo])
    g_b2 = links.group(buf.at[pl.ds(0, NZ), pl.ds(0, 3), c, lo])
    g_dd = links.group(buf.at[pl.ds(0, NZ), pl.ds(0, NX), c])

    def a_send(s, k, e):
        if (s, k, e) in a2:
            piece = buf.at[zz(-s * (k - 1)), xx(e), c, lo]
            links.put(piece, piece, g_a2, a2[s, k, e], sp_0=zz(s))

    def a_hop(s, k, e):
        if (s, k, e) in a2:
            links.got(buf.at[zz(-s * k), xx(e), c, lo], a2[s, k, e], sp_0=zz(s))
            a_send(s, k + 1, e)

    def a_side(dx):
        links.got(buf.at[z, xx(-dx), c, lo], a1[dx], sp_1=xx(dx))
        for s in both:
            a_send(s, 1, NX - dx)

    def b_send(s, k):
        if (s, k) in b1:
            piece = buf.at[zz(-s * (k - 1)), x, c, hi]
            links.put(piece, piece, g_b1, b1[s, k], sp_0=zz(s))

    def b_spread(d):
        piece = buf.at[zz(d), x, c, hi]
        for dx in (1, 3, 2):
            links.put(piece, piece, g_b2, b2[d], sp_1=xx(dx))

    def b_hop(s, k):
        if (s, k) in b1:
            links.got(buf.at[zz(-s * k), x, c, hi], b1[s, k], sp_0=zz(s))
            b_send(s, k + 1)
            if not by_row:
                b_spread(-s * k if k < 4 else 4)

    def row_done(d):
        links.got(buf.at[zz(d), pl.ds(0, 3), c, hi], b2[d], sp_1=xx(1))
        row = buf.at[zz(d), pl.ds(0, NX), c]
        links.put(row, row, g_dd, dd[d], **other)

    def first():
        own = buf.at[z, x, c, lo]
        for dx in (1, 3, 2):
            links.put(own, own, g_a1, a1[dx], sp_1=xx(dx))
        for s in both:
            b_send(s, 1)
            a_send(s, 1, 0)

    def arrived(d):
        of = zz(d) if by_row else pl.ds(0, NZ)
        links.got(buf.at[of, pl.ds(0, NX), 1 - c], dd[d], **other)

    def at(f, *args):
        return functools.partial(f, *args)

    along_b = [[at(b_spread, 0)]] + [[at(b_hop, s, k) for s in both] for k in range(1, 5)]
    along_a = [[first], [at(a_side, 1), at(a_side, 3)]]
    along_a[1] += [at(a_hop, s, 1, 0) for s in both] + [at(a_side, 2)]
    for k in range(2, 6):
        along_a.append(
            [at(a_hop, s, k, 0) for s in both]
            + [at(a_hop, s, k - 1, e) for e in (3, 1, 2) for s in both]
        )
    rows = [[at(row_done, d) for d in ds] for ds in ((0,), (-1, 1), (-2, 2), (-3, 3), (4,))]
    spread = [[at(b_spread, d) for d in ds] for ds in ((0,), (-1, 1), (-2, 2), (-3, 3), (4,))]
    return along_a, along_b, rows, arrived, spread


def logistic(v):
    return 1.0 / (1.0 + jnp.exp(-v))


def one_minus_exp(y, e):
    series = y * (-1.0 / 720.0) - 1.0 / 120.0
    for n in (24.0, 6.0, 2.0, 1.0):
        series = y * series - 1.0 / n
    return jnp.where(y > -0.125, y * series, 1.0 - e)


def root(v):
    return v * lax.rsqrt(jnp.maximum(v, 1e-37))


def layer(
    tokens, gain, wpi, wli, pmix, taps, rgate, igate, decay, logd, start, wop, wol, own, rs1, rs3,
    tok, nrm, wl, wp, wout, pmv, rgv, igv, ldb, box, rcp, ulf, hal, cvb, pext, pdf, gs, aa, bb,
    sg, ex, c1, c2, ycat, part, rs2, mg, send, recv, local,
):
    z, x, c = (lax.axis_index(n) for n in SP)
    y = lax.axis_index("tp")
    s = (z * NX + x) * NC + c
    links = Links(send, recv)

    def zz(d):
        return lax.rem(z + (d + NZ), NZ)

    def xx(d):
        return lax.rem(x + (d + NX), NX)

    def yy(d):
        return lax.rem(y + (d + NY), NY)

    def run_dev(d):
        t = lax.rem(s + (d + NZ * NX * NC), NZ * NX * NC)
        return {"sp_0": t // (NX * NC), "sp_1": lax.rem(t // NC, NX), "sp_2": lax.rem(t, NC)}

    after, before = run_dev(1), run_dev(-1)

    loads = [
        pltpu.make_async_copy(tokens, tok.at[y], local.at[0]),
        pltpu.make_async_copy(wpi, wp.at[z, x, c], local.at[1]),
        pltpu.make_async_copy(wli, wl.at[z, x, c], local.at[2]),
        pltpu.make_async_copy(pmix, pmv, local.at[3]),
        pltpu.make_async_copy(rgate, rgv, local.at[4]),
        pltpu.make_async_copy(igate, igv, local.at[5]),
        pltpu.make_async_copy(wop, wout.at[z, x, c, :, pl.ds(0, CH)], local.at[6]),
        pltpu.make_async_copy(wol, wout.at[z, x, c, :, pl.ds(CH, CH)], local.at[7]),
    ]
    for load in loads:
        load.start()

    barrier = pltpu.get_barrier_semaphore()
    peers = [{"tp": yy(1)}, {"tp": yy(-1)}, {"tp": yy(2)}, after, before]
    peers += [{"sp_0": zz(d)} for d in range(1, NZ)]
    around = [(dx, dc) for dx in range(NX) for dc in range(NC) if dx or dc]
    for dx, dc in around:
        peers.append({"sp_1": xx(dx), "sp_2": lax.rem(c + dc, NC)})
    for peer in peers:
        pl.semaphore_signal(barrier, inc=1, device_id=peer, device_id_type=pl.DeviceIdType.MESH)

    for d in range(2):
        for i in range(TOK // 128):
            rows = slice(i * 128, (i + 1) * 128)
            ldb[d, rows, :] = jnp.broadcast_to(logd[d : d + 1, rows], (128, 128)).T
    half = lax.shift_left(jnp.int32(1), y)
    grid_rows = TOK // GRID_W
    row_count = grid_rows * NZ * NX * NC
    first_row = s * grid_rows

    def boxes(i, _):
        at = pl.multiple_of(i * 32, 32)
        er = lax.shift_right_logical(lax.broadcasted_iota(jnp.int32, (32, EXT), 1), 5)
        ec = lax.broadcasted_iota(jnp.int32, (32, EXT), 1) & (GRID_W - 1)
        col = lax.broadcasted_iota(jnp.int32, (32, EXT), 0)
        low = jnp.maximum(i - half, -first_row) + REACH
        high = jnp.minimum(i + half, row_count - first_row) + REACH
        inside = (er >= low) & (er < high) & (ec >= col - half) & (ec < col + half)
        box[pl.ds(at, 32), :] = jnp.where(inside, 1.0, 0.0).astype(BF16)
        cc = lax.broadcasted_iota(jnp.int32, (32, 128), 0)
        cols = jnp.minimum(cc + half, GRID_W) - jnp.maximum(cc - half, 0)
        rcp[pl.ds(at, 32), :] = 1.0 / (cols * (high - low)).astype(F32)
        return 0

    lax.fori_loop(0, grid_rows, boxes, 0)

    pl.semaphore_wait(barrier, len(peers))
    for load in loads[:3] + loads[6:]:
        load.wait()

    halves = (pl.ds(0, TOK // 2), pl.ds(TOK // 2, TOK // 2))
    g_t1 = links.group(tok.at[pl.ds(0, 2)])
    g_t2 = links.group(tok.at[0])
    t1 = {(d, h): links.slot() for d in (1, -1) for h in (0, 1)}
    t2 = {d: links.slot() for d in (1, -1)}
    for i in (0, 1):
        for d in (1, -1):
            h = i if d == 1 else 1 - i
            piece = tok.at[y, halves[h]]
            links.put(piece, piece, g_t1, t1[d, h], tp=yy(d))
    g_ch, g_hs = links.group(hal.at[0]), links.group(hal.at[pl.ds(0, 3)])
    ch, hs = {d: links.slot() for d in (1, -1)}, links.slot()
    links.put(tok.at[y, pl.ds(TOK - PAD, PAD)], hal.at[y, 0], g_ch, ch[1], **after)
    links.put(tok.at[y, pl.ds(0, PAD)], hal.at[y, 1], g_ch, ch[-1], **before)
    lru_a, lru_b, lru_rows, lru_arrived, _ = weight_gather(links, wl, z, x, c, False)
    pool_a, pool_b, pool_rows, pool_arrived, _ = weight_gather(links, wp, z, x, c, False)
    out_a, out_b, out_rows, out_arrived, out_x = weight_gather(links, wout, z, x, c, True)

    def serve(*rounds):
        for turn in rounds:
            for step in turn:
                step()

    serve(lru_a[0], lru_b[0], pool_a[0])

    def token_relay():
        for d, h in ((1, 0), (-1, 1)):
            piece = tok.at[yy(-d), halves[h]]
            links.got(piece, t1[d, h], tp=yy(d))
            links.put(piece, piece, g_t2, t2[d], tp=yy(d))

    serve(lru_a[1][:2], lru_b[1], lru_a[1][2:], pool_b[0])
    links.got(hal.at[y, 0], ch[1], **after)
    links.got(hal.at[y, 1], ch[-1], **before)
    for d in (1, -1, 2):
        links.put(hal.at[y], hal.at[y], g_hs, hs, tp=yy(d))
    serve(lru_b[2], lru_a[2], lru_rows[0], pool_b[1], pool_a[1])
    token_relay()
    serve(lru_b[3], lru_a[3], lru_rows[1])
    serve(out_a[0], pool_b[2], pool_a[2], pool_rows[0])
    serve(lru_b[4], lru_a[4], lru_rows[2])
    serve(pool_b[3], pool_a[3], pool_rows[1])
    serve(lru_a[5], lru_rows[3], lru_rows[4], out_b[0])
    for d, h in ((1, 1), (-1, 0)):
        links.got(tok.at[yy(-d), halves[h]], t1[d, h], tp=yy(d))
    for d, h in ((1, 0), (-1, 1)):
        links.got(tok.at[yy(2), halves[h]], t2[d], tp=yy(d))

    links.got(hal.at[pl.ds(0, 3)], hs, tp=yy(1))

    def normed(parts, rows):
        total = jnp.zeros((32, 1), F32)
        for k in range(NY):
            v = parts(k).astype(F32)
            total = total + jnp.sum(v * v, axis=1, keepdims=True)
        scale = lax.rsqrt(total * (1.0 / D) + EPS)
        for k in range(NY):
            cols = slice(k * CH, (k + 1) * CH)
            v = parts(k).astype(F32)
            nrm[rows, cols] = (v * scale * gain[:, cols]).astype(BF16)

    def norm(i, _):
        rows = pl.ds(pl.multiple_of(i * 32, 32), 32)
        normed(lambda k: tok[k, rows, :], rows)
        return 0

    lax.fori_loop(0, TOK // 32, norm, 0)
    normed(lambda k: hal[k].reshape(2 * PAD, CH), pl.ds(TOK, 2 * PAD))
    serve(pool_b[4], pool_a[4], pool_rows[2])
    lru_arrived(0)

    has_before = jnp.where(s > 0, 1.0, 0.0).astype(F32)
    has_after = jnp.where(s < NZ * NX * NC - 1, 1.0, 0.0).astype(F32)

    def project(weights, col, rows):
        w = weights[:, :, :, :, col : col + 256].reshape(D, 256)
        return jnp.dot(nrm[:rows, :], w, preferred_element_type=F32).astype(BF16)

    for n in range(2):
        u = project(wl, n * 256, TOK + 2 * PAD)
        for k in range(2):
            v = u[:, k * 128 : (k + 1) * 128].astype(F32)
            ulf[2 * n + k, PAD : PAD + TOK, :] = v[:TOK]
            ulf[2 * n + k, 0:PAD, :] = v[TOK : TOK + PAD] * has_before
            ulf[2 * n + k, PAD + TOK :, :] = v[TOK + PAD :] * has_after
    serve(out_b[1], out_x[1], out_a[1])
    for load in loads[4:6]:
        load.wait()

    def block(b):
        lanes = slice(b * 128, (b + 1) * 128)
        tap = taps[:, lanes].astype(F32)
        acc = ulf[b, PAD - 2 : PAD - 2 + TOK, :] * tap[0:1]
        for k in range(1, 4):
            acc = acc + ulf[b, PAD - 2 + k : PAD - 2 + k + TOK, :] * tap[k : k + 1]
        conv = acc.astype(BF16)
        cvb[...] = conv.astype(F32)
        for d in range(2):
            gs[2 * d] = jnp.dot(conv, rgv[d, b], preferred_element_type=F32)
            gs[2 * d + 1] = jnp.dot(conv, igv[d, b], preferred_element_type=F32)

        for j in range(SEGS):
            rows, padded = slice(j * SEG, (j + 1) * SEG), slice(j * STEP, j * STEP + SEG)
            value = cvb[rows, :]
            for d in range(2):
                rate = logistic(gs[2 * d, rows, :])
                gate = logistic(gs[2 * d + 1, rows, :])
                keep_log = -8.0 * rate * decay[d : d + 1, lanes] + ldb[d, rows, :]
                keep = jnp.exp(keep_log)
                rest = one_minus_exp(2.0 * keep_log, keep * keep)
                aa[d, b, padded, :] = keep
                bb[d, b, padded, :] = root(rest) * gate * value

    block(0)
    block(1)
    block(2)
    serve(pool_a[5], pool_rows[3], pool_rows[4])
    block(3)

    def scan_step(t, carry):
        new = []
        for d in range(2):
            at = pl.ds(t if d == 0 else SEG - 1 - t, SEGS, stride=STEP)
            for b in range(4):
                prod, state = carry[2 * (4 * d + b)], carry[2 * (4 * d + b) + 1]
                keep = aa[d, b, at, :]
                state = keep * state + bb[d, b, at, :]
                prod = prod * keep
                aa[d, b, at, :] = prod
                bb[d, b, at, :] = state
                new += [prod, state]
        return tuple(new)

    ones, zeros = jnp.ones((SEGS, 128), F32), jnp.zeros((SEGS, 128), F32)
    ends = lax.fori_loop(0, SEG, scan_step, (ones, zeros) * 8, unroll=2)
    for d in range(2):
        for b in range(4):
            for k in range(2):
                sg[k, d, :, b * 128 : (b + 1) * 128] = ends[2 * (4 * d + b) + k]
    me = x * NC + c
    for d in range(2):
        prod, state = jnp.ones((1, CH), F32), jnp.zeros((1, CH), F32)
        for j in range(SEGS) if d == 0 else reversed(range(SEGS)):
            ex[0, d, j : j + 1, :] = prod
            ex[1, d, j : j + 1, :] = state
            keep = sg[0, d, j : j + 1, :]
            state = keep * state + sg[1, d, j : j + 1, :]
            prod = prod * keep
        c1[me, 2 * d : 2 * d + 1, :] = prod
        c1[me, 2 * d + 1 : 2 * d + 2, :] = state
    g_k1, k1 = links.group(c1.at[pl.ds(0, 7)]), links.slot()
    for dx, dc in around:
        links.put(c1.at[me], c1.at[me], g_k1, k1, sp_1=xx(dx), sp_2=lax.rem(c + dc, NC))

    serve(out_b[2], out_a[2])
    pool_arrived(0)
    for n in range(2):
        pext[OWN : OWN + TOK, n * 256 : (n + 1) * 256] = project(wp, n * 256, TOK)
    g_ph = links.group(pext.at[pl.ds(0, 2 * OWN)])
    ph = {d: links.slot() for d in (1, -1)}
    links.put(pext.at[pl.ds(TOK, OWN)], pext.at[pl.ds(0, OWN)], g_ph, ph[1], **after)
    links.put(pext.at[pl.ds(OWN, OWN)], pext.at[pl.ds(OWN + TOK, OWN)], g_ph, ph[-1], **before)

    def combine(table, mine):
        full, inside = [], []
        for d in range(2):
            count = NZ
            prod, state = jnp.ones((1, CH), F32), jnp.zeros((1, CH), F32)
            in_p, in_s = prod, state
            for k in range(count) if d == 0 else reversed(range(count)):
                keep = table[k, 2 * d : 2 * d + 1, :]
                state = keep * state + table[k, 2 * d + 1 : 2 * d + 2, :]
                prod = prod * keep
                passed = (k < mine) if d == 0 else (k > mine)
                in_p = jnp.where(passed, prod, in_p)
                in_s = jnp.where(passed, state, in_s)
            full.append((prod, state))
            inside.append((in_p, in_s))
        return full, inside

    def pooled(n):
        cols = slice(n * 256, (n + 1) * 256)
        total = jnp.dot(box[...], pext[:, cols], preferred_element_type=F32)
        own = pext[OWN : OWN + TOK, cols].astype(F32)
        scale = jnp.concatenate([rcp[...], rcp[...]], axis=1)
        pdf[:, cols] = (total * scale - own).astype(BF16)

    serve(out_x[2])
    links.got(c1.at[pl.ds(0, 7)], k1, **after)
    full, near = combine(c1, me)
    for d in range(2):
        c2[z, 2 * d : 2 * d + 1, :] = full[d][0]
        c2[z, 2 * d + 1 : 2 * d + 2, :] = full[d][1]
    g_k2, k2 = links.group(c2.at[pl.ds(0, 7)]), links.slot()
    for d in range(1, NZ):
        links.put(c2.at[z], c2.at[z], g_k2, k2, sp_0=zz(d))

    serve(out_b[3], out_x[3], out_a[3], out_rows[0], out_rows[1])
    loads[3].wait()
    links.got(pext.at[pl.ds(0, OWN)], ph[1], **after)
    links.got(pext.at[pl.ds(OWN + TOK, OWN)], ph[-1], **before)
    for n in range(2):
        pooled(n)
    for n in range(2):
        cols = slice(n * 256, (n + 1) * 256)
        ycat[:, cols] = jnp.dot(pdf[...], pmv[0, :, cols], preferred_element_type=F32).astype(BF16)

    links.got(c2.at[pl.ds(0, 7)], k2, **after)
    _, far = combine(c2, z)
    for d in range(2):
        (np_, ns_), (fp_, fs_) = near[d], far[d]
        enter = np_ * fs_ + ns_ + (np_ * fp_) * start[d : d + 1, :]
        ex[0, d] = ex[1, d] + ex[0, d] * enter
    for j in range(SEGS):
        rows, padded = slice(j * SEG, (j + 1) * SEG), slice(j * STEP, j * STEP + SEG)
        for b in range(4):
            lanes = slice(b * 128, (b + 1) * 128)
            h0 = bb[0, b, padded, :] + aa[0, b, padded, :] * ex[0, 0, j : j + 1, lanes]
            h1 = bb[1, b, padded, :] + aa[1, b, padded, :] * ex[0, 1, j : j + 1, lanes]
            ycat[rows, CH + b * 128 : CH + (b + 1) * 128] = (h0 + h1).astype(BF16)
    g_q1, g_q2, g_q3 = links.group(rs1), links.group(rs2), links.group(rs3)
    q1, q3 = links.slot(), links.slot()
    q2 = [links.slot() for _ in range(NZ)]

    def tile(n):
        turn = (0, -1, 1, -2, 2, -3, 3, 4)[n]
        return pl.ds(pl.multiple_of(zz(turn) * 256, 256), 256)

    def relay(n):
        cols = slice(n * 256, (n + 1) * 256)
        d = 1 if n % 2 == 0 else -1
        at = rs2.at[:, pl.ds(n * 256, 256)]
        links.got(at, q2[n], tp=yy(d))
        mg[:, cols] = (rs2[:, cols].astype(F32) + part[yy(d), :, cols].astype(F32)).astype(BF16)
        there = pl.ds(n * 256, 256)
        links.put(mg.at[:, there], rs3.at[:, tile(n)], g_q3, q3, tp=yy(d))

    for n, turn in enumerate((0, -1, 1, -2, 2, -3, 3, 4)):
        cols = slice(n * 256, (n + 1) * 256)
        here = pl.ds(n * 256, 256)
        out_arrived(turn)
        w = wout[zz(turn)].reshape(256, 2 * CH)
        acc = lax.dot_general(ycat[...], w, NT, preferred_element_type=F32)
        for k in range(NY):
            part[k, :, cols] = acc[k * OUT_ROWS : (k + 1) * OUT_ROWS].astype(BF16)
        d = 1 if n % 2 == 0 else -1
        links.put(part.at[yy(2), :, here], rs2.at[:, here], g_q2, q2[n], tp=yy(d))
        links.put(part.at[yy(-d), :, here], rs1.at[:, tile(n)], g_q1, q1, tp=yy(-d))
        pltpu.make_async_copy(part.at[y, :, here], own.at[:, tile(n)], local.at[0]).start()
        if n == 1:
            serve(out_b[4], out_x[4], out_a[4], out_rows[2], out_rows[3])
        if n == 4:
            serve(out_a[5], out_rows[4])
        if n >= 5:
            relay(n - 5)
    for n in range(3, NZ):
        relay(n)
    links.got(rs1, q1, **after)
    links.got(rs3, q3, **after)
    pltpu.make_async_copy(rs1, own, local.at[0]).wait()
    links.drain(**after)


def per_device(
    tokens, norm_gain, w_pool_in, w_lru_in, pool_mix, conv_taps, rec_gate, in_gate, decay_rate,
    log_decay, start_state, w_out_pool, w_out_lru,
):
    anywhere = pl.BlockSpec(memory_space=pl.ANY)
    near = pl.BlockSpec(memory_space=pltpu.VMEM)
    buf = pltpu.VMEM
    own, near_sum, far_sum = pl.pallas_call(
        layer,
        out_shape=[jax.ShapeDtypeStruct((OUT_ROWS, D), BF16)] * 3,
        in_specs=[
            anywhere, near, anywhere, anywhere, anywhere, near, anywhere, anywhere, near, near,
            near, anywhere, anywhere,
        ],
        out_specs=[anywhere] * 3,
        scratch_shapes=[
            buf((NY, TOK, CH), BF16),
            buf((TOK + 2 * PAD, D), BF16),
            buf((NZ, NX, NC, 32, CH), BF16),
            buf((NZ, NX, NC, 32, CH), BF16),
            buf((NZ, NX, NC, 32, 2 * CH), BF16),
            buf((1, CH, CH), BF16),
            buf((2, 4, 128, 128), BF16),
            buf((2, 4, 128, 128), BF16),
            buf((2, TOK, 128), F32),
            buf((TOK, EXT), BF16),
            buf((TOK, 128), F32),
            buf((4, TOK + 2 * PAD, 128), F32),
            buf((NY, 2, PAD, CH), BF16),
            buf((TOK, 128), F32),
            buf((EXT, CH), BF16),
            buf((TOK, CH), BF16),
            buf((4, TOK, 128), F32),
            buf((2, 4, SEGS * STEP + SEG, 128), F32),
            buf((2, 4, SEGS * STEP + SEG, 128), F32),
            buf((2, 2, SEGS, CH), F32),
            buf((2, 2, SEGS, CH), F32),
            buf((NX * NC, 4, CH), F32),
            buf((NZ, 4, CH), F32),
            buf((TOK, 2 * CH), BF16),
            buf((NY, OUT_ROWS, D), BF16),
            buf((OUT_ROWS, D), BF16),
            buf((OUT_ROWS, D), BF16),
            pltpu.SemaphoreType.DMA((N_SEND,)),
            pltpu.SemaphoreType.DMA((N_RECV,)),
            pltpu.SemaphoreType.DMA((N_LOCAL,)),
        ],
        compiler_params=pltpu.CompilerParams(
            collective_id=0, has_side_effects=True, vmem_limit_bytes=60 * 1024 * 1024
        ),
        name="layer",
    )(
        tokens, norm_gain.reshape(1, D), w_pool_in, w_lru_in, pool_mix, conv_taps, rec_gate,
        in_gate, decay_rate, log_decay, start_state, w_out_pool.T, w_out_lru.T,
    )
    total = own.astype(F32) + near_sum.astype(F32) + far_sum.astype(F32)
    return total.astype(BF16)


def solution(mesh):
    torus = Mesh(mesh.devices.reshape(NZ, NX, NC, mesh.shape["tp"]), SP_TP)
    in_specs = (
        P(SP, "tp"),
        P(),
        P(SP, "tp"),
        P(SP, "tp"),
        P("tp", None, None),
        P(None, "tp"),
        P(None, "tp", None, None),
        P(None, "tp", None, None),
        P(None, "tp"),
        P(None, SP),
        P(None, "tp"),
        P("tp", SP),
        P("tp", SP),
    )
    return jax.shard_map(
        per_device, mesh=torus, in_specs=in_specs, out_specs=P(SP_TP, None), check_vma=False
    )
```

```python
import functools

import jax
import jax.numpy as jnp
from jax import lax
from jax.experimental import pallas as pl
from jax.experimental.pallas import tpu as pltpu
from jax.sharding import Mesh
from jax.sharding import PartitionSpec as P

GRID_W = 32
REACH = 8
EPS = 1e-06
SP = ("sp_0", "sp_1", "sp_2")
SP_TP = ("sp_0", "sp_1", "sp_2", "tp")
NZ, NX, NC, NY = 8, 4, 2, 4
TOK = 384
D = 2048
CH = 512
SEGS = 8
SEG = TOK // SEGS
STEP = SEG + 1
OWN = REACH * GRID_W
EXT = TOK + 2 * OWN
PAD = 16
OUT_ROWS = TOK // NY
N_SEND = 25
N_RECV = 148
N_LOCAL = 8
F32 = jnp.float32
BF16 = jnp.bfloat16
NT = (((1,), (1,)), ((), ()))


class Links:
    def __init__(self, send, recv):
        self.send, self.recv, self.groups, self.used = send, recv, [], 0

    def slot(self):
        self.used += 1
        return self.used - 1

    def group(self, region):
        self.groups.append(region)
        return len(self.groups) - 1

    def copy(self, src, dst, group, slot, dev):
        return pltpu.make_async_remote_copy(
            src_ref=src,
            dst_ref=dst,
            send_sem=self.send.at[group],
            recv_sem=self.recv.at[slot],
            device_id=dev,
            device_id_type=pl.DeviceIdType.MESH,
        )

    def put(self, src, dst, group, slot, **dev):
        self.copy(src, dst, group, slot, dev).start()

    def got(self, region, slot, **dev):
        self.copy(region, region, 0, slot, dev).wait_recv()

    def drain(self, **dev):
        for group, region in enumerate(self.groups):
            self.copy(region, region, group, 0, dev).wait_send()


def weight_gather(links, buf, z, x, c, by_row):
    lo, hi = pl.ds(0, 16), pl.ds(16, 16)

    def zz(d):
        return lax.rem(z + (d + NZ), NZ)

    def xx(d):
        return lax.rem(x + (d + NX), NX)

    other = {"sp_2": 1 - c}
    both = (1, -1)
    rel = [0, -1, 1, -2, 2, -3, 3, 4]
    a1 = {dx: links.slot() for dx in (1, 3, 2)}
    turn_slots = [links.slot() for _ in range(5)] if by_row else []
    a2 = {
        (s, k, e): 0 if by_row else links.slot()
        for s in both
        for e in range(NX)
        for k in range(1, 5 if (s == 1) == (e < 2) else 4)
    }
    turns = [[p for p in a2 if p[1] + (p[2] > 0) == r] for r in range(6)]
    if by_row:
        a2 = {p: slot for turn, slot in zip(turns[1:], turn_slots) for p in turn}
    b1 = {(s, k): links.slot() for s in both for k in range(1, 5 if s == 1 else 4)}
    b2 = {d: links.slot() for d in rel}
    dd = {d: links.slot() for d in rel} if by_row else dict.fromkeys(rel, links.slot())
    g_a1 = links.group(buf.at[0, pl.ds(0, 3), c, lo])
    g_a2 = links.group(buf.at[pl.ds(0, 7), pl.ds(0, NX), c, lo])
    g_b1 = links.group(buf.at[pl.ds(0, 7), 0, c, lo])
    g_b2 = links.group(buf.at[pl.ds(0, NZ), pl.ds(0, 3), c, lo])
    g_dd = links.group(buf.at[pl.ds(0, NZ), pl.ds(0, NX), c])

    def a_send(s, k, e):
        if (s, k, e) in a2:
            piece = buf.at[zz(-s * (k - 1)), xx(e), c, lo]
            links.put(piece, piece, g_a2, a2[s, k, e], sp_0=zz(s))

    def a_hop(s, k, e):
        if (s, k, e) in a2:
            links.got(buf.at[zz(-s * k), xx(e), c, lo], a2[s, k, e], sp_0=zz(s))
            a_send(s, k + 1, e)

    def a_turn(r):
        links.got(buf.at[pl.ds(0, len(turns[r])), 0, c, lo], turn_slots[r - 1], sp_0=zz(1))
        for s, k, e in turns[r]:
            a_send(s, k + 1, e)

    def a_side(dx):
        links.got(buf.at[z, xx(-dx), c, lo], a1[dx], sp_1=xx(dx))
        for s in both:
            a_send(s, 1, NX - dx)

    def b_send(s, k):
        if (s, k) in b1:
            piece = buf.at[zz(-s * (k - 1)), x, c, hi]
            links.put(piece, piece, g_b1, b1[s, k], sp_0=zz(s))

    def b_spread(d):
        piece = buf.at[zz(d), x, c, hi]
        for dx in (1, 3, 2):
            links.put(piece, piece, g_b2, b2[d], sp_1=xx(dx))

    def b_hop(s, k):
        if (s, k) in b1:
            links.got(buf.at[zz(-s * k), x, c, hi], b1[s, k], sp_0=zz(s))
            b_send(s, k + 1)
            if not by_row:
                b_spread(-s * k if k < 4 else 4)

    def row_done(d):
        links.got(buf.at[zz(d), pl.ds(0, 3), c, hi], b2[d], sp_1=xx(1))
        row = buf.at[zz(d), pl.ds(0, NX), c]
        links.put(row, row, g_dd, dd[d], **other)

    def first():
        own = buf.at[z, x, c, lo]
        for dx in (1, 3, 2):
            links.put(own, own, g_a1, a1[dx], sp_1=xx(dx))
        for s in both:
            b_send(s, 1)
            a_send(s, 1, 0)

    def arrived(d):
        of = zz(d) if by_row else pl.ds(0, NZ)
        links.got(buf.at[of, pl.ds(0, NX), 1 - c], dd[d], **other)

    def at(f, *args):
        return functools.partial(f, *args)

    along_b = [[at(b_spread, 0)]] + [[at(b_hop, s, k) for s in both] for k in range(1, 5)]
    along_a = [[first], [at(a_side, 1), at(a_side, 3)]]
    along_a[1] += [at(a_hop, s, 1, 0) for s in both] + [at(a_side, 2)]
    for k in range(2, 6):
        along_a.append(
            [at(a_hop, s, k, 0) for s in both]
            + [at(a_hop, s, k - 1, e) for e in (3, 1, 2) for s in both]
        )
    if by_row:
        along_a[1] = [at(a_side, 1), at(a_side, 3), at(a_turn, 1), at(a_side, 2)]
        along_a[2:] = [[at(a_turn, r)] for r in range(2, 6)]
    rows = [[at(row_done, d) for d in ds] for ds in ((0,), (-1, 1), (-2, 2), (-3, 3), (4,))]
    spread = [[at(b_spread, d) for d in ds] for ds in ((0,), (-1, 1), (-2, 2), (-3, 3), (4,))]
    return along_a, along_b, rows, arrived, spread


def logistic(v):
    return 1.0 / (1.0 + jnp.exp(-v))


def one_minus_exp(y, e):
    series = y * (-1.0 / 720.0) - 1.0 / 120.0
    for n in (24.0, 6.0, 2.0, 1.0):
        series = y * series - 1.0 / n
    return jnp.where(y > -0.125, y * series, 1.0 - e)


def root(v):
    return v * lax.rsqrt(jnp.maximum(v, 1e-37))


def layer(
    tokens, gain, wpi, wli, pmix, taps, rgate, igate, decay, logd, start, wop, wol, own, rs1, rs3,
    tok, nrm, wl, wp, wout, pmv, rgv, igv, ldb, box, rcp, ulf, hal, cvb, pext, pdf, gs, aa, bb,
    sg, ex, c1, c2, ycat, part, rs2, mg, send, recv, local,
):
    z, x, c = (lax.axis_index(n) for n in SP)
    y = lax.axis_index("tp")
    s = (z * NX + x) * NC + c
    links = Links(send, recv)

    def zz(d):
        return lax.rem(z + (d + NZ), NZ)

    def xx(d):
        return lax.rem(x + (d + NX), NX)

    def yy(d):
        return lax.rem(y + (d + NY), NY)

    def run_dev(d):
        t = lax.rem(s + (d + NZ * NX * NC), NZ * NX * NC)
        return {"sp_0": t // (NX * NC), "sp_1": lax.rem(t // NC, NX), "sp_2": lax.rem(t, NC)}

    after, before = run_dev(1), run_dev(-1)

    loads = [
        pltpu.make_async_copy(tokens, tok.at[y], local.at[0]),
        pltpu.make_async_copy(wpi, wp.at[z, x, c], local.at[1]),
        pltpu.make_async_copy(wli, wl.at[z, x, c], local.at[2]),
        pltpu.make_async_copy(pmix, pmv, local.at[3]),
        pltpu.make_async_copy(rgate, rgv, local.at[4]),
        pltpu.make_async_copy(igate, igv, local.at[5]),
        pltpu.make_async_copy(wop, wout.at[z, x, c, :, pl.ds(0, CH)], local.at[6]),
        pltpu.make_async_copy(wol, wout.at[z, x, c, :, pl.ds(CH, CH)], local.at[7]),
    ]
    for load in loads:
        load.start()

    barrier = pltpu.get_barrier_semaphore()
    peers = [{"tp": yy(1)}, {"tp": yy(-1)}, {"tp": yy(2)}, after, before]
    peers += [{"sp_0": zz(d)} for d in range(1, NZ)]
    around = [(dx, dc) for dx in range(NX) for dc in range(NC) if dx or dc]
    for dx, dc in around:
        peers.append({"sp_1": xx(dx), "sp_2": lax.rem(c + dc, NC)})
    for peer in peers:
        pl.semaphore_signal(barrier, inc=1, device_id=peer, device_id_type=pl.DeviceIdType.MESH)

    for d in range(2):
        for i in range(TOK // 128):
            rows = slice(i * 128, (i + 1) * 128)
            ldb[d, rows, :] = jnp.broadcast_to(logd[d : d + 1, rows], (128, 128)).T
    half = lax.shift_left(jnp.int32(1), y)
    grid_rows = TOK // GRID_W
    row_count = grid_rows * NZ * NX * NC
    first_row = s * grid_rows

    def boxes(i, _):
        at = pl.multiple_of(i * 32, 32)
        er = lax.shift_right_logical(lax.broadcasted_iota(jnp.int32, (32, EXT), 1), 5)
        ec = lax.broadcasted_iota(jnp.int32, (32, EXT), 1) & (GRID_W - 1)
        col = lax.broadcasted_iota(jnp.int32, (32, EXT), 0)
        low = jnp.maximum(i - half, -first_row) + REACH
        high = jnp.minimum(i + half, row_count - first_row) + REACH
        inside = (er >= low) & (er < high) & (ec >= col - half) & (ec < col + half)
        box[pl.ds(at, 32), :] = jnp.where(inside, 1.0, 0.0).astype(BF16)
        cc = lax.broadcasted_iota(jnp.int32, (32, 128), 0)
        cols = jnp.minimum(cc + half, GRID_W) - jnp.maximum(cc - half, 0)
        rcp[pl.ds(at, 32), :] = 1.0 / (cols * (high - low)).astype(F32)
        return 0

    lax.fori_loop(0, grid_rows, boxes, 0)

    pl.semaphore_wait(barrier, len(peers))
    for load in loads[:3] + loads[6:]:
        load.wait()

    halves = (pl.ds(0, TOK // 2), pl.ds(TOK // 2, TOK // 2))
    g_t1 = links.group(tok.at[pl.ds(0, 2)])
    g_t2 = links.group(tok.at[0])
    t1 = {(d, h): links.slot() for d in (1, -1) for h in (0, 1)}
    t2 = {d: links.slot() for d in (1, -1)}
    for i in (0, 1):
        for d in (1, -1):
            h = i if d == 1 else 1 - i
            piece = tok.at[y, halves[h]]
            links.put(piece, piece, g_t1, t1[d, h], tp=yy(d))
    g_ch, g_hs = links.group(hal.at[0]), links.group(hal.at[pl.ds(0, 3)])
    ch, hs = {d: links.slot() for d in (1, -1)}, links.slot()
    links.put(tok.at[y, pl.ds(TOK - PAD, PAD)], hal.at[y, 0], g_ch, ch[1], **after)
    links.put(tok.at[y, pl.ds(0, PAD)], hal.at[y, 1], g_ch, ch[-1], **before)
    lru_a, lru_b, lru_rows, lru_arrived, _ = weight_gather(links, wl, z, x, c, False)
    pool_a, pool_b, pool_rows, pool_arrived, _ = weight_gather(links, wp, z, x, c, False)
    out_a, out_b, out_rows, out_arrived, out_x = weight_gather(links, wout, z, x, c, True)

    def serve(*rounds):
        for turn in rounds:
            for step in turn:
                step()

    serve(lru_a[0], lru_b[0], pool_a[0])

    def token_relay():
        for d, h in ((1, 0), (-1, 1)):
            piece = tok.at[yy(-d), halves[h]]
            links.got(piece, t1[d, h], tp=yy(d))
            links.put(piece, piece, g_t2, t2[d], tp=yy(d))

    serve(lru_a[1][:2], lru_b[1], lru_a[1][2:], pool_b[0])
    links.got(hal.at[y, 0], ch[1], **after)
    links.got(hal.at[y, 1], ch[-1], **before)
    for d in (1, -1, 2):
        links.put(hal.at[y], hal.at[y], g_hs, hs, tp=yy(d))
    serve(lru_b[2], lru_a[2], lru_rows[0], pool_b[1], pool_a[1])
    token_relay()
    serve(lru_b[3], lru_a[3], lru_rows[1])
    serve(out_a[0], pool_b[2], pool_a[2], pool_rows[0])
    serve(lru_b[4], lru_a[4], lru_rows[2])
    serve(pool_b[3], pool_a[3], pool_rows[1])
    serve(lru_a[5], lru_rows[3], lru_rows[4], out_b[0])
    for d, h in ((1, 1), (-1, 0)):
        links.got(tok.at[yy(-d), halves[h]], t1[d, h], tp=yy(d))
    for d, h in ((1, 0), (-1, 1)):
        links.got(tok.at[yy(2), halves[h]], t2[d], tp=yy(d))

    links.got(hal.at[pl.ds(0, 3)], hs, tp=yy(1))

    def normed(parts, rows):
        total = jnp.zeros((32, 1), F32)
        for k in range(NY):
            v = parts(k).astype(F32)
            total = total + jnp.sum(v * v, axis=1, keepdims=True)
        scale = lax.rsqrt(total * (1.0 / D) + EPS)
        for k in range(NY):
            cols = slice(k * CH, (k + 1) * CH)
            v = parts(k).astype(F32)
            nrm[rows, cols] = (v * scale * gain[:, cols]).astype(BF16)

    def norm(i, _):
        rows = pl.ds(pl.multiple_of(i * 32, 32), 32)
        normed(lambda k: tok[k, rows, :], rows)
        return 0

    lax.fori_loop(0, TOK // 32, norm, 0)
    normed(lambda k: hal[k].reshape(2 * PAD, CH), pl.ds(TOK, 2 * PAD))
    serve(pool_b[4], pool_a[4], pool_rows[2])
    lru_arrived(0)

    has_before = jnp.where(s > 0, 1.0, 0.0).astype(F32)
    has_after = jnp.where(s < NZ * NX * NC - 1, 1.0, 0.0).astype(F32)

    def project(weights, col, rows):
        w = weights[:, :, :, :, col : col + 256].reshape(D, 256)
        return jnp.dot(nrm[:rows, :], w, preferred_element_type=F32).astype(BF16)

    for n in range(2):
        u = project(wl, n * 256, TOK + 2 * PAD)
        for k in range(2):
            v = u[:, k * 128 : (k + 1) * 128].astype(F32)
            ulf[2 * n + k, PAD : PAD + TOK, :] = v[:TOK]
            ulf[2 * n + k, 0:PAD, :] = v[TOK : TOK + PAD] * has_before
            ulf[2 * n + k, PAD + TOK :, :] = v[TOK + PAD :] * has_after
    serve(out_b[1], out_x[1], out_a[1])
    for load in loads[4:6]:
        load.wait()

    def block(b):
        lanes = slice(b * 128, (b + 1) * 128)
        tap = taps[:, lanes].astype(F32)
        acc = ulf[b, PAD - 2 : PAD - 2 + TOK, :] * tap[0:1]
        for k in range(1, 4):
            acc = acc + ulf[b, PAD - 2 + k : PAD - 2 + k + TOK, :] * tap[k : k + 1]
        conv = acc.astype(BF16)
        cvb[...] = conv.astype(F32)
        for d in range(2):
            gs[2 * d] = jnp.dot(conv, rgv[d, b], preferred_element_type=F32)
            gs[2 * d + 1] = jnp.dot(conv, igv[d, b], preferred_element_type=F32)

        for j in range(SEGS):
            rows, padded = slice(j * SEG, (j + 1) * SEG), slice(j * STEP, j * STEP + SEG)
            value = cvb[rows, :]
            for d in range(2):
                rate = logistic(gs[2 * d, rows, :])
                gate = logistic(gs[2 * d + 1, rows, :])
                keep_log = -8.0 * rate * decay[d : d + 1, lanes] + ldb[d, rows, :]
                keep = jnp.exp(keep_log)
                rest = one_minus_exp(2.0 * keep_log, keep * keep)
                aa[d, b, padded, :] = keep
                bb[d, b, padded, :] = root(rest) * gate * value

    block(0)
    block(1)
    block(2)
    serve(pool_a[5], pool_rows[3], pool_rows[4])
    block(3)

    def scan_step(t, carry):
        new = []
        for d in range(2):
            at = pl.ds(t if d == 0 else SEG - 1 - t, SEGS, stride=STEP)
            for b in range(4):
                prod, state = carry[2 * (4 * d + b)], carry[2 * (4 * d + b) + 1]
                keep = aa[d, b, at, :]
                state = keep * state + bb[d, b, at, :]
                prod = prod * keep
                aa[d, b, at, :] = prod
                bb[d, b, at, :] = state
                new += [prod, state]
        return tuple(new)

    ones, zeros = jnp.ones((SEGS, 128), F32), jnp.zeros((SEGS, 128), F32)
    ends = lax.fori_loop(0, SEG, scan_step, (ones, zeros) * 8, unroll=2)
    for d in range(2):
        for b in range(4):
            for k in range(2):
                sg[k, d, :, b * 128 : (b + 1) * 128] = ends[2 * (4 * d + b) + k]
    me = x * NC + c
    for d in range(2):
        prod, state = jnp.ones((1, CH), F32), jnp.zeros((1, CH), F32)
        for j in range(SEGS) if d == 0 else reversed(range(SEGS)):
            ex[0, d, j : j + 1, :] = prod
            ex[1, d, j : j + 1, :] = state
            keep = sg[0, d, j : j + 1, :]
            state = keep * state + sg[1, d, j : j + 1, :]
            prod = prod * keep
        c1[me, 2 * d : 2 * d + 1, :] = prod
        c1[me, 2 * d + 1 : 2 * d + 2, :] = state
    g_k1, k1 = links.group(c1.at[pl.ds(0, 7)]), links.slot()
    for dx, dc in around:
        links.put(c1.at[me], c1.at[me], g_k1, k1, sp_1=xx(dx), sp_2=lax.rem(c + dc, NC))

    serve(out_b[2], out_a[2])
    pool_arrived(0)
    for n in range(2):
        pext[OWN : OWN + TOK, n * 256 : (n + 1) * 256] = project(wp, n * 256, TOK)
    g_ph = links.group(pext.at[pl.ds(0, 2 * OWN)])
    ph = {d: links.slot() for d in (1, -1)}
    links.put(pext.at[pl.ds(TOK, OWN)], pext.at[pl.ds(0, OWN)], g_ph, ph[1], **after)
    links.put(pext.at[pl.ds(OWN, OWN)], pext.at[pl.ds(OWN + TOK, OWN)], g_ph, ph[-1], **before)

    def combine(table, mine):
        full, inside = [], []
        for d in range(2):
            count = NZ
            prod, state = jnp.ones((1, CH), F32), jnp.zeros((1, CH), F32)
            in_p, in_s = prod, state
            for k in range(count) if d == 0 else reversed(range(count)):
                keep = table[k, 2 * d : 2 * d + 1, :]
                state = keep * state + table[k, 2 * d + 1 : 2 * d + 2, :]
                prod = prod * keep
                passed = (k < mine) if d == 0 else (k > mine)
                in_p = jnp.where(passed, prod, in_p)
                in_s = jnp.where(passed, state, in_s)
            full.append((prod, state))
            inside.append((in_p, in_s))
        return full, inside

    def pooled(n):
        cols = slice(n * 256, (n + 1) * 256)
        total = jnp.dot(box[...], pext[:, cols], preferred_element_type=F32)
        own = pext[OWN : OWN + TOK, cols].astype(F32)
        scale = jnp.concatenate([rcp[...], rcp[...]], axis=1)
        pdf[:, cols] = (total * scale - own).astype(BF16)

    serve(out_x[2])
    links.got(c1.at[pl.ds(0, 7)], k1, **after)
    full, near = combine(c1, me)
    for d in range(2):
        c2[z, 2 * d : 2 * d + 1, :] = full[d][0]
        c2[z, 2 * d + 1 : 2 * d + 2, :] = full[d][1]
    g_k2, k2 = links.group(c2.at[pl.ds(0, 7)]), links.slot()
    for d in range(1, NZ):
        links.put(c2.at[z], c2.at[z], g_k2, k2, sp_0=zz(d))

    serve(out_b[3], out_x[3], out_a[3], out_rows[0], out_rows[1])
    loads[3].wait()
    links.got(pext.at[pl.ds(0, OWN)], ph[1], **after)
    links.got(pext.at[pl.ds(OWN + TOK, OWN)], ph[-1], **before)
    for n in range(2):
        pooled(n)
    for n in range(2):
        cols = slice(n * 256, (n + 1) * 256)
        ycat[:, cols] = jnp.dot(pdf[...], pmv[0, :, cols], preferred_element_type=F32).astype(BF16)

    links.got(c2.at[pl.ds(0, 7)], k2, **after)
    _, far = combine(c2, z)
    for d in range(2):
        (np_, ns_), (fp_, fs_) = near[d], far[d]
        enter = np_ * fs_ + ns_ + (np_ * fp_) * start[d : d + 1, :]
        ex[0, d] = ex[1, d] + ex[0, d] * enter
    for j in range(SEGS):
        rows, padded = slice(j * SEG, (j + 1) * SEG), slice(j * STEP, j * STEP + SEG)
        for b in range(4):
            lanes = slice(b * 128, (b + 1) * 128)
            h0 = bb[0, b, padded, :] + aa[0, b, padded, :] * ex[0, 0, j : j + 1, lanes]
            h1 = bb[1, b, padded, :] + aa[1, b, padded, :] * ex[0, 1, j : j + 1, lanes]
            ycat[rows, CH + b * 128 : CH + (b + 1) * 128] = (h0 + h1).astype(BF16)
    g_q1, g_q2, g_q3 = links.group(rs1), links.group(rs2), links.group(rs3)
    q1, q3 = links.slot(), links.slot()
    q2 = [links.slot() for _ in range(NZ)]

    def tile(n):
        turn = (0, -1, 1, -2, 2, -3, 3, 4)[n]
        return pl.ds(pl.multiple_of(zz(turn) * 256, 256), 256)

    def relay(n):
        cols = slice(n * 256, (n + 1) * 256)
        d = 1 if n % 2 == 0 else -1
        at = rs2.at[:, pl.ds(n * 256, 256)]
        links.got(at, q2[n], tp=yy(d))
        mg[:, cols] = (rs2[:, cols].astype(F32) + part[yy(d), :, cols].astype(F32)).astype(BF16)
        there = pl.ds(n * 256, 256)
        links.put(mg.at[:, there], rs3.at[:, tile(n)], g_q3, q3, tp=yy(d))

    for n, turn in enumerate((0, -1, 1, -2, 2, -3, 3, 4)):
        cols = slice(n * 256, (n + 1) * 256)
        here = pl.ds(n * 256, 256)
        out_arrived(turn)
        w = wout[zz(turn)].reshape(256, 2 * CH)
        acc = lax.dot_general(ycat[...], w, NT, preferred_element_type=F32)
        for k in range(NY):
            part[k, :, cols] = acc[k * OUT_ROWS : (k + 1) * OUT_ROWS].astype(BF16)
        d = 1 if n % 2 == 0 else -1
        links.put(part.at[yy(2), :, here], rs2.at[:, here], g_q2, q2[n], tp=yy(d))
        links.put(part.at[yy(-d), :, here], rs1.at[:, tile(n)], g_q1, q1, tp=yy(-d))
        pltpu.make_async_copy(part.at[y, :, here], own.at[:, tile(n)], local.at[0]).start()
        if n == 1:
            serve(out_b[4], out_x[4], out_a[4], out_rows[2], out_rows[3])
        if n == 4:
            serve(out_a[5], out_rows[4])
        if n >= 5:
            relay(n - 5)
    for n in range(3, NZ):
        relay(n)
    links.got(rs1, q1, **after)
    links.got(rs3, q3, **after)
    pltpu.make_async_copy(rs1, own, local.at[0]).wait()
    links.drain(**after)


def per_device(
    tokens, norm_gain, w_pool_in, w_lru_in, pool_mix, conv_taps, rec_gate, in_gate, decay_rate,
    log_decay, start_state, w_out_pool, w_out_lru,
):
    anywhere = pl.BlockSpec(memory_space=pl.ANY)
    near = pl.BlockSpec(memory_space=pltpu.VMEM)
    buf = pltpu.VMEM
    own, near_sum, far_sum = pl.pallas_call(
        layer,
        out_shape=[jax.ShapeDtypeStruct((OUT_ROWS, D), BF16)] * 3,
        in_specs=[
            anywhere, near, anywhere, anywhere, anywhere, near, anywhere, anywhere, near, near,
            near, anywhere, anywhere,
        ],
        out_specs=[anywhere] * 3,
        scratch_shapes=[
            buf((NY, TOK, CH), BF16),
            buf((TOK + 2 * PAD, D), BF16),
            buf((NZ, NX, NC, 32, CH), BF16),
            buf((NZ, NX, NC, 32, CH), BF16),
            buf((NZ, NX, NC, 32, 2 * CH), BF16),
            buf((1, CH, CH), BF16),
            buf((2, 4, 128, 128), BF16),
            buf((2, 4, 128, 128), BF16),
            buf((2, TOK, 128), F32),
            buf((TOK, EXT), BF16),
            buf((TOK, 128), F32),
            buf((4, TOK + 2 * PAD, 128), F32),
            buf((NY, 2, PAD, CH), BF16),
            buf((TOK, 128), F32),
            buf((EXT, CH), BF16),
            buf((TOK, CH), BF16),
            buf((4, TOK, 128), F32),
            buf((2, 4, SEGS * STEP + SEG, 128), F32),
            buf((2, 4, SEGS * STEP + SEG, 128), F32),
            buf((2, 2, SEGS, CH), F32),
            buf((2, 2, SEGS, CH), F32),
            buf((NX * NC, 4, CH), F32),
            buf((NZ, 4, CH), F32),
            buf((TOK, 2 * CH), BF16),
            buf((NY, OUT_ROWS, D), BF16),
            buf((OUT_ROWS, D), BF16),
            buf((OUT_ROWS, D), BF16),
            pltpu.SemaphoreType.DMA((N_SEND,)),
            pltpu.SemaphoreType.DMA((N_RECV,)),
            pltpu.SemaphoreType.DMA((N_LOCAL,)),
        ],
        compiler_params=pltpu.CompilerParams(
            collective_id=0, has_side_effects=True, vmem_limit_bytes=60 * 1024 * 1024
        ),
        name="layer",
    )(
        tokens, norm_gain.reshape(1, D), w_pool_in, w_lru_in, pool_mix, conv_taps, rec_gate,
        in_gate, decay_rate, log_decay, start_state, w_out_pool.T, w_out_lru.T,
    )
    total = own.astype(F32) + near_sum.astype(F32) + far_sum.astype(F32)
    return total.astype(BF16)


def solution(mesh):
    torus = Mesh(mesh.devices.reshape(NZ, NX, NC, mesh.shape["tp"]), SP_TP)
    in_specs = (
        P(SP, "tp"),
        P(),
        P(SP, "tp"),
        P(SP, "tp"),
        P("tp", None, None),
        P(None, "tp"),
        P(None, "tp", None, None),
        P(None, "tp", None, None),
        P(None, "tp"),
        P(None, SP),
        P(None, "tp"),
        P("tp", SP),
        P("tp", SP),
    )
    return jax.shard_map(
        per_device, mesh=torus, in_specs=in_specs, out_specs=P(SP_TP, None), check_vma=False
    )
```
